128 devices in a mesh: sp: 16 (over z, y), tp: 4 (over x), dp: 2 (over core).
Axes of the slice: x: 4, y: 4, z: 4, core: 2. Of those that a mesh axis runs over, the one named last changes fastest.
Arguments:
- latent: bfloat16 [2, 12288, 2048], P('dp', ('sp', 'tp')), may hold values from -3 to 3
- cond: bfloat16 [2, 2048], P('dp', 'sp'), may hold values from -6 to 6
- cond_ctx: bfloat16 [2048], P('sp'), may hold values from -6 to 6
- context: bfloat16 [2, 512, 2048], P('dp', 'sp'), may hold values from -6 to 6
- norm_gain: bfloat16 [2048], replicated, may hold values from 0.099609375 to 1.8984375
- mod_shift: bfloat16 [2048, 2048], P('sp', 'tp'), may hold values from -0.125 to 0.125
- mod_scale: bfloat16 [2048, 2048], P('sp', 'tp'), may hold values from -0.125 to 0.125
- mod_gate: bfloat16 [2048, 2048], P('sp', 'tp'), may hold values from -0.125 to 0.125
- w_query: bfloat16 [2048, 1024], P(None, 'tp'), may hold values from -0.125 to 0.125
- w_key: bfloat16 [2048, 256], P(None, 'tp'), may hold values from -0.125 to 0.125
- w_value: bfloat16 [2048, 256], P(None, 'tp'), may hold values from -0.125 to 0.125
- q_gain: bfloat16 [64], replicated, may hold values from 1 to 5.5
- k_gain: bfloat16 [64], replicated, may hold values from 1 to 5.5
- ctx_lift: float32 [16], P('tp'), may hold values from 1 to 3
- w_out: bfloat16 [1024, 2048], replicated, may hold values from -1.5 to 1.5
Outputs:
- mixed: bfloat16 [2, 12288, 2048], P('dp', ('sp', 'tp'))
The draws below stay inside these ranges and needn't reach their ends.
All inputs are finite; a program needn't handle non-finite values.
Results may differ from the reference program's by a relative error of at most 0.009.
The reference program's roundings to bfloat16 on the way count: a program that leaves them out, or rounds other values in their place, can miss the bound.
Values may be sent and summed in bfloat16 or wider, within the bound.
A program may use at most 64 MiB of HBM per device.

```python
import jax
import jax.numpy as jnp
from jax import lax

D = 2048
HEADS = 16
KV_HEADS = 4
HD = 64
GRID_W = 128
TOK_DEV = 768
CTX = 512
SAMPLES = 2
LAT = 12288
QW = 1024
KVW = 256
N_SP = 16


def draw_gain(key, salt):
    base = jax.random.uniform(jax.random.fold_in(key, salt), (HD,), jnp.float32, 1.0, 1.8)
    return base.astype(jnp.bfloat16)


def draw_q_gain(key, part):
    return draw_gain(key, 1)


def draw_k_gain(key, part):
    return draw_gain(key, 2)


def level_of(rng, shape, shards, low, top_value):
    def one(dim, blocks):
        draws = jax.random.uniform(jax.random.fold_in(jax.random.fold_in(rng, 6), dim), (blocks,), jnp.float32, low / len(shards), top_value / len(shards))
        return jnp.repeat(jnp.exp(draws), shape[dim] // blocks).reshape((-1,) + (1,) * (len(shape) - dim - 1))

    level = one(*shards[0])
    for cut in shards[1:]:
        level = level * one(*cut)
    return level


def bell_draw(key, dims, spread, reach, shards=(), held_as=jnp.bfloat16):
    entries = spread * jax.random.normal(key, dims, jnp.float32)
    if shards:
        entries = entries * level_of(key, dims, shards, -0.22, 0.18)
    return jnp.clip(entries, -reach, reach).astype(held_as)


def setup_inputs(seed: int = 0) -> dict:
    arg_keys = jax.random.split(jax.random.key(seed), 16)
    return {
        "latent": bell_draw(arg_keys[0], (SAMPLES, LAT, D), 0.5, 3.0, ((0, 2), (1, 64))),
        "cond": bell_draw(arg_keys[1], (SAMPLES, D), 1.0, 6.0, ((0, 2), (1, 16))),
        "cond_ctx": bell_draw(arg_keys[2], (D,), 1.0, 6.0, ((0, 16),)),
        "context": bell_draw(arg_keys[3], (SAMPLES, CTX, D), 1.0, 6.0, ((0, 2), (1, 16))),
        "norm_gain": jnp.clip(1.0 + 0.18 * jax.random.normal(arg_keys[4], (D,), jnp.float32), 0.099609375, 1.8984375).astype(jnp.bfloat16),
        "mod_shift": bell_draw(arg_keys[5], (D, D), D ** -0.5, 0.125, ((0, 16), (1, 4))),
        "mod_scale": bell_draw(arg_keys[6], (D, D), D ** -0.5, 0.125, ((0, 16), (1, 4))),
        "mod_gate": bell_draw(arg_keys[7], (D, D), D ** -0.5, 0.125, ((0, 16), (1, 4))),
        "w_query": bell_draw(arg_keys[8], (D, QW), D ** -0.5, 0.125, ((1, 4),)),
        "w_key": bell_draw(arg_keys[9], (D, KVW), D ** -0.5, 0.125, ((1, 4),)),
        "w_value": bell_draw(arg_keys[10], (D, KVW), D ** -0.5, 0.125, ((1, 4),)),
        "q_gain": draw_q_gain(jax.random.fold_in(arg_keys[15], 71), 0),
        "k_gain": draw_k_gain(jax.random.fold_in(arg_keys[15], 71), 0),
        "ctx_lift": jnp.clip(1.0 + 2.0 * jax.random.uniform(arg_keys[13], (HEADS,), jnp.float32) ** level_of(arg_keys[13], (HEADS,), ((0, 4),), -0.2, 0.2), 1.0, 3.0),
        "w_out": bell_draw(arg_keys[14], (QW, D), (QW // 64) ** -0.5, 1.5),
    }


EPS = 1e-06
THETA = 10000.0

def modulate(row_block, gain_vec, shift_rows, scale_rows):
    values = row_block.astype(jnp.float32)
    normed = values * lax.rsqrt(lax.optimization_barrier(jnp.mean(values * values, axis=-1, keepdims=True)) + EPS) * gain_vec.astype(jnp.float32)
    return (normed * (1.0 + scale_rows) + shift_rows).astype(jnp.bfloat16)

def head_norm(raw_proj, gain_vec):
    samples, tokens, width = raw_proj.shape
    pieces = raw_proj.reshape(samples, tokens, width // HD, HD)
    normed = pieces * lax.rsqrt(lax.optimization_barrier(jnp.mean(pieces * pieces, axis=-1, keepdims=True)) + EPS) * gain_vec.astype(jnp.float32)
    return normed.transpose(0, 2, 1, 3)

def rotate(vector, positions):
    pairs_count = vector.shape[-1] // 4
    grid_row = (positions // GRID_W).astype(jnp.float32)
    grid_col = (positions % GRID_W).astype(jnp.float32)
    inverse = THETA ** (-jnp.arange(pairs_count, dtype=jnp.float32) / pairs_count)
    angles = jnp.concatenate([grid_row[:, None] * inverse, grid_col[:, None] * inverse], axis=-1)
    cosine = jnp.cos(angles)
    sine_val = jnp.sin(angles)
    first_half = vector[..., 0::2]
    second_half = vector[..., 1::2]
    turned = jnp.stack([first_half * cosine - second_half * sine_val, first_half * sine_val + second_half * cosine], axis=-1)
    return turned.reshape(vector.shape)

def attend_head(operands):
    query_head, key_head, value_head, ctx_key_head, ctx_value_head, lift_row = operands
    group_size = query_head.shape[0]
    factor = HD ** (-0.5)
    query_blocks = jnp.moveaxis(query_head.reshape(group_size, N_SP, TOK_DEV, HD), 1, 0)

    def one_block(query_block):
        query_wide = query_block.astype(jnp.float32)
        scores = jnp.einsum('gbd,td->gbt', query_wide, key_head.astype(jnp.float32)) * factor
        ctx_scores = jnp.einsum('gbd,td->gbt', query_wide, ctx_key_head.astype(jnp.float32)) * factor + lift_row[:, None, None]
        peak = jnp.maximum(lax.optimization_barrier(jnp.max(scores, axis=-1)), lax.optimization_barrier(jnp.max(ctx_scores, axis=-1)))
        weights = jnp.exp(scores - peak[..., None])
        ctx_weights = jnp.exp(ctx_scores - peak[..., None])
        total = lax.optimization_barrier(jnp.sum(weights, axis=-1)) + lax.optimization_barrier(jnp.sum(ctx_weights, axis=-1))
        weights_low = lax.optimization_barrier(weights.astype(jnp.bfloat16)).astype(jnp.float32)
        ctx_low = lax.optimization_barrier(ctx_weights.astype(jnp.bfloat16)).astype(jnp.float32)
        summed = jnp.einsum('gbt,td->gbd', weights_low, value_head.astype(jnp.float32))
        summed = summed + jnp.einsum('gbt,td->gbd', ctx_low, ctx_value_head.astype(jnp.float32))
        return (summed / total[..., None]).astype(jnp.bfloat16)
    outputs = lax.map(one_block, query_blocks)
    return jnp.moveaxis(outputs, 0, 1).reshape(group_size, N_SP * TOK_DEV, HD)

def reference(latent, cond, cond_ctx, context, norm_gain, mod_shift, mod_scale, mod_gate, w_query, w_key, w_value, q_gain, k_gain, ctx_lift, w_out):
    samples = latent.shape[0]
    tokens = latent.shape[1]
    group_size = HEADS // KV_HEADS
    active = jax.nn.silu(jnp.concatenate([cond, cond_ctx[None, :]], axis=0).astype(jnp.float32)).astype(jnp.bfloat16)
    shift_rows = jnp.dot(active, mod_shift, preferred_element_type=jnp.float32)
    scale_rows = jnp.dot(active, mod_scale, preferred_element_type=jnp.float32)
    gate_rows = jnp.dot(active, mod_gate, preferred_element_type=jnp.float32)
    modulated = modulate(latent, norm_gain, shift_rows[:samples, None, :], scale_rows[:samples, None, :])
    ctx_mod = modulate(context, norm_gain, shift_rows[samples], scale_rows[samples])
    flat = modulated.reshape(-1, D)
    ctx_flat = ctx_mod.reshape(-1, D)
    qraw = jnp.dot(flat, w_query, preferred_element_type=jnp.float32).reshape(samples, tokens, QW)
    kraw = jnp.dot(flat, w_key, preferred_element_type=jnp.float32).reshape(samples, tokens, KVW)
    value_rows = jnp.dot(flat, w_value, preferred_element_type=jnp.float32).astype(jnp.bfloat16)
    kcraw = jnp.dot(ctx_flat, w_key, preferred_element_type=jnp.float32).reshape(samples, CTX, KVW)
    ctx_value_rows = jnp.dot(ctx_flat, w_value, preferred_element_type=jnp.float32).astype(jnp.bfloat16)
    positions = jnp.arange(tokens, dtype=jnp.int32)
    queries = rotate(head_norm(qraw, q_gain), positions).astype(jnp.bfloat16)
    queries = queries.reshape(samples, KV_HEADS, group_size, tokens, HD)
    key_rows = rotate(head_norm(kraw, k_gain), positions).astype(jnp.bfloat16)
    value_heads = value_rows.reshape(samples, tokens, KV_HEADS, HD).transpose(0, 2, 1, 3)
    ctx_keys = head_norm(kcraw, k_gain).astype(jnp.bfloat16)
    ctx_values = ctx_value_rows.reshape(samples, CTX, KV_HEADS, HD).transpose(0, 2, 1, 3)
    lift_table = ctx_lift.astype(jnp.float32).reshape(KV_HEADS, group_size)
    results = []
    for sample_idx in range(samples):
        attended = lax.map(attend_head, (queries[sample_idx], key_rows[sample_idx], value_heads[sample_idx], ctx_keys[sample_idx], ctx_values[sample_idx], lift_table))
        results.append(attended.transpose(2, 0, 1, 3).reshape(tokens, QW))
    head_rows = jnp.stack(results, axis=0)
    projected = jnp.dot(head_rows.reshape(-1, QW), w_out, preferred_element_type=jnp.float32).reshape(samples, tokens, D)
    return (latent.astype(jnp.float32) + gate_rows[:samples, None, :] * projected).astype(jnp.bfloat16)
```

```python
import functools

import jax
import jax.numpy as jnp
import numpy as np
from jax import lax
from jax.experimental import pallas as pl
from jax.experimental.pallas import tpu as pltpu
from jax.sharding import PartitionSpec as P

MESH = pl.DeviceIdType.MESH
HD = 64
GRID_W = 128
EPS = 1e-06
THETA = 10000.0
LOG2E = 1.4426950408889634
N_SP = 16
N_TP = 4
F32 = jnp.float32
BF16 = jnp.bfloat16
VMEM = pl.BlockSpec(memory_space=pltpu.VMEM)
ANY = pl.BlockSpec(memory_space=pl.ANY)
SMEM = pl.BlockSpec(memory_space=pltpu.SMEM)
LIMIT = 60 * 2**20


def angle_table():
    i = (np.arange(HD) // 2) % 16
    f = (THETA ** (-(i.astype(np.float32)) / np.float32(16))).astype(np.float32)
    table = np.repeat(f[:, None], GRID_W, axis=1)
    table[32:] = table[32:] * np.arange(GRID_W, dtype=np.float32)[None, :]
    return table.astype(np.float32)


def tall(x):
    return jnp.concatenate([x, jnp.zeros_like(x)], axis=0)


def project_kernel(
    lat, cond, condc, ctx, gain, m_shift, m_scale, m_gate, wq, wk, wv, qg, kg, table,
    q_out, kv_out, ctx_out, gate_out,
    xbuf, part, psum_in, mine, full, wall, ubuf, raw, cosb, sinb, scl, sft, cown, cbuf,
    x_send, x_recv, p_send, p_recv, t_send, t_recv, c_send, c_recv,
):
    sp = lax.axis_index("sp")
    tp = lax.axis_index("tp")
    rows = lat.shape[0]
    half = rows // 2

    def sp_at(k):
        return {"sp": lax.rem(sp + k, N_SP)}

    def tp_at(k):
        return {"tp": lax.rem(tp + k, N_TP)}

    barrier = pltpu.get_barrier_semaphore()
    for k in range(1, N_SP):
        pl.semaphore_signal(barrier, inc=1, device_id=sp_at(k), device_id_type=MESH)
    for k in range(1, N_TP):
        pl.semaphore_signal(barrier, inc=1, device_id=tp_at(k), device_id_type=MESH)
    pl.semaphore_wait(barrier, N_SP - 1 + N_TP - 1)

    def send(src, dst, s_sem, r_sem, target):
        return pltpu.make_async_remote_copy(
            src_ref=src, dst_ref=dst, send_sem=s_sem, recv_sem=r_sem,
            device_id=target, device_id_type=MESH,
        )

    h0, h1 = pl.ds(0, half), pl.ds(half, half)
    r0 = send(lat.at[h0], xbuf.at[0, h0], x_send.at[0], x_recv.at[0], tp_at(1))
    l1 = send(lat.at[h1], xbuf.at[2, h1], x_send.at[1], x_recv.at[1], tp_at(3))
    r1 = send(lat.at[h1], xbuf.at[0, h1], x_send.at[2], x_recv.at[2], tp_at(1))
    l0 = send(lat.at[h0], xbuf.at[2, h0], x_send.at[3], x_recv.at[3], tp_at(3))
    f0 = send(xbuf.at[0, h0], xbuf.at[1, h0], x_send.at[4], x_recv.at[4], tp_at(1))
    f1 = send(xbuf.at[2, h1], xbuf.at[1, h1], x_send.at[5], x_recv.at[5], tp_at(3))
    r0.start()
    l1.start()

    at = lax.broadcasted_iota(jnp.int32, (16, 128), 0)
    given = jnp.where(
        at == 0,
        jnp.broadcast_to(cond[...].astype(F32), (16, 128)),
        jnp.where(at == 1, jnp.broadcast_to(condc[...].astype(F32), (16, 128)), 0.0),
    )
    active = (given / (1.0 + jnp.exp(-given))).astype(BF16)
    for k, weight in enumerate((m_shift, m_scale, m_gate)):
        product = jnp.dot(active, weight[...], preferred_element_type=F32)
        for r in range(2):
            for c in range(4):
                i = r * 12 + k * 4 + c
                part[i : i + 1, :] = product[r : r + 1, c * 128 : (c + 1) * 128]
    p_copies = [
        send(part, psum_in.at[k - 1], p_send.at[k - 1], p_recv.at[k - 1], sp_at(k))
        for k in range(1, N_SP)
    ]
    for copy in p_copies:
        copy.start()

    wall[:, 0:256] = wq[...]
    wall[:, 256:384] = jnp.concatenate([wk[...], wv[...]], axis=1)
    row_id = lax.broadcasted_iota(jnp.int32, (HD, GRID_W), 0)
    even = lax.rem(row_id, 2) == 0
    for g in range(6):
        grid_row = (sp * 6 + g).astype(F32)
        angle = table[...] * jnp.where(row_id < 32, grid_row, 1.0)
        cosb[g] = jnp.cos(angle)
        sine = jnp.sin(angle)
        sinb[g] = jnp.where(even, -sine, sine)

    for copy in p_copies:
        copy.wait_recv()
    total = part[...]
    for k in range(N_SP - 1):
        total = total + psum_in[k]
    mine[...] = total
    t_copies = [
        send(mine, full.at[tp], t_send.at[k - 1], t_recv.at[k - 1], tp_at(k))
        for k in range(1, N_TP)
    ]
    for copy in t_copies:
        copy.start()
    r1.start()
    l0.start()
    full[tp] = total
    for copy in t_copies:
        copy.wait_recv()

    def vector(r, k):
        pieces = [
            full[t, r * 12 + k * 4 + c : r * 12 + k * 4 + c + 1, :]
            for t in range(N_TP)
            for c in range(4)
        ]
        return jnp.concatenate(pieces, axis=1)

    width = lat.shape[1]
    for r in range(2):
        scaled = gain[...].astype(F32) * (1.0 + vector(r, 1))
        scl[r] = jnp.broadcast_to(scaled, (8, width))
        sft[r] = jnp.broadcast_to(vector(r, 0), (8, width))
    gate_out[...] = vector(0, 2)

    def modulate(src, r, count):
        values = src.astype(F32)
        inverse = lax.rsqrt(jnp.mean(values * values, axis=-1, keepdims=True) + EPS)
        normed = (values * inverse).reshape(count // 8, 8, width)
        return (normed * scl[r][None] + sft[r][None]).reshape(count, width).astype(BF16)

    uc = modulate(ctx[...], 1, ctx.shape[0])
    craw = jnp.dot(uc, wall[:, 256:384], preferred_element_type=F32)
    lane = lax.broadcasted_iota(jnp.int32, craw.shape, 1)
    square = jnp.where(lane < HD, craw * craw, 0.0)
    mean = jnp.sum(square, axis=-1, keepdims=True) * (1.0 / HD)
    keys = craw * lax.rsqrt(mean + EPS) * jnp.concatenate(
        [kg[...].astype(F32).T, jnp.ones((1, HD), F32)], axis=1
    )
    cown[...] = jnp.where(lane < HD, keys, craw).astype(BF16)
    c_copies = [
        send(cown, cbuf.at[k - 1], c_send.at[k - 1], c_recv.at[k - 1], sp_at(k))
        for k in range(1, N_SP)
    ]
    for copy in c_copies:
        copy.start()

    def project(x, owner):
        @pl.loop(0, rows // 32)
        def _(i):
            at_rows = pl.ds(pl.multiple_of(i * 32, 32), 32)
            ubuf[at_rows, :] = modulate(x[at_rows, :], 0, 32)

        raw[pl.ds(pl.multiple_of(owner * rows, rows), rows), :] = jnp.dot(
            ubuf[...], wall[...], preferred_element_type=F32
        )

    project(lat, tp)
    r0.wait_recv()
    f0.start()
    l1.wait_recv()
    f1.start()
    r1.wait_recv()
    project(xbuf.at[0], lax.rem(tp + 3, N_TP))
    l0.wait_recv()
    project(xbuf.at[2], lax.rem(tp + 1, N_TP))
    f0.wait_recv()
    f1.wait_recv()
    project(xbuf.at[1], lax.rem(tp + 2, N_TP))

    def turned(x, gain_column, g):
        square = jnp.sum(x * x, axis=0, keepdims=True) * (1.0 / HD)
        normed = x * lax.rsqrt(square + EPS) * gain_column
        up = pltpu.roll(normed, HD - 1, axis=0)
        down = pltpu.roll(normed, 1, axis=0)
        return normed * cosb[g] + jnp.where(even, up, down) * sinb[g]

    q_gain = qg[...].astype(F32)
    k_gain = kg[...].astype(F32)
    scale = LOG2E * HD ** (-0.5)
    for g in range(6):
        block = raw[g * 128 : (g + 1) * 128, :]
        for pair in range(2):
            side = block[:, pair * 128 : (pair + 1) * 128].T
            for h in range(2):
                q = turned(side[h * HD : (h + 1) * HD], q_gain, g)
                lanes = g * 512 + (pair * 2 + h) * 128
                q_out[:, lanes : lanes + 128] = (q * scale).astype(BF16)
        side = block[:, 256:384].T
        k = turned(side[0:HD], k_gain, g).T
        kv_out[g * 64 : (g + 1) * 64, :] = jnp.concatenate([k[0:64], k[64:128]], axis=1).astype(
            BF16
        )
    for s in range(2):
        order = [(g, p) for p in range(2) for g in (3 * s, 3 * s + 1, 3 * s + 2)]
        for b in range(3):
            pieces = [
                raw[g * 128 + p * 64 : g * 128 + p * 64 + 64, 256:384]
                for g, p in order[2 * b : 2 * b + 2]
            ]
            side = jnp.concatenate(pieces, axis=0).T
            at_row = 384 + (3 * s + b) * 64
            kv_out[at_row : at_row + 64, :] = side[HD : 2 * HD].astype(BF16)

    for copy in c_copies:
        copy.wait_recv()
    ctx_out[0:32, :] = cown[...]
    for k in range(N_SP - 1):
        ctx_out[32 * (k + 1) : 32 * (k + 2), :] = cbuf[k]
    for copy in p_copies + t_copies + c_copies + [r0, l1, r1, l0, f0, f1]:
        copy.wait_send()


def run_project(lat, cond, condc, ctx, gain, ms, mc, mg, wq, wk, wv, qg, kg):
    rows, width = lat.shape
    dma = pltpu.SemaphoreType.DMA
    return pl.pallas_call(
        project_kernel,
        name="project",
        out_shape=(
            jax.ShapeDtypeStruct((HD, 3072), BF16),
            jax.ShapeDtypeStruct((768, 128), BF16),
            jax.ShapeDtypeStruct((512, 128), BF16),
            jax.ShapeDtypeStruct((1, width), F32),
        ),
        in_specs=[VMEM] * 14,
        out_specs=(VMEM,) * 4,
        scratch_shapes=[
            pltpu.VMEM((3, rows, width), BF16),
            pltpu.VMEM((24, 128), F32),
            pltpu.VMEM((N_SP - 1, 24, 128), F32),
            pltpu.VMEM((24, 128), F32),
            pltpu.VMEM((N_TP, 24, 128), F32),
            pltpu.VMEM((width, 384), BF16),
            pltpu.VMEM((rows, width), BF16),
            pltpu.VMEM((768, 384), F32),
            pltpu.VMEM((6, HD, GRID_W), F32),
            pltpu.VMEM((6, HD, GRID_W), F32),
            pltpu.VMEM((2, 8, width), F32),
            pltpu.VMEM((2, 8, width), F32),
            pltpu.VMEM((32, 128), BF16),
            pltpu.VMEM((N_SP - 1, 32, 128), BF16),
            dma((6,)), dma((6,)), dma((15,)), dma((15,)),
            dma((3,)), dma((3,)), dma((15,)), dma((15,)),
        ],
        compiler_params=pltpu.CompilerParams(
            collective_id=0, has_side_effects=True, vmem_limit_bytes=LIMIT
        ),
    )(lat, cond, condc, ctx, gain, ms, mc, mg, wq, wk, wv, qg, kg, jnp.asarray(angle_table()))


SLOTS = [
    (0, 0), (-1, 0), (1, 0), (0, -1), (0, 1), (2, 0), (-1, -1), (-1, 1),
    (1, -1), (1, 1), (0, 2), (2, -1), (2, 1), (-1, 2), (1, 2), (2, 2),
]
SENDS = [
    (0, 1, 1, 0), (0, 2, -1, 0), (0, 3, 0, 1), (0, 4, 0, -1),
    (1, 5, 1, 0), (1, 6, 0, 1), (1, 7, 0, -1),
    (2, 8, 0, 1), (2, 9, 0, -1),
    (3, 10, 0, 1),
    (5, 11, 0, 1), (5, 12, 0, -1),
    (7, 13, 0, -1), (8, 14, 0, 1), (12, 15, 0, -1),
]
TILE = 1024
VROWS = 80


def attend_kernel(
    q_ref, kv_own, ctx, lift, o_out, l_out, kv_all,
    kvbuf, acc, peak, pbuf, send_sem, recv_sem, keep_sem,
):
    sp = lax.axis_index("sp")
    y, z = lax.rem(sp, 4), lax.div(sp, 4)
    tiles = q_ref.shape[1] // TILE

    def near(dy, dz):
        return {"sp": lax.rem(z + dz + 4, 4) * 4 + lax.rem(y + dy + 4, 4)}

    barrier = pltpu.get_barrier_semaphore()
    for dy, dz in ((1, 0), (-1, 0), (0, 1), (0, -1)):
        pl.semaphore_signal(barrier, inc=1, device_id=near(dy, dz), device_id_type=MESH)
    pl.semaphore_wait(barrier, 4)

    sends = []
    for i, (here, there, dy, dz) in enumerate(SENDS):
        sends.append(
            pltpu.make_async_remote_copy(
                src_ref=kv_own if here == 0 else kvbuf.at[here],
                dst_ref=kvbuf.at[there],
                send_sem=send_sem.at[i],
                recv_sem=recv_sem.at[there],
                device_id=near(dy, dz),
                device_id_type=MESH,
            )
        )

    def start_from(slot):
        for copy, (here, _, _, _) in zip(sends, SENDS):
            if here == slot:
                copy.start()

    def arrival(slot):
        return next(copy for copy, (_, there, _, _) in zip(sends, SENDS) if there == slot)

    def keep(slot):
        src = kv_own if slot == 0 else kvbuf.at[slot]
        return pltpu.make_async_copy(src, kv_all.at[slot], keep_sem.at[slot])

    start_from(0)
    keep(0).start()
    kvbuf[0] = kv_own[...]

    lifts = jnp.concatenate([jnp.full((1, 128), lift[h] * LOG2E, F32) for h in range(4)], axis=1)
    lifts = jnp.concatenate([lifts] * (TILE // 512), axis=1)
    ones = jnp.ones((VROWS - HD, 768), BF16)

    def lanes(t):
        if isinstance(t, int):
            return pl.ds(t * TILE, TILE)
        return pl.ds(pl.multiple_of(t * TILE, TILE), TILE)

    cv = ctx[...].astype(F32).T[HD : 2 * HD].astype(BF16)
    cv = jnp.concatenate([cv, ones[:, 0:512]], axis=0)

    for t in range(tiles):
        scores = jnp.dot(ctx[...], tall(q_ref[:, lanes(t)]), preferred_element_type=F32) + lifts
        top = jnp.max(scores, axis=0, keepdims=True)
        peak[:, lanes(t)] = top
        weights = jnp.exp2(scores - top).astype(BF16)
        acc[:, lanes(t)] = jnp.dot(cv, weights, preferred_element_type=F32)

    def score(b, t, slot):
        q = q_ref[:, lanes(t)]
        left = tall(q)
        right = jnp.concatenate([jnp.zeros_like(q), q], axis=0)
        top = peak[:, lanes(t)]
        for s in range(2):
            k = kvbuf[b, pl.ds(s * 192, 192), :]
            for p, query in enumerate((left, right)):
                x = jnp.dot(k, query, preferred_element_type=F32)
                pbuf[slot, pl.ds(s * 384 + p * 192, 192), :] = jnp.exp2(x - top).astype(BF16)

    def value(b, t, slot):
        v = [kvbuf[b, pl.ds(384 + g * 64, 64), :] for g in range(6)]
        v = jnp.concatenate([jnp.concatenate(v, axis=1), ones], axis=0)
        acc[:, lanes(t)] += jnp.dot(v, pbuf[slot], preferred_element_type=F32)

    score(0, 0, 0)

    def step(b, carry):
        for t in range(tiles - 1):
            value(b, t, t % 2)
            score(b, t + 1, (t + 1) % 2)
        for slot in range(1, N_SP):

            @pl.when(b == slot - 1)
            def _(slot=slot):
                arrival(slot).wait_recv()
                start_from(slot)
                keep(slot).start()

        last = tiles - 1
        value(b, last, last % 2)
        score(jnp.minimum(b + 1, N_SP - 1), 0, 0)
        return carry

    lax.fori_loop(0, N_SP, step, 0)

    l_out[...] = acc[HD : HD + 8, :]
    for g in range(6):
        at_lanes = pl.ds(g * 512, 512)
        mean = acc[0:HD, at_lanes] / acc[HD : HD + 1, at_lanes]
        stack = jnp.concatenate([mean[:, h * 128 : (h + 1) * 128] for h in range(4)], axis=0)
        o_out[g * 128 : (g + 1) * 128, :] = stack.T.astype(BF16)
    for copy in sends:
        copy.wait_send()
    for slot in range(N_SP):
        keep(slot).wait()


def run_attend(q, kv, ctx, lift):
    dma = pltpu.SemaphoreType.DMA
    return pl.pallas_call(
        attend_kernel,
        name="attend",
        out_shape=(
            jax.ShapeDtypeStruct((768, 256), BF16),
            jax.ShapeDtypeStruct((8, 3072), F32),
            jax.ShapeDtypeStruct((N_SP, 768, 128), BF16),
        ),
        in_specs=[VMEM, VMEM, VMEM, SMEM],
        out_specs=(VMEM, VMEM, ANY),
        scratch_shapes=[
            pltpu.VMEM((N_SP, 768, 128), BF16),
            pltpu.VMEM((VROWS, 3072), F32),
            pltpu.VMEM((1, 3072), F32),
            pltpu.VMEM((2, 768, TILE), BF16),
            dma((len(SENDS),)),
            dma((N_SP,)),
            dma((N_SP,)),
        ],
        compiler_params=pltpu.CompilerParams(
            collective_id=1, has_side_effects=True, vmem_limit_bytes=LIMIT
        ),
    )(q, kv, ctx, lift)


def repair_kernel(
    l_ref, o_in, q_hbm, kv_hbm, ctx_hbm, lift, o_out,
    q_ref, kvbuf, ctx, acc, peak, o_buf, sem,
):
    safe = jnp.all(l_ref[...] < 2.0**100)

    @pl.when(jnp.logical_not(safe))
    def _():
        for src, dst in ((q_hbm, q_ref), (kv_hbm, kvbuf), (ctx_hbm, ctx)):
            copy = pltpu.make_async_copy(src, dst, sem)
            copy.start()
            copy.wait()
        wide = 512
        ones = jnp.ones((VROWS - HD, 768), BF16)
        lifts = jnp.concatenate(
            [jnp.full((1, 128), lift[h] * LOG2E, F32) for h in range(4)], axis=1
        )
        cv = ctx[...].astype(F32).T[HD : 2 * HD].astype(BF16)
        cv = jnp.concatenate([cv, ones[:, 0:512]], axis=0)

        @pl.loop(0, q_ref.shape[1] // wide)
        def _(t):
            lanes = pl.ds(pl.multiple_of(t * wide, wide), wide)
            q = q_ref[:, lanes]
            left = tall(q)
            right = jnp.concatenate([jnp.zeros_like(q), q], axis=0)
            scores = jnp.dot(ctx[...], left, preferred_element_type=F32) + lifts
            top = jnp.max(scores, axis=0, keepdims=True)
            peak[...] = top
            weights = jnp.exp2(scores - top).astype(BF16)
            acc[...] = jnp.dot(cv, weights, preferred_element_type=F32)

            @pl.loop(0, N_SP)
            def _(b):
                parts = []
                for s in range(2):
                    k = kvbuf[b, pl.ds(s * 192, 192), :]
                    for query in (left, right):
                        parts.append(jnp.dot(k, query, preferred_element_type=F32))
                x = jnp.concatenate(parts, axis=0)
                old = peak[...]
                new = jnp.maximum(old, jnp.max(x, axis=0, keepdims=True))
                peak[...] = new
                v = [kvbuf[b, pl.ds(384 + g * 64, 64), :] for g in range(6)]
                v = jnp.concatenate([jnp.concatenate(v, axis=1), ones], axis=0)
                weights = jnp.exp2(x - new).astype(BF16)
                acc[...] = acc[...] * jnp.exp2(old - new) + jnp.dot(
                    v, weights, preferred_element_type=F32
                )

            mean = acc[0:HD, :] / acc[HD : HD + 1, :]
            stack = jnp.concatenate([mean[:, h * 128 : (h + 1) * 128] for h in range(4)], axis=0)
            o_buf[...] = stack.T.astype(BF16)
            rows = pl.ds(pl.multiple_of(t * 128, 128), 128)
            copy = pltpu.make_async_copy(o_buf, o_out.at[rows], sem)
            copy.start()
            copy.wait()


def run_repair(l, o, q, kv_all, ctx, lift):
    return pl.pallas_call(
        repair_kernel,
        name="repair",
        out_shape=jax.ShapeDtypeStruct(o.shape, o.dtype),
        in_specs=[VMEM, ANY, ANY, ANY, ANY, SMEM],
        out_specs=ANY,
        input_output_aliases={1: 0},
        scratch_shapes=[
            pltpu.VMEM((HD, 3072), BF16),
            pltpu.VMEM((N_SP, 768, 128), BF16),
            pltpu.VMEM((512, 128), BF16),
            pltpu.VMEM((VROWS, 512), F32),
            pltpu.VMEM((1, 512), F32),
            pltpu.VMEM((128, 256), BF16),
            pltpu.SemaphoreType.DMA(()),
        ],
        compiler_params=pltpu.CompilerParams(vmem_limit_bytes=LIMIT),
    )(l, o, q, kv_all, ctx, lift)


def output_kernel(
    o_ref, w_hbm, lat, gate, out,
    wbuf, obuf, send_sem, recv_sem, w_sem,
):
    tp = lax.axis_index("tp")
    rows = lat.shape[0]

    def tp_at(k):
        return lax.rem(tp + k, N_TP)

    load = pltpu.make_async_copy(w_hbm, wbuf, w_sem)
    load.start()
    barrier = pltpu.get_barrier_semaphore()
    for k in range(1, N_TP):
        pl.semaphore_signal(barrier, inc=1, device_id={"tp": tp_at(k)}, device_id_type=MESH)
    pl.semaphore_wait(barrier, N_TP - 1)
    copies = []
    for k in range(1, N_TP):
        theirs = pl.ds(pl.multiple_of(tp_at(k) * rows, rows), rows)
        copies.append(
            pltpu.make_async_remote_copy(
                src_ref=o_ref.at[theirs], dst_ref=obuf.at[tp],
                send_sem=send_sem.at[k - 1], recv_sem=recv_sem.at[k - 1],
                device_id={"tp": tp_at(k)}, device_id_type=MESH,
            )
        )
        copies[-1].start()
    obuf[tp] = o_ref[pl.ds(pl.multiple_of(tp * rows, rows), rows), :]
    load.wait()
    for copy in copies:
        copy.wait_recv()
    wide = 512
    for n in range(out.shape[1] // wide):
        cols = slice(n * wide, (n + 1) * wide)
        total = None
        for t in range(N_TP):
            term = jnp.dot(
                obuf[t], wbuf[t * 256 : (t + 1) * 256, cols], preferred_element_type=F32
            )
            total = term if total is None else total + term
        out[:, cols] = (lat[:, cols].astype(F32) + gate[:, cols] * total).astype(BF16)
    for copy in copies:
        copy.wait_send()


def run_output(o, w_out, lat, gate):
    rows, width = lat.shape
    dma = pltpu.SemaphoreType.DMA
    return pl.pallas_call(
        output_kernel,
        name="output",
        out_shape=jax.ShapeDtypeStruct((rows, width), BF16),
        in_specs=[VMEM, ANY, VMEM, VMEM],
        out_specs=VMEM,
        scratch_shapes=[
            pltpu.VMEM(w_out.shape, BF16),
            pltpu.VMEM((N_TP, rows, 256), BF16),
            dma((N_TP - 1,)),
            dma((N_TP - 1,)),
            dma(()),
        ],
        compiler_params=pltpu.CompilerParams(
            collective_id=2, has_side_effects=True, vmem_limit_bytes=LIMIT
        ),
    )(o, w_out, lat, gate)


def on_device(
    latent, cond, cond_ctx, context, norm_gain, mod_shift, mod_scale, mod_gate,
    w_query, w_key, w_value, q_gain, k_gain, ctx_lift, w_out,
):
    lat = latent[0]
    q, kv, ctx, gate = run_project(
        lat, cond, cond_ctx[None, :], context[0], norm_gain[None, :],
        mod_shift, mod_scale, mod_gate, w_query, w_key, w_value,
        q_gain[:, None], k_gain[:, None],
    )
    o, l, kv_all = run_attend(q, kv, ctx, ctx_lift)
    o = run_repair(l, o, q, kv_all, ctx, ctx_lift)
    return run_output(o, w_out, lat, gate)[None]


def solution(mesh):
    in_specs = (
        P("dp", ("sp", "tp"), None),
        P("dp", "sp"),
        P("sp"),
        P("dp", "sp", None),
        P(),
        P("sp", "tp"),
        P("sp", "tp"),
        P("sp", "tp"),
        P(None, "tp"),
        P(None, "tp"),
        P(None, "tp"),
        P(),
        P(),
        P("tp"),
        P(),
    )
    return jax.shard_map(
        on_device, mesh=mesh, in_specs=in_specs,
        out_specs=P("dp", ("sp", "tp"), None), check_vma=False,
    )
```

```python
import functools

import jax
import jax.numpy as jnp
import numpy as np
from jax import lax
from jax.experimental import pallas as pl
from jax.experimental.pallas import tpu as pltpu
from jax.sharding import PartitionSpec as P

MESH = pl.DeviceIdType.MESH
HD = 64
GRID_W = 128
EPS = 1e-06
THETA = 10000.0
LOG2E = 1.4426950408889634
N_SP = 16
N_TP = 4
F32 = jnp.float32
BF16 = jnp.bfloat16
VMEM = pl.BlockSpec(memory_space=pltpu.VMEM)
ANY = pl.BlockSpec(memory_space=pl.ANY)
SMEM = pl.BlockSpec(memory_space=pltpu.SMEM)
LIMIT = 60 * 2**20


def angle_table():
    i = (np.arange(HD) // 2) % 16
    f = (THETA ** (-(i.astype(np.float32)) / np.float32(16))).astype(np.float32)
    return np.repeat(f[:, None], GRID_W, axis=1)


def tall(x):
    return jnp.concatenate([x, jnp.zeros_like(x)], axis=0)


SENDS = [
    (0, 1, 1, 0), (0, 2, -1, 0), (0, 3, 0, 1), (0, 4, 0, -1),
    (1, 5, 1, 0), (1, 6, 0, 1), (1, 7, 0, -1),
    (2, 8, 0, 1), (2, 9, 0, -1),
    (3, 10, 0, 1),
    (5, 11, 0, 1), (5, 12, 0, -1),
    (7, 13, 0, -1), (8, 14, 0, 1), (12, 15, 0, -1),
]
TILE = 1536
VROWS = 80
FIRST = 5
UNITS = 32


def attention_kernel(
    lat, cond, condc, ctx, gain, m_shift, m_scale, m_gate, wq, wk, wv, qg, kg, table, lift,
    o_out, l_out, q_out, kv_all, ctx_out, gate_out,
    xbuf, part, psum_in, mine, full, wall, ubuf, raw, cosb, sinb, scl, sft, cbuf,
    kvbuf, acc, peak, pbuf,
    x_send, x_recv, p_send, p_recv, t_send, t_recv, c_send, c_recv, kv_send, kv_recv, keep_sem,
):
    sp = lax.axis_index("sp")
    tp = lax.axis_index("tp")
    y, z = lax.rem(sp, 4), lax.div(sp, 4)
    rows, width = lat.shape
    half = rows // 2

    def sp_at(k):
        return {"sp": lax.rem(sp + k, N_SP)}

    def tp_at(k):
        return {"tp": lax.rem(tp + k, N_TP)}

    def near(dy, dz):
        return {"sp": lax.rem(z + dz + 4, 4) * 4 + lax.rem(y + dy + 4, 4)}

    barrier = pltpu.get_barrier_semaphore()
    for k in range(1, N_SP):
        pl.semaphore_signal(barrier, inc=1, device_id=sp_at(k), device_id_type=MESH)
    for k in range(1, N_TP):
        pl.semaphore_signal(barrier, inc=1, device_id=tp_at(k), device_id_type=MESH)
    pl.semaphore_wait(barrier, N_SP - 1 + N_TP - 1)

    def send(src, dst, s_sem, r_sem, target):
        return pltpu.make_async_remote_copy(
            src_ref=src, dst_ref=dst, send_sem=s_sem, recv_sem=r_sem,
            device_id=target, device_id_type=MESH,
        )

    def x_copy(i, src, to_row, count, k):
        return send(src, xbuf.at[pl.ds(to_row, count)], x_send.at[i], x_recv.at[i], tp_at(k))

    ra = x_copy(0, lat.at[pl.ds(0, 64)], 0, 64, 1)
    la = x_copy(1, lat.at[pl.ds(half, 64)], 96, 64, 3)
    rb = x_copy(2, lat.at[pl.ds(64, 32)], 64, 32, 1)
    lb = x_copy(3, lat.at[pl.ds(half + 64, 32)], 160, 32, 3)
    rc = x_copy(4, lat.at[pl.ds(half, half)], 192, half, 1)
    lc = x_copy(5, lat.at[pl.ds(0, half)], 288, half, 3)
    rf = x_copy(6, xbuf.at[pl.ds(0, half)], 384, half, 1)
    lf = x_copy(7, xbuf.at[pl.ds(half, half)], 480, half, 3)
    x_copies = [ra, la, rb, lb, rc, lc, rf, lf]
    ra.start()
    la.start()

    at = lax.broadcasted_iota(jnp.int32, (16, 128), 0)
    given = jnp.where(
        at == 0,
        jnp.broadcast_to(cond[...].astype(F32), (16, 128)),
        jnp.where(at == 1, jnp.broadcast_to(condc[...].astype(F32), (16, 128)), 0.0),
    )
    active = (given / (1.0 + jnp.exp(-given))).astype(BF16)
    for k, weight in enumerate((m_shift, m_scale, m_gate)):
        product = jnp.dot(active, weight[...], preferred_element_type=F32)
        for r in range(2):
            for c in range(4):
                i = r * 12 + k * 4 + c
                part[i : i + 1, :] = product[r : r + 1, c * 128 : (c + 1) * 128]
    p_copies = [
        send(part, psum_in.at[k - 1], p_send.at[k - 1], p_recv.at[k - 1], sp_at(k))
        for k in range(1, N_SP)
    ]
    for copy in p_copies:
        copy.start()

    wall[:, 0:256] = wq[...]
    wall[:, 256:384] = jnp.concatenate([wk[...], wv[...]], axis=0).T

    for copy in p_copies:
        copy.wait_recv()
    total = part[...]
    for k in range(N_SP - 1):
        total = total + psum_in[k]
    mine[...] = total
    full[tp] = total
    t_copies = [
        send(mine, full.at[tp], t_send.at[k - 1], t_recv.at[k - 1], tp_at(k))
        for k in range(1, N_TP)
    ]
    for copy in t_copies:
        copy.start()
    for copy in (rb, lb, rc, lc):
        copy.start()

    row_id = lax.broadcasted_iota(jnp.int32, (HD, GRID_W), 0)
    lane_id = lax.broadcasted_iota(jnp.int32, (HD, GRID_W), 1)
    even = lax.rem(row_id, 2) == 0
    left, right, opposite = (lax.rem(tp + k, N_TP) * rows for k in (3, 1, 2))
    for g in range(6):
        n = lane_id + g * 128
        shift = jnp.where(
            n < 192,
            tp * rows,
            jnp.where(
                n < 288,
                left - 192,
                jnp.where(
                    n < 384,
                    right - 192,
                    jnp.where(
                        n < 480,
                        left - 288,
                        jnp.where(n < 576, right - 480, opposite - 576),
                    ),
                ),
            ),
        )
        at_token = n + shift + sp * 768
        grid_at = jnp.where(row_id < 32, at_token >> 7, at_token & 127)
        angle = table[...] * grid_at.astype(F32)
        cosb[g] = jnp.cos(angle)
        sine = jnp.sin(angle)
        sinb[g] = jnp.where(even, -sine, sine)

    for copy in t_copies:
        copy.wait_recv()

    def vector(r, k):
        pieces = [
            full[t, r * 12 + k * 4 + c : r * 12 + k * 4 + c + 1, :]
            for t in range(N_TP)
            for c in range(4)
        ]
        return jnp.concatenate(pieces, axis=1)

    gains = gain[...].astype(F32)
    gains = jnp.concatenate([gains[i : i + 1, :] for i in range(width // 128)], axis=1)
    for r in range(2):
        scl[r] = jnp.broadcast_to(gains * (1.0 + vector(r, 1)), (8, width))
        sft[r] = jnp.broadcast_to(vector(r, 0), (8, width))
    gate_out[...] = vector(0, 2)

    def modulate(src, r, count):
        values = src.astype(F32)
        inverse = lax.rsqrt(jnp.mean(values * values, axis=-1, keepdims=True) + EPS)
        normed = (values * inverse).reshape(count // 8, 8, width)
        return (normed * scl[r][None] + sft[r][None]).reshape(count, width).astype(BF16)

    uc = modulate(ctx[...], 1, ctx.shape[0])
    craw = jnp.dot(uc, wall[:, 256:384], preferred_element_type=F32)
    lane = lax.broadcasted_iota(jnp.int32, craw.shape, 1)
    square = jnp.where(lane < HD, craw * craw, 0.0)
    mean = jnp.sum(square, axis=-1, keepdims=True) * (1.0 / HD)
    k_row = kg[...].astype(F32)
    keys = craw * lax.rsqrt(mean + EPS) * jnp.concatenate([k_row, jnp.ones((1, HD), F32)], axis=1)
    cbuf[pl.ds(0, 32), :] = jnp.where(lane < HD, keys, craw).astype(BF16)

    def project(x, first, to_row):
        @pl.loop(0, rows // 32)
        def _(i):
            at_rows = pl.ds(pl.multiple_of(i * 32, 32), 32)
            from_rows = pl.ds(pl.multiple_of(first + i * 32, 32), 32)
            ubuf[at_rows, :] = modulate(x[from_rows, :], 0, 32)

        raw[pl.ds(to_row, rows), :] = jnp.dot(ubuf[...], wall[...], preferred_element_type=F32)

    def column(ref):
        r = lax.broadcasted_iota(jnp.int32, (HD, HD), 0)
        c = lax.broadcasted_iota(jnp.int32, (HD, HD), 1)
        spread = jnp.broadcast_to(ref[...].astype(F32), (HD, HD))
        return jnp.sum(jnp.where(r == c, spread, 0.0), axis=1, keepdims=True)

    q_gain = column(qg)
    k_gain = column(kg)

    def turned(x, gain_column, g):
        square = jnp.sum(x * x, axis=0, keepdims=True) * (1.0 / HD)
        normed = x * lax.rsqrt(square + EPS) * gain_column
        up = pltpu.roll(normed, HD - 1, axis=0)
        down = pltpu.roll(normed, 1, axis=0)
        return normed * cosb[g] + jnp.where(even, up, down) * sinb[g]

    scale = LOG2E * HD ** (-0.5)

    def finish_kv(s):
        slot = s * N_SP
        for i in range(3):
            g = 3 * s + i
            side = raw[g * 128 : (g + 1) * 128, 256:384].T
            k = turned(side[0:HD], k_gain, g).T
            kvbuf[slot, i * 64 : (i + 1) * 64, :] = jnp.concatenate(
                [k[0:64], k[64:128]], axis=1
            ).astype(BF16)
        order = [(g, p) for p in range(2) for g in (3 * s, 3 * s + 1, 3 * s + 2)]
        for b in range(3):
            pieces = [
                raw[g * 128 + p * 64 : g * 128 + p * 64 + 64, 256:384]
                for g, p in order[2 * b : 2 * b + 2]
            ]
            side = jnp.concatenate(pieces, axis=0).T
            at_row = 192 + b * 64
            kvbuf[slot, at_row : at_row + 64, :] = side[HD : 2 * HD].astype(BF16)

    def finish_q(s):
        for g in range(3 * s, 3 * s + 3):
            block = raw[g * 128 : (g + 1) * 128, :]
            for pair in range(2):
                side = block[:, pair * 128 : (pair + 1) * 128].T
                for h in range(2):
                    q = turned(side[h * HD : (h + 1) * HD], q_gain, g)
                    at_lane = g * 512 + (pair * 2 + h) * 128
                    q_out[:, at_lane : at_lane + 128] = (q * scale).astype(BF16)

    kv_copies = [[], []]
    for s in range(2):
        for i, (here, there, dy, dz) in enumerate(SENDS):
            here, there = here + s * N_SP, there + s * N_SP
            kv_copies[s].append(
                send(
                    kvbuf.at[here], kvbuf.at[there],
                    kv_send.at[i + s * len(SENDS)], kv_recv.at[there], near(dy, dz),
                )
            )

    def start_from(s, slot):
        for copy, (here, _, _, _) in zip(kv_copies[s], SENDS):
            if here == slot:
                copy.start()

    def keep(s, slot):
        slot = slot + s * N_SP
        return pltpu.make_async_copy(kvbuf.at[slot], kv_all.at[slot], keep_sem.at[slot])

    def arrive(s, slot):
        if slot > 0:
            next(
                copy for copy, (_, there, _, _) in zip(kv_copies[s], SENDS) if there == slot
            ).wait_recv()
        start_from(s, slot)
        keep(s, slot).start()

    lifts = jnp.concatenate([jnp.full((1, 128), lift[h] * LOG2E, F32) for h in range(4)], axis=1)
    lifts = jnp.concatenate([lifts] * (TILE // 512), axis=1)
    ones = jnp.ones((VROWS - HD, 768), BF16)

    def lanes(t):
        if isinstance(t, int):
            return pl.ds(t * TILE, TILE)
        return pl.ds(pl.multiple_of(t * TILE, TILE), TILE)

    def context(t):
        cv = cbuf[...].astype(F32).T[HD : 2 * HD].astype(BF16)
        cv = jnp.concatenate([cv, ones[:, 0:512]], axis=0)
        scores = jnp.dot(cbuf[...], tall(q_out[:, lanes(t)]), preferred_element_type=F32) + lifts
        top = jnp.max(scores, axis=0, keepdims=True)
        peak[:, lanes(t)] = top
        weights = jnp.exp2(scores - top).astype(BF16)
        acc[:, lanes(t)] = jnp.dot(cv, weights, preferred_element_type=F32)

    def score(pair, t, slot):
        q = q_out[:, lanes(t)]
        lower = tall(q)
        upper = jnp.concatenate([jnp.zeros_like(q), q], axis=0)
        top = peak[:, lanes(t)]
        for s in range(2):
            k = kvbuf[pair * 2 + s, pl.ds(0, 192), :]
            for p, query in enumerate((lower, upper)):
                x = jnp.dot(k, query, preferred_element_type=F32)
                pbuf[slot, pl.ds(s * 384 + p * 192, 192), :] = jnp.exp2(x - top).astype(BF16)

    def value(pair, t, slot):
        v = [kvbuf[pair * 2 + s, pl.ds(192 + i * 64, 64), :] for s in range(2) for i in range(3)]
        v = jnp.concatenate([jnp.concatenate(v, axis=1), ones], axis=0)
        acc[:, lanes(t)] += jnp.dot(v, pbuf[slot], preferred_element_type=F32)

    def unit(j):
        pair = jnp.where(
            j < 10, j - FIRST, jnp.where(j < 16, 5 + (j - 10) // 2, jnp.where(j < 24, j - 8, j - 16))
        )
        tile = jnp.where(
            j < 10, 1, jnp.where(j < 16, lax.rem(j, 2), jnp.where(j < 24, 0, 1))
        )
        return pair, tile

    project(lat, 0, 0)
    c_copies = [
        send(
            cbuf.at[pl.ds(0, 32)], cbuf.at[pl.ds(32 * k, 32)],
            c_send.at[k - 1], c_recv.at[k - 1], sp_at(k),
        )
        for k in range(1, N_SP)
    ]
    for copy in c_copies:
        copy.start()
    ra.wait_recv()
    rb.wait_recv()
    rf.start()
    la.wait_recv()
    lb.wait_recv()
    lf.start()
    project(xbuf, 0, 192)
    finish_kv(0)
    finish_q(0)
    arrive(0, 0)
    for copy in c_copies:
        copy.wait_recv()
    context(0)
    arrive(0, 1)
    score(0, 0, 0)

    def first_step(j, carry):
        for pair in range(1, FIRST):

            @pl.when(j == pair - 1)
            def _(pair=pair):
                arrive(0, 2 * pair)
                arrive(0, 2 * pair + 1)

        slot = lax.rem(j, 2)
        value(j, 0, slot)
        score(j + 1, 0, 1 - slot)
        return carry

    lax.fori_loop(0, FIRST - 1, first_step, 0)
    value(FIRST - 1, 0, (FIRST - 1) % 2)

    rc.wait_recv()
    lc.wait_recv()
    project(xbuf, 192, 384)
    rf.wait_recv()
    lf.wait_recv()
    project(xbuf, 384, 576)
    finish_kv(1)
    finish_q(1)
    arrive(1, 0)
    context(1)
    score(0, 1, FIRST % 2)

    events = {5: (0, 5), 6: (0, 6), 7: (0, 7)}
    for pair, j in enumerate((9, 10, 11, 12, 13, 14, 16, 18)):
        events[j] = (1, pair)

    def second_step(j, carry):
        for when, (s, pair) in events.items():

            @pl.when(j == when)
            def _(s=s, pair=pair):
                for slot in (2 * pair, 2 * pair + 1):
                    if slot > 0:
                        arrive(s, slot)

        slot = lax.rem(j, 2)
        value(*unit(j), slot)
        score(*unit(j + 1), 1 - slot)
        return carry

    lax.fori_loop(FIRST, UNITS - 1, second_step, 0)
    value(15, 1, (UNITS - 1) % 2)

    l_out[...] = acc[HD : HD + 8, :]
    for g in range(6):
        at_lanes = pl.ds(g * 512, 512)
        mean = acc[0:HD, at_lanes] / acc[HD : HD + 1, at_lanes]
        stack = jnp.concatenate([mean[:, h * 128 : (h + 1) * 128] for h in range(4)], axis=0)
        o_out[g * 128 : (g + 1) * 128, :] = stack.T.astype(BF16)
    ctx_out[...] = cbuf[...]
    for copy in x_copies + p_copies + t_copies + c_copies + kv_copies[0] + kv_copies[1]:
        copy.wait_send()
    for s in range(2):
        for slot in range(N_SP):
            keep(s, slot).wait()


def run_attention(lat, cond, condc, ctx, gain, ms, mc, mg, wq, wk, wv, qg, kg, lift):
    rows, width = lat.shape
    dma = pltpu.SemaphoreType.DMA
    return pl.pallas_call(
        attention_kernel,
        name="attention",
        out_shape=(
            jax.ShapeDtypeStruct((768, 256), BF16),
            jax.ShapeDtypeStruct((8, 3072), F32),
            jax.ShapeDtypeStruct((HD, 3072), BF16),
            jax.ShapeDtypeStruct((2 * N_SP, 384, 128), BF16),
            jax.ShapeDtypeStruct((512, 128), BF16),
            jax.ShapeDtypeStruct((1, width), F32),
        ),
        in_specs=[VMEM] * 14 + [SMEM],
        out_specs=(VMEM, VMEM, VMEM, ANY, VMEM, VMEM),
        scratch_shapes=[
            pltpu.VMEM((3 * rows, width), BF16),
            pltpu.VMEM((24, 128), F32),
            pltpu.VMEM((N_SP - 1, 24, 128), F32),
            pltpu.VMEM((24, 128), F32),
            pltpu.VMEM((N_TP, 24, 128), F32),
            pltpu.VMEM((width, 384), BF16),
            pltpu.VMEM((rows, width), BF16),
            pltpu.VMEM((768, 384), F32),
            pltpu.VMEM((6, HD, GRID_W), F32),
            pltpu.VMEM((6, HD, GRID_W), F32),
            pltpu.VMEM((2, 8, width), F32),
            pltpu.VMEM((2, 8, width), F32),
            pltpu.VMEM((512, 128), BF16),
            pltpu.VMEM((2 * N_SP, 384, 128), BF16),
            pltpu.VMEM((VROWS, 3072), F32),
            pltpu.VMEM((1, 3072), F32),
            pltpu.VMEM((2, 768, TILE), BF16),
            dma((8,)), dma((8,)), dma((15,)), dma((15,)),
            dma((3,)), dma((3,)), dma((15,)), dma((15,)),
            dma((2 * len(SENDS),)), dma((2 * N_SP,)), dma((2 * N_SP,)),
        ],
        compiler_params=pltpu.CompilerParams(
            collective_id=0, has_side_effects=True, vmem_limit_bytes=LIMIT
        ),
    )(
        lat, cond, condc, ctx, gain, ms, mc, mg, wq, wk, wv, qg, kg,
        jnp.asarray(angle_table()), lift,
    )


def repair_kernel(
    l_ref, o_in, q_hbm, kv_hbm, ctx_hbm, lift, o_out,
    q_ref, kvbuf, ctx, acc, peak, o_buf, sem,
):
    safe = jnp.all(l_ref[...] < 2.0**100)

    @pl.when(jnp.logical_not(safe))
    def _():
        for src, dst in ((q_hbm, q_ref), (kv_hbm, kvbuf), (ctx_hbm, ctx)):
            copy = pltpu.make_async_copy(src, dst, sem)
            copy.start()
            copy.wait()
        wide = 512
        ones = jnp.ones((VROWS - HD, 768), BF16)
        lifts = jnp.concatenate(
            [jnp.full((1, 128), lift[h] * LOG2E, F32) for h in range(4)], axis=1
        )
        cv = ctx[...].astype(F32).T[HD : 2 * HD].astype(BF16)
        cv = jnp.concatenate([cv, ones[:, 0:512]], axis=0)

        @pl.loop(0, q_ref.shape[1] // wide)
        def _(t):
            lanes = pl.ds(pl.multiple_of(t * wide, wide), wide)
            q = q_ref[:, lanes]
            left = tall(q)
            right = jnp.concatenate([jnp.zeros_like(q), q], axis=0)
            scores = jnp.dot(ctx[...], left, preferred_element_type=F32) + lifts
            top = jnp.max(scores, axis=0, keepdims=True)
            peak[...] = top
            weights = jnp.exp2(scores - top).astype(BF16)
            acc[...] = jnp.dot(cv, weights, preferred_element_type=F32)

            @pl.loop(0, N_SP)
            def _(b):
                parts = []
                for s in range(2):
                    k = kvbuf[b * 2 + s, pl.ds(0, 192), :]
                    for query in (left, right):
                        parts.append(jnp.dot(k, query, preferred_element_type=F32))
                x = jnp.concatenate(parts, axis=0)
                old = peak[...]
                new = jnp.maximum(old, jnp.max(x, axis=0, keepdims=True))
                peak[...] = new
                v = [
                    kvbuf[b * 2 + s, pl.ds(192 + i * 64, 64), :] for s in range(2) for i in range(3)
                ]
                v = jnp.concatenate([jnp.concatenate(v, axis=1), ones], axis=0)
                weights = jnp.exp2(x - new).astype(BF16)
                acc[...] = acc[...] * jnp.exp2(old - new) + jnp.dot(
                    v, weights, preferred_element_type=F32
                )

            mean = acc[0:HD, :] / acc[HD : HD + 1, :]
            stack = jnp.concatenate([mean[:, h * 128 : (h + 1) * 128] for h in range(4)], axis=0)
            o_buf[...] = stack.T.astype(BF16)
            rows = pl.ds(pl.multiple_of(t * 128, 128), 128)
            copy = pltpu.make_async_copy(o_buf, o_out.at[rows], sem)
            copy.start()
            copy.wait()


def run_repair(l, o, q, kv_all, ctx, lift):
    return pl.pallas_call(
        repair_kernel,
        name="repair",
        out_shape=jax.ShapeDtypeStruct(o.shape, o.dtype),
        in_specs=[VMEM, ANY, ANY, ANY, ANY, SMEM],
        out_specs=ANY,
        input_output_aliases={1: 0},
        scratch_shapes=[
            pltpu.VMEM((HD, 3072), BF16),
            pltpu.VMEM((2 * N_SP, 384, 128), BF16),
            pltpu.VMEM((512, 128), BF16),
            pltpu.VMEM((VROWS, 512), F32),
            pltpu.VMEM((1, 512), F32),
            pltpu.VMEM((128, 256), BF16),
            pltpu.SemaphoreType.DMA(()),
        ],
        compiler_params=pltpu.CompilerParams(vmem_limit_bytes=LIMIT),
    )(l, o, q, kv_all, ctx, lift)


def exchange_kernel(o_ref, out, obuf, send_sem, recv_sem):
    tp = lax.axis_index("tp")
    rows = o_ref.shape[0] // N_TP
    half = rows // 2

    def tp_at(k):
        return {"tp": lax.rem(tp + k, N_TP)}

    barrier = pltpu.get_barrier_semaphore()
    for k in range(1, N_TP):
        pl.semaphore_signal(barrier, inc=1, device_id=tp_at(k), device_id_type=MESH)
    pl.semaphore_wait(barrier, N_TP - 1)
    plan = [(2, 576, 0, rows), (3, 192, 0, half), (1, 288, half, half), (3, 384, half, half),
            (1, 480, 0, half)]
    copies = []
    for i, (k, here, there, count) in enumerate(plan):
        copies.append(
            pltpu.make_async_remote_copy(
                src_ref=o_ref.at[pl.ds(here, count)],
                dst_ref=obuf.at[tp, pl.ds(there, count)],
                send_sem=send_sem.at[i], recv_sem=recv_sem.at[i],
                device_id=tp_at(k), device_id_type=MESH,
            )
        )
        copies[-1].start()
    out[tp] = o_ref[0:rows, :]
    for copy in copies:
        copy.wait_recv()
    for k in range(1, N_TP):
        source = lax.rem(tp + k, N_TP)
        out[source] = obuf[source]
    for copy in copies:
        copy.wait_send()


def run_exchange(o):
    rows = o.shape[0] // N_TP
    dma = pltpu.SemaphoreType.DMA
    return pl.pallas_call(
        exchange_kernel,
        name="exchange",
        out_shape=jax.ShapeDtypeStruct((N_TP, rows, 256), BF16),
        in_specs=[VMEM],
        out_specs=VMEM,
        scratch_shapes=[pltpu.VMEM((N_TP, rows, 256), BF16), dma((5,)), dma((5,))],
        compiler_params=pltpu.CompilerParams(collective_id=2, has_side_effects=True),
    )(o)


def output_kernel(o_ref, w, lat, gate, out):
    total = None
    for t in range(N_TP):
        term = jnp.dot(o_ref[t], w[t * 256 : (t + 1) * 256, :], preferred_element_type=F32)
        total = term if total is None else total + term
    out[...] = (lat[...].astype(F32) + gate[...] * total).astype(BF16)


def run_output(o, w_out, lat, gate):
    rows, width = lat.shape
    wide = 512
    return pl.pallas_call(
        output_kernel,
        name="output",
        grid=(width // wide,),
        out_shape=jax.ShapeDtypeStruct((rows, width), BF16),
        in_specs=[
            pl.BlockSpec((N_TP, rows, 256), lambda n: (0, 0, 0)),
            pl.BlockSpec((w_out.shape[0], wide), lambda n: (0, n)),
            pl.BlockSpec((rows, wide), lambda n: (0, n)),
            pl.BlockSpec((1, wide), lambda n: (0, n)),
        ],
        out_specs=pl.BlockSpec((rows, wide), lambda n: (0, n)),
    )(o, w_out, lat, gate)


def on_device(
    latent, cond, cond_ctx, context, norm_gain, mod_shift, mod_scale, mod_gate,
    w_query, w_key, w_value, q_gain, k_gain, ctx_lift, w_out,
):
    lat = latent[0]
    o, l, q, kv_all, ctx, gate = run_attention(
        lat, cond, cond_ctx[None, :], context[0], norm_gain.reshape(-1, 128),
        mod_shift, mod_scale, mod_gate, w_query, w_key.T, w_value.T,
        q_gain[None, :], k_gain[None, :], ctx_lift,
    )
    o = run_repair(l, o, q, kv_all, ctx, ctx_lift)
    return run_output(run_exchange(o), w_out, lat, gate)[None]


def solution(mesh):
    in_specs = (
        P("dp", ("sp", "tp"), None),
        P("dp", "sp"),
        P("sp"),
        P("dp", "sp", None),
        P(),
        P("sp", "tp"),
        P("sp", "tp"),
        P("sp", "tp"),
        P(None, "tp"),
        P(None, "tp"),
        P(None, "tp"),
        P(),
        P(),
        P("tp"),
        P(),
    )
    return jax.shard_map(
        on_device, mesh=mesh, in_specs=in_specs,
        out_specs=P("dp", ("sp", "tp"), None), check_vma=False,
    )
```

```python
import functools

import jax
import jax.numpy as jnp
import numpy as np
from jax import lax
from jax.experimental import pallas as pl
from jax.experimental.pallas import tpu as pltpu
from jax.sharding import PartitionSpec as P

MESH = pl.DeviceIdType.MESH
HD = 64
GRID_W = 128
EPS = 1e-06
THETA = 10000.0
LOG2E = 1.4426950408889634
N_SP = 16
N_TP = 4
F32 = jnp.float32
BF16 = jnp.bfloat16
VMEM = pl.BlockSpec(memory_space=pltpu.VMEM)
HBM = pl.BlockSpec(memory_space=pltpu.HBM)
SMEM = pl.BlockSpec(memory_space=pltpu.SMEM)


def angle_table():
    i = (np.arange(HD) // 2) % 16
    f = (THETA ** (-(i.astype(np.float32)) / np.float32(16))).astype(np.float32)
    return np.repeat(f[:, None], GRID_W, axis=1)


def tall(x):
    return jnp.concatenate([x, jnp.zeros_like(x)], axis=0)


SENDS = [
    (0, 1, 1, 0), (0, 2, -1, 0), (0, 3, 0, 1), (0, 4, 0, -1),
    (1, 5, 1, 0), (1, 6, 0, 1), (1, 7, 0, -1),
    (2, 8, 0, 1), (2, 9, 0, -1),
    (3, 10, 0, 1),
    (5, 11, 0, 1), (5, 12, 0, -1),
    (7, 13, 0, -1), (8, 14, 0, 1), (12, 15, 0, -1),
]
TILE = 1536
NARROW = 512
VROWS = 80
FIRST = 5
UNITS = 32


def attention_kernel(
    lat_hbm, ctx_hbm, ms_hbm, mc_hbm, mg_hbm, wq_hbm, wk_hbm, wv_hbm,
    cond, condc, gain, qg, kg, table, lift,
    o_out, l_out, q_all, kv_all, ctx_all, gate_out,
    xbuf, part, psum_in, mine, full, wall, ubuf, raw, cosb, sinb, scl, sft, cbuf,
    q_out, kvbuf, acc, peak, p_even, p_odd, lat, ctx, m_shift, m_scale, m_gate, wq, wk, wv, load_sem,
    x_send, x_recv, p_send, p_recv, t_send, t_recv, c_send, c_recv, kv_send, kv_recv, keep_sem,
):
    sp = lax.axis_index("sp")
    tp = lax.axis_index("tp")
    y, z = lax.rem(sp, 4), lax.div(sp, 4)
    rows, width = lat.shape
    half = rows // 2

    def sp_at(k):
        return {"sp": lax.rem(sp + k, N_SP)}

    def tp_at(k):
        return {"tp": lax.rem(tp + k, N_TP)}

    def near(dy, dz):
        return {"sp": lax.rem(z + dz + 4, 4) * 4 + lax.rem(y + dy + 4, 4)}

    barrier = pltpu.get_barrier_semaphore()
    for k in range(1, N_SP):
        pl.semaphore_signal(barrier, inc=1, device_id=sp_at(k), device_id_type=MESH)
    for k in range(1, N_TP):
        pl.semaphore_signal(barrier, inc=1, device_id=tp_at(k), device_id_type=MESH)
    pairs = zip(
        (ms_hbm, mc_hbm, mg_hbm, lat_hbm, ctx_hbm, wq_hbm, wk_hbm, wv_hbm),
        (m_shift, m_scale, m_gate, lat, ctx, wq, wk, wv),
    )
    loads = [pltpu.make_async_copy(a, b, load_sem.at[i]) for i, (a, b) in enumerate(pairs)]
    for load in loads:
        load.start()
    pl.semaphore_wait(barrier, N_SP - 1 + N_TP - 1)

    def send(src, dst, s_sem, r_sem, target):
        return pltpu.make_async_remote_copy(
            src_ref=src, dst_ref=dst, send_sem=s_sem, recv_sem=r_sem,
            device_id=target, device_id_type=MESH,
        )

    def x_copy(i, src, to_row, count, k):
        return send(src, xbuf.at[pl.ds(to_row, count)], x_send.at[i], x_recv.at[i], tp_at(k))

    ra = x_copy(0, lat_hbm.at[pl.ds(0, 64)], 0, 64, 1)
    la = x_copy(1, lat_hbm.at[pl.ds(half, 64)], 96, 64, 3)
    rb = x_copy(2, lat_hbm.at[pl.ds(64, 32)], 64, 32, 1)
    lb = x_copy(3, lat_hbm.at[pl.ds(half + 64, 32)], 160, 32, 3)
    rc = x_copy(4, lat_hbm.at[pl.ds(half, half)], 192, half, 1)
    lc = x_copy(5, lat_hbm.at[pl.ds(0, half)], 288, half, 3)
    rf = x_copy(6, xbuf.at[pl.ds(0, half)], 384, half, 1)
    lf = x_copy(7, xbuf.at[pl.ds(half, half)], 480, half, 3)
    x_copies = [ra, la, rb, lb, rc, lc, rf, lf]
    ra.start()
    la.start()

    at = lax.broadcasted_iota(jnp.int32, (16, 128), 0)
    given = jnp.where(
        at == 0,
        jnp.broadcast_to(cond[...].astype(F32), (16, 128)),
        jnp.where(at == 1, jnp.broadcast_to(condc[...].astype(F32), (16, 128)), 0.0),
    )
    for load in loads[0:3]:
        load.wait()
    active = (given / (1.0 + jnp.exp(-given))).astype(BF16)
    for k, weight in enumerate((m_shift, m_scale, m_gate)):
        product = jnp.dot(active, weight[...], preferred_element_type=F32)
        for r in range(2):
            for c in range(4):
                i = r * 12 + k * 4 + c
                part[i : i + 1, :] = product[r : r + 1, c * 128 : (c + 1) * 128]
    p_copies = [
        send(part, psum_in.at[k - 1], p_send.at[k - 1], p_recv.at[k - 1], sp_at(k))
        for k in range(1, N_SP)
    ]
    for copy in p_copies:
        copy.start()

    for load in loads[3:]:
        load.wait()
    wall[:, 0:256] = wq[...]
    wall[:, 256:384] = jnp.concatenate([wk[...], wv[...]], axis=0).T

    for copy in p_copies:
        copy.wait_recv()
    total = part[...]
    for k in range(N_SP - 1):
        total = total + psum_in[k]
    mine[...] = total
    full[tp] = total
    t_copies = [
        send(mine, full.at[tp], t_send.at[k - 1], t_recv.at[k - 1], tp_at(k))
        for k in range(1, N_TP)
    ]
    for copy in t_copies:
        copy.start()
    for copy in (rb, lb, rc, lc):
        copy.start()

    row_id = lax.broadcasted_iota(jnp.int32, (HD, GRID_W), 0)
    lane_id = lax.broadcasted_iota(jnp.int32, (HD, GRID_W), 1)
    even = lax.rem(row_id, 2) == 0
    left, right, opposite = (lax.rem(tp + k, N_TP) * rows for k in (3, 1, 2))
    for g in range(6):
        n = lane_id + g * 128
        shift = jnp.where(
            n < 192,
            tp * rows,
            jnp.where(
                n < 288,
                left - 192,
                jnp.where(
                    n < 384,
                    right - 192,
                    jnp.where(
                        n < 480,
                        left - 288,
                        jnp.where(n < 576, right - 480, opposite - 576),
                    ),
                ),
            ),
        )
        at_token = n + shift + sp * 768
        grid_at = jnp.where(row_id < 32, at_token >> 7, at_token & 127)
        angle = table[...] * grid_at.astype(F32)
        cosb[g] = jnp.cos(angle)
        sine = jnp.sin(angle)
        sinb[g] = jnp.where(even, -sine, sine)

    for copy in t_copies:
        copy.wait_recv()

    def vector(r, k):
        pieces = [
            full[t, r * 12 + k * 4 + c : r * 12 + k * 4 + c + 1, :]
            for t in range(N_TP)
            for c in range(4)
        ]
        return jnp.concatenate(pieces, axis=1)

    gains = gain[...].astype(F32)
    gains = jnp.concatenate([gains[i : i + 1, :] for i in range(width // 128)], axis=1)
    for r in range(2):
        scl[r] = jnp.broadcast_to(gains * (1.0 + vector(r, 1)), (8, width))
        sft[r] = jnp.broadcast_to(vector(r, 0), (8, width))
    gate_out[...] = vector(0, 2)

    def modulate(src, r, count):
        values = src.astype(F32)
        inverse = lax.rsqrt(jnp.mean(values * values, axis=-1, keepdims=True) + EPS)
        normed = (values * inverse).reshape(count // 8, 8, width)
        return (normed * scl[r][None] + sft[r][None]).reshape(count, width).astype(BF16)

    uc = modulate(ctx[...], 1, ctx.shape[0])
    craw = jnp.dot(uc, wall[:, 256:384], preferred_element_type=F32)
    lane = lax.broadcasted_iota(jnp.int32, craw.shape, 1)
    square = jnp.where(lane < HD, craw * craw, 0.0)
    mean = jnp.sum(square, axis=-1, keepdims=True) * (1.0 / HD)
    k_row = kg[...].astype(F32)
    keys = craw * lax.rsqrt(mean + EPS) * jnp.concatenate([k_row, jnp.ones((1, HD), F32)], axis=1)
    cbuf[pl.ds(0, 32), :] = jnp.where(lane < HD, keys, craw).astype(BF16)

    def project(x, first, to_row, between=None):
        @pl.loop(0, rows // 32)
        def _(i):
            at_rows = pl.ds(pl.multiple_of(i * 32, 32), 32)
            from_rows = pl.ds(pl.multiple_of(first + i * 32, 32), 32)
            ubuf[at_rows, :] = modulate(x[from_rows, :], 0, 32)

        if between is not None:
            between()
        raw[pl.ds(to_row, rows), :] = jnp.dot(ubuf[...], wall[...], preferred_element_type=F32)

    def column(ref):
        r = lax.broadcasted_iota(jnp.int32, (HD, HD), 0)
        c = lax.broadcasted_iota(jnp.int32, (HD, HD), 1)
        spread = jnp.broadcast_to(ref[...].astype(F32), (HD, HD))
        return jnp.sum(jnp.where(r == c, spread, 0.0), axis=1, keepdims=True)

    q_gain = column(qg)
    k_gain = column(kg)

    def turned(x, gain_column, g):
        square = jnp.sum(x * x, axis=0, keepdims=True) * (1.0 / HD)
        normed = x * lax.rsqrt(square + EPS) * gain_column
        up = pltpu.roll(normed, HD - 1, axis=0)
        down = pltpu.roll(normed, 1, axis=0)
        return normed * cosb[g] + jnp.where(even, up, down) * sinb[g]

    scale = LOG2E * HD ** (-0.5)

    def finish_kv(s):
        slot = s * N_SP
        for i in range(3):
            g = 3 * s + i
            side = raw[g * 128 : (g + 1) * 128, 256:384].T
            k = turned(side[0:HD], k_gain, g).T
            kvbuf[slot, i * 64 : (i + 1) * 64, :] = jnp.concatenate(
                [k[0:64], k[64:128]], axis=1
            ).astype(BF16)
        order = [(g, p) for p in range(2) for g in (3 * s, 3 * s + 1, 3 * s + 2)]
        for b in range(3):
            pieces = [
                raw[g * 128 + p * 64 : g * 128 + p * 64 + 64, 256:384]
                for g, p in order[2 * b : 2 * b + 2]
            ]
            side = jnp.concatenate(pieces, axis=0).T
            at_row = 192 + b * 64
            kvbuf[slot, at_row : at_row + 64, :] = side[HD : 2 * HD].astype(BF16)

    def finish_q(blocks):
        for g in blocks:
            block = raw[g * 128 : (g + 1) * 128, :]
            for pair in range(2):
                side = block[:, pair * 128 : (pair + 1) * 128].T
                for h in range(2):
                    q = turned(side[h * HD : (h + 1) * HD], q_gain, g)
                    at_lane = g * 512 + (pair * 2 + h) * 128
                    q_out[:, at_lane : at_lane + 128] = (q * scale).astype(BF16)

    kv_copies = [[], []]
    for s in range(2):
        for i, (here, there, dy, dz) in enumerate(SENDS):
            here, there = here + s * N_SP, there + s * N_SP
            kv_copies[s].append(
                send(
                    kvbuf.at[here], kvbuf.at[there],
                    kv_send.at[i + s * len(SENDS)], kv_recv.at[there], near(dy, dz),
                )
            )

    def start_from(s, slot):
        for copy, (here, _, _, _) in zip(kv_copies[s], SENDS):
            if here == slot:
                copy.start()

    def keep(s, slot):
        slot = slot + s * N_SP
        return pltpu.make_async_copy(kvbuf.at[slot], kv_all.at[slot], keep_sem.at[slot])

    def arrive(s, slot):
        if slot > 0:
            next(
                copy for copy, (_, there, _, _) in zip(kv_copies[s], SENDS) if there == slot
            ).wait_recv()
        start_from(s, slot)
        keep(s, slot).start()

    lifts = jnp.concatenate([jnp.full((1, 128), lift[h] * LOG2E, F32) for h in range(4)], axis=1)
    lifts = jnp.concatenate([lifts] * (TILE // 512), axis=1)
    ones = jnp.ones((VROWS - HD, 768), BF16)

    def lanes(t):
        if isinstance(t, int):
            return pl.ds(t * TILE, TILE)
        return pl.ds(pl.multiple_of(t * TILE, TILE), TILE)

    def narrow(t, n):
        start = t * TILE + n * NARROW
        return pl.ds(start if isinstance(t, int) else pl.multiple_of(start, NARROW), NARROW)

    def context(t):
        cv = cbuf[...].astype(F32).T[HD : 2 * HD].astype(BF16)
        cv = jnp.concatenate([cv, ones[:, 0:512]], axis=0)
        scores = jnp.dot(cbuf[...], tall(q_out[:, lanes(t)]), preferred_element_type=F32) + lifts
        top = jnp.max(scores, axis=0, keepdims=True)
        peak[:, lanes(t)] = top
        weights = jnp.exp2(scores - top).astype(BF16)
        acc[:, lanes(t)] = jnp.dot(cv, weights, preferred_element_type=F32)

    def query_forms(at_lanes):
        q = q_out[:, at_lanes]
        return tall(q), jnp.concatenate([jnp.zeros_like(q), q], axis=0)

    def values_of(pair):
        v = [kvbuf[pair * 2 + s, pl.ds(192 + i * 64, 64), :] for s in range(2) for i in range(3)]
        return jnp.concatenate([jnp.concatenate(v, axis=1), ones], axis=0)

    def work(now, then, read, write):
        if now is not None:
            v = values_of(now[0])
        for n in range(TILE // NARROW):
            cols = slice(n * NARROW, (n + 1) * NARROW)
            if then is not None:
                theirs = narrow(then[1], n)
                forms = query_forms(theirs)
                top = peak[:, theirs]
            total = None
            for i in range(4):
                if then is not None:
                    s, p = i % 2, i // 2
                    k = kvbuf[then[0] * 2 + s, pl.ds(0, 192), :]
                    x = jnp.dot(k, forms[p], preferred_element_type=F32)
                    write[pl.ds(s * 384 + p * 192, 192), cols] = jnp.exp2(x - top).astype(BF16)
                if now is not None and i < 3:
                    term = jnp.dot(
                        v[:, i * 256 : (i + 1) * 256], read[pl.ds(i * 256, 256), cols],
                        preferred_element_type=F32,
                    )
                    total = term if total is None else total + term
            if now is not None:
                acc[:, narrow(now[1], n)] += total

    def unit(j):
        pair = jnp.where(
            j < 2 * FIRST,
            j - FIRST,
            jnp.where(
                j < 16, FIRST + (j - 2 * FIRST) // 2, jnp.where(j < 24, j - 8, j - 16)
            ),
        )
        tile = jnp.where(
            j < 2 * FIRST, 1, jnp.where(j < 16, lax.rem(j, 2), jnp.where(j < 24, 0, 1))
        )
        return pair, tile

    c_copies = [
        send(
            cbuf.at[pl.ds(0, 32)], cbuf.at[pl.ds(32 * k, 32)],
            c_send.at[k - 1], c_recv.at[k - 1], sp_at(k),
        )
        for k in range(1, N_SP)
    ]

    def start_context():
        for copy in c_copies:
            copy.start()

    project(lat, 0, 0, start_context)
    ra.wait_recv()
    rb.wait_recv()
    rf.start()
    la.wait_recv()
    lb.wait_recv()
    lf.start()
    project(xbuf, 0, 192)
    finish_kv(0)
    finish_q((0,))
    arrive(0, 0)
    finish_q((1, 2))
    for copy in c_copies:
        copy.wait_recv()
    context(0)
    arrive(0, 1)
    work(None, (0, 0), None, p_even)

    def first_step(d, carry):
        for pair in range(1, FIRST):

            @pl.when(d == (pair - 1) // 2)
            def _(pair=pair):
                arrive(0, 2 * pair)
                arrive(0, 2 * pair + 1)

        work((2 * d, 0), (2 * d + 1, 0), p_even, p_odd)
        work((2 * d + 1, 0), (2 * d + 2, 0), p_odd, p_even)
        return carry

    lax.fori_loop(0, FIRST // 2, first_step, 0)
    work((FIRST - 1, 0), None, p_even, None)

    rc.wait_recv()
    lc.wait_recv()
    project(xbuf, 192, 384)
    rf.wait_recv()
    lf.wait_recv()
    project(xbuf, 384, 576)
    finish_kv(1)
    finish_q((3,))
    arrive(1, 0)
    finish_q((4, 5))
    context(1)
    keep_rest = [
        pltpu.make_async_copy(q_out, q_all, keep_sem.at[2 * N_SP]),
        pltpu.make_async_copy(cbuf, ctx_all, keep_sem.at[2 * N_SP + 1]),
    ]
    for copy in keep_rest:
        copy.start()
    work(None, (0, 1), None, p_even)

    events = [(0, 0, (5,)), (1, 0, (6,)), (2, 1, (0, 1)), (3, 0, (7,)), (3, 1, (2, 3)),
              (4, 1, (4,)), (5, 1, (5,)), (6, 1, (6,)), (8, 1, (7,))]

    def second_step(d, carry):
        for when, s, pairs in events:

            @pl.when(d == when)
            def _(s=s, pairs=pairs):
                for pair in pairs:
                    for slot in (2 * pair, 2 * pair + 1):
                        if slot > 0:
                            arrive(s, slot)

        j = FIRST + 2 * d
        work(unit(j), unit(j + 1), p_even, p_odd)
        work(unit(j + 1), unit(j + 2), p_odd, p_even)
        return carry

    lax.fori_loop(0, (UNITS - 1 - FIRST) // 2, second_step, 0)
    work((15, 1), None, p_even, None)

    l_out[...] = acc[HD : HD + 8, :]
    for g in range(6):
        at_lanes = pl.ds(g * 512, 512)
        mean = acc[0:HD, at_lanes] / acc[HD : HD + 1, at_lanes]
        stack = jnp.concatenate([mean[:, h * 128 : (h + 1) * 128] for h in range(4)], axis=0)
        o_out[g * 128 : (g + 1) * 128, :] = stack.T.astype(BF16)
    for copy in x_copies + p_copies + t_copies + c_copies + kv_copies[0] + kv_copies[1]:
        copy.wait_send()
    for s in range(2):
        for slot in range(N_SP):
            keep(s, slot).wait()
    for copy in keep_rest:
        copy.wait()


def run_attention(lat, cond, condc, ctx, gain, ms, mc, mg, wq, wk, wv, qg, kg, lift):
    rows, width = lat.shape
    dma = pltpu.SemaphoreType.DMA
    loaded = (lat, ctx, ms, mc, mg, wq, wk, wv)
    return pl.pallas_call(
        attention_kernel,
        name="attention",
        out_shape=(
            jax.ShapeDtypeStruct((768, 256), BF16),
            jax.ShapeDtypeStruct((8, 3072), F32),
            jax.ShapeDtypeStruct((HD, 3072), BF16),
            jax.ShapeDtypeStruct((2 * N_SP, 384, 128), BF16),
            jax.ShapeDtypeStruct((512, 128), BF16),
            jax.ShapeDtypeStruct((1, width), F32),
        ),
        in_specs=[HBM] * 8 + [VMEM] * 6 + [SMEM],
        out_specs=(VMEM, VMEM, HBM, HBM, HBM, VMEM),
        scratch_shapes=[
            pltpu.VMEM((3 * rows, width), BF16),
            pltpu.VMEM((24, 128), F32),
            pltpu.VMEM((N_SP - 1, 24, 128), F32),
            pltpu.VMEM((24, 128), F32),
            pltpu.VMEM((N_TP, 24, 128), F32),
            pltpu.VMEM((width, 384), BF16),
            pltpu.VMEM((rows, width), BF16),
            pltpu.VMEM((768, 384), F32),
            pltpu.VMEM((6, HD, GRID_W), F32),
            pltpu.VMEM((6, HD, GRID_W), F32),
            pltpu.VMEM((2, 8, width), F32),
            pltpu.VMEM((2, 8, width), F32),
            pltpu.VMEM((512, 128), BF16),
            pltpu.VMEM((HD, 3072), BF16),
            pltpu.VMEM((2 * N_SP, 384, 128), BF16),
            pltpu.VMEM((VROWS, 3072), F32),
            pltpu.VMEM((1, 3072), F32),
            pltpu.VMEM((768, TILE), BF16),
            pltpu.VMEM((768, TILE), BF16),
            *[pltpu.VMEM(a.shape, BF16) for a in loaded],
            dma((len(loaded),)),
            dma((8,)), dma((8,)), dma((15,)), dma((15,)),
            dma((3,)), dma((3,)), dma((15,)), dma((15,)),
            dma((2 * len(SENDS),)), dma((2 * N_SP,)), dma((2 * N_SP + 2,)),
        ],
        compiler_params=pltpu.CompilerParams(
            collective_id=0, has_side_effects=True, vmem_limit_bytes=60 * 2**20
        ),
        cost_estimate=pl.CostEstimate(
            flops=2 * 10**10, bytes_accessed=10**7, transcendentals=4 * 10**7
        ),
    )(
        *loaded, cond, condc, gain, qg, kg, jnp.asarray(angle_table()), lift,
    )


def repair_kernel(
    l_ref, o_in, q_hbm, kv_hbm, ctx_hbm, lift, o_out,
    q_ref, kvbuf, ctx, acc, peak, sem,
):
    safe = jnp.all(l_ref[...] < 2.0**100)
    o_out[...] = o_in[...]

    @pl.when(jnp.logical_not(safe))
    def _():
        for src, dst in ((q_hbm, q_ref), (kv_hbm, kvbuf), (ctx_hbm, ctx)):
            copy = pltpu.make_async_copy(src, dst, sem)
            copy.start()
            copy.wait()
        wide = 512
        ones = jnp.ones((VROWS - HD, 768), BF16)
        lifts = jnp.concatenate(
            [jnp.full((1, 128), lift[h] * LOG2E, F32) for h in range(4)], axis=1
        )
        cv = ctx[...].astype(F32).T[HD : 2 * HD].astype(BF16)
        cv = jnp.concatenate([cv, ones[:, 0:512]], axis=0)

        @pl.loop(0, q_ref.shape[1] // wide)
        def _(t):
            lanes = pl.ds(pl.multiple_of(t * wide, wide), wide)
            q = q_ref[:, lanes]
            left = tall(q)
            right = jnp.concatenate([jnp.zeros_like(q), q], axis=0)
            scores = jnp.dot(ctx[...], left, preferred_element_type=F32) + lifts
            top = jnp.max(scores, axis=0, keepdims=True)
            peak[...] = top
            weights = jnp.exp2(scores - top).astype(BF16)
            acc[...] = jnp.dot(cv, weights, preferred_element_type=F32)

            @pl.loop(0, N_SP)
            def _(b):
                parts = []
                for s in range(2):
                    k = kvbuf[b * 2 + s, pl.ds(0, 192), :]
                    for query in (left, right):
                        parts.append(jnp.dot(k, query, preferred_element_type=F32))
                x = jnp.concatenate(parts, axis=0)
                old = peak[...]
                new = jnp.maximum(old, jnp.max(x, axis=0, keepdims=True))
                peak[...] = new
                v = [
                    kvbuf[b * 2 + s, pl.ds(192 + i * 64, 64), :] for s in range(2) for i in range(3)
                ]
                v = jnp.concatenate([jnp.concatenate(v, axis=1), ones], axis=0)
                weights = jnp.exp2(x - new).astype(BF16)
                acc[...] = acc[...] * jnp.exp2(old - new) + jnp.dot(
                    v, weights, preferred_element_type=F32
                )

            mean = acc[0:HD, :] / acc[HD : HD + 1, :]
            stack = jnp.concatenate([mean[:, h * 128 : (h + 1) * 128] for h in range(4)], axis=0)
            rows = pl.ds(pl.multiple_of(t * 128, 128), 128)
            o_out[rows, :] = stack.T.astype(BF16)


def run_repair(l, o, q, kv_all, ctx, lift):
    return pl.pallas_call(
        repair_kernel,
        name="repair",
        out_shape=jax.ShapeDtypeStruct(o.shape, o.dtype),
        in_specs=[VMEM, VMEM, HBM, HBM, HBM, SMEM],
        out_specs=VMEM,
        scratch_shapes=[
            pltpu.VMEM((HD, 3072), BF16),
            pltpu.VMEM((2 * N_SP, 384, 128), BF16),
            pltpu.VMEM((512, 128), BF16),
            pltpu.VMEM((VROWS, 512), F32),
            pltpu.VMEM((1, 512), F32),
            pltpu.SemaphoreType.DMA(()),
        ],
        compiler_params=pltpu.CompilerParams(vmem_limit_bytes=60 * 2**20),
    )(l, o, q, kv_all, ctx, lift)


def exchange_kernel(o_ref, out, obuf, send_sem, recv_sem):
    tp = lax.axis_index("tp")
    rows = o_ref.shape[0] // N_TP
    half = rows // 2

    def tp_at(k):
        return {"tp": lax.rem(tp + k, N_TP)}

    barrier = pltpu.get_barrier_semaphore()
    for k in range(1, N_TP):
        pl.semaphore_signal(barrier, inc=1, device_id=tp_at(k), device_id_type=MESH)
    pl.semaphore_wait(barrier, N_TP - 1)
    plan = [(2, 576, 0, rows), (3, 192, 0, half), (1, 288, half, half), (3, 384, half, half),
            (1, 480, 0, half)]
    copies = []
    for i, (k, here, there, count) in enumerate(plan):
        copies.append(
            pltpu.make_async_remote_copy(
                src_ref=o_ref.at[pl.ds(here, count)],
                dst_ref=obuf.at[tp, pl.ds(there, count)],
                send_sem=send_sem.at[i], recv_sem=recv_sem.at[i],
                device_id=tp_at(k), device_id_type=MESH,
            )
        )
        copies[-1].start()
    out[tp] = o_ref[0:rows, :]
    for copy in copies:
        copy.wait_recv()
    for k in range(1, N_TP):
        source = lax.rem(tp + k, N_TP)
        out[source] = obuf[source]
    for copy in copies:
        copy.wait_send()


def run_exchange(o):
    rows = o.shape[0] // N_TP
    dma = pltpu.SemaphoreType.DMA
    return pl.pallas_call(
        exchange_kernel,
        name="exchange",
        out_shape=jax.ShapeDtypeStruct((N_TP, rows, 256), BF16),
        in_specs=[VMEM],
        out_specs=VMEM,
        scratch_shapes=[pltpu.VMEM((N_TP, rows, 256), BF16), dma((5,)), dma((5,))],
        compiler_params=pltpu.CompilerParams(
            collective_id=2, has_side_effects=True, vmem_limit_bytes=4 * 2**20
        ),
        cost_estimate=pl.CostEstimate(flops=0, bytes_accessed=25 * 10**6, transcendentals=0),
    )(o)


def output_kernel(o_ref, w, lat, gate, out):
    wide = 512
    for n in range(out.shape[1] // wide):
        cols = slice(n * wide, (n + 1) * wide)
        total = None
        for t in range(N_TP):
            term = jnp.dot(
                o_ref[t], w[t * 256 : (t + 1) * 256, cols], preferred_element_type=F32
            )
            total = term if total is None else total + term
        out[:, cols] = (lat[:, cols].astype(F32) + gate[:, cols] * total).astype(BF16)


def run_output(o, w_out, lat, gate):
    return pl.pallas_call(
        output_kernel,
        name="output",
        out_shape=jax.ShapeDtypeStruct(lat.shape, BF16),
        in_specs=[VMEM] * 4,
        out_specs=VMEM,
        compiler_params=pltpu.CompilerParams(vmem_limit_bytes=12 * 2**20),
    )(o, w_out, lat, gate)


def on_device(
    latent, cond, cond_ctx, context, norm_gain, mod_shift, mod_scale, mod_gate,
    w_query, w_key, w_value, q_gain, k_gain, ctx_lift, w_out,
):
    lat = latent[0]
    o, l, q, kv_all, ctx, gate = run_attention(
        lat, cond, cond_ctx[None, :], context[0], norm_gain.reshape(-1, 128),
        mod_shift, mod_scale, mod_gate, w_query, w_key.T, w_value.T,
        q_gain[None, :], k_gain[None, :], ctx_lift,
    )
    o = run_repair(l, o, q, kv_all, ctx, ctx_lift)
    return run_output(run_exchange(o), w_out, lat, gate)[None]


def solution(mesh):
    in_specs = (
        P("dp", ("sp", "tp"), None),
        P("dp", "sp"),
        P("sp"),
        P("dp", "sp", None),
        P(),
        P("sp", "tp"),
        P("sp", "tp"),
        P("sp", "tp"),
        P(None, "tp"),
        P(None, "tp"),
        P(None, "tp"),
        P(),
        P(),
        P("tp"),
        P(),
    )
    return jax.shard_map(
        on_device, mesh=mesh, in_specs=in_specs,
        out_specs=P("dp", ("sp", "tp"), None), check_vma=False,
    )
```

```python
import functools

import jax
import jax.numpy as jnp
import numpy as np
from jax import lax
from jax.experimental import pallas as pl
from jax.experimental.pallas import tpu as pltpu
from jax.sharding import PartitionSpec as P

MESH = pl.DeviceIdType.MESH
HD = 64
GRID_W = 128
EPS = 1e-06
THETA = 10000.0
LOG2E = 1.4426950408889634
N_SP = 16
N_TP = 4
F32 = jnp.float32
BF16 = jnp.bfloat16
VMEM = pl.BlockSpec(memory_space=pltpu.VMEM)
HBM = pl.BlockSpec(memory_space=pltpu.HBM)
SMEM = pl.BlockSpec(memory_space=pltpu.SMEM)


def angle_table():
    i = (np.arange(HD) // 2) % 16
    f = (THETA ** (-(i.astype(np.float32)) / np.float32(16))).astype(np.float32)
    return np.repeat(f[:, None], GRID_W, axis=1)


def tall(x):
    return jnp.concatenate([x, jnp.zeros_like(x)], axis=0)


SENDS = [
    (0, 1, 1, 0), (0, 2, -1, 0), (0, 3, 0, 1), (0, 4, 0, -1),
    (1, 5, 1, 0), (1, 6, 0, 1), (1, 7, 0, -1),
    (2, 8, 0, 1), (2, 9, 0, -1),
    (3, 10, 0, 1),
    (5, 11, 0, 1), (5, 12, 0, -1),
    (7, 13, 0, -1), (8, 14, 0, 1), (12, 15, 0, -1),
]
TILE = 1536
NARROW = 512
VROWS = 80
FIRST = 5
UNITS = 32
RETURNS = [(2, 576, 0, 192), (3, 384, 96, 96), (1, 480, 0, 96), (3, 192, 0, 96), (1, 288, 96, 96)]


def attention_kernel(
    lat_hbm, ctx_hbm, ms_hbm, mc_hbm, mg_hbm, wq_hbm, wk_hbm, wv_hbm,
    cond, condc, gain, qg, kg, table, lift,
    rows_out, flag_out, o_out, l_out, q_all, kv_all, ctx_all, gate_out,
    xbuf, part, psum_in, mine, full, wall, ubuf, raw, cosb, sinb, scl, sft, cbuf,
    q_out, kvbuf, acc, peak, p_even, p_odd, lat, ctx, m_shift, m_scale, m_gate, wq, wk, wv, load_sem,
    x_send, x_recv, p_send, p_recv, t_send, t_recv, c_send, c_recv, kv_send, kv_recv, keep_sem,
    obuf, fbuf, flag, o_send, o_recv, f_send, f_recv,
):
    sp = lax.axis_index("sp")
    tp = lax.axis_index("tp")
    y, z = lax.rem(sp, 4), lax.div(sp, 4)
    rows, width = lat.shape
    half = rows // 2

    def sp_at(k):
        return {"sp": lax.rem(sp + k, N_SP)}

    def tp_at(k):
        return {"tp": lax.rem(tp + k, N_TP)}

    def near(dy, dz):
        return {"sp": lax.rem(z + dz + 4, 4) * 4 + lax.rem(y + dy + 4, 4)}

    barrier = pltpu.get_barrier_semaphore()
    for k in range(1, N_SP):
        pl.semaphore_signal(barrier, inc=1, device_id=sp_at(k), device_id_type=MESH)
    for k in range(1, N_TP):
        pl.semaphore_signal(barrier, inc=1, device_id=tp_at(k), device_id_type=MESH)
    pairs = zip(
        (ms_hbm, mc_hbm, mg_hbm, lat_hbm, ctx_hbm, wq_hbm, wk_hbm, wv_hbm),
        (m_shift, m_scale, m_gate, lat, ctx, wq, wk, wv),
    )
    loads = [pltpu.make_async_copy(a, b, load_sem.at[i]) for i, (a, b) in enumerate(pairs)]
    for load in loads:
        load.start()
    pl.semaphore_wait(barrier, N_SP - 1 + N_TP - 1)

    def send(src, dst, s_sem, r_sem, target):
        return pltpu.make_async_remote_copy(
            src_ref=src, dst_ref=dst, send_sem=s_sem, recv_sem=r_sem,
            device_id=target, device_id_type=MESH,
        )

    def x_copy(i, src, to_row, count, k):
        return send(src, xbuf.at[pl.ds(to_row, count)], x_send.at[i], x_recv.at[i], tp_at(k))

    ra = x_copy(0, lat_hbm.at[pl.ds(0, 64)], 0, 64, 1)
    la = x_copy(1, lat_hbm.at[pl.ds(half, 64)], 96, 64, 3)
    rb = x_copy(2, lat_hbm.at[pl.ds(64, 32)], 64, 32, 1)
    lb = x_copy(3, lat_hbm.at[pl.ds(half + 64, 32)], 160, 32, 3)
    rc = x_copy(4, lat_hbm.at[pl.ds(half, half)], 192, half, 1)
    lc = x_copy(5, lat_hbm.at[pl.ds(0, half)], 288, half, 3)
    rf = x_copy(6, xbuf.at[pl.ds(0, half)], 384, half, 1)
    lf = x_copy(7, xbuf.at[pl.ds(half, half)], 480, half, 3)
    x_copies = [ra, la, rb, lb, rc, lc, rf, lf]
    ra.start()
    la.start()

    at = lax.broadcasted_iota(jnp.int32, (16, 128), 0)
    given = jnp.where(
        at == 0,
        jnp.broadcast_to(cond[...].astype(F32), (16, 128)),
        jnp.where(at == 1, jnp.broadcast_to(condc[...].astype(F32), (16, 128)), 0.0),
    )
    for load in loads[0:3]:
        load.wait()
    active = (given / (1.0 + jnp.exp(-given))).astype(BF16)
    for k, weight in enumerate((m_shift, m_scale, m_gate)):
        product = jnp.dot(active, weight[...], preferred_element_type=F32)
        for r in range(2):
            for c in range(4):
                i = r * 12 + k * 4 + c
                part[i : i + 1, :] = product[r : r + 1, c * 128 : (c + 1) * 128]
    p_copies = [
        send(part, psum_in.at[k - 1], p_send.at[k - 1], p_recv.at[k - 1], sp_at(k))
        for k in range(1, N_SP)
    ]
    for copy in p_copies:
        copy.start()

    for load in loads[3:]:
        load.wait()
    wall[:, 0:256] = wq[...]
    wall[:, 256:384] = jnp.concatenate([wk[...], wv[...]], axis=0).T

    for copy in p_copies:
        copy.wait_recv()
    total = part[...]
    for k in range(N_SP - 1):
        total = total + psum_in[k]
    mine[...] = total
    full[tp] = total
    t_copies = [
        send(mine, full.at[tp], t_send.at[k - 1], t_recv.at[k - 1], tp_at(k))
        for k in range(1, N_TP)
    ]
    for copy in t_copies:
        copy.start()
    for copy in (rb, lb, rc, lc):
        copy.start()

    row_id = lax.broadcasted_iota(jnp.int32, (HD, GRID_W), 0)
    lane_id = lax.broadcasted_iota(jnp.int32, (HD, GRID_W), 1)
    even = lax.rem(row_id, 2) == 0
    left, right, opposite = (lax.rem(tp + k, N_TP) * rows for k in (3, 1, 2))
    for g in range(6):
        n = lane_id + g * 128
        shift = jnp.where(
            n < 192,
            tp * rows,
            jnp.where(
                n < 288,
                left - 192,
                jnp.where(
                    n < 384,
                    right - 192,
                    jnp.where(
                        n < 480,
                        left - 288,
                        jnp.where(n < 576, right - 480, opposite - 576),
                    ),
                ),
            ),
        )
        at_token = n + shift + sp * 768
        grid_at = jnp.where(row_id < 32, at_token >> 7, at_token & 127)
        angle = table[...] * grid_at.astype(F32)
        cosb[g] = jnp.cos(angle)
        sine = jnp.sin(angle)
        sinb[g] = jnp.where(even, -sine, sine)

    for copy in t_copies:
        copy.wait_recv()

    def vector(r, k):
        pieces = [
            full[t, r * 12 + k * 4 + c : r * 12 + k * 4 + c + 1, :]
            for t in range(N_TP)
            for c in range(4)
        ]
        return jnp.concatenate(pieces, axis=1)

    gains = gain[...].astype(F32)
    gains = jnp.concatenate([gains[i : i + 1, :] for i in range(width // 128)], axis=1)
    for r in range(2):
        scl[r] = jnp.broadcast_to(gains * (1.0 + vector(r, 1)), (8, width))
        sft[r] = jnp.broadcast_to(vector(r, 0), (8, width))
    gate_out[...] = vector(0, 2)

    def modulate(src, r, count):
        values = src.astype(F32)
        inverse = lax.rsqrt(jnp.mean(values * values, axis=-1, keepdims=True) + EPS)
        normed = (values * inverse).reshape(count // 8, 8, width)
        return (normed * scl[r][None] + sft[r][None]).reshape(count, width).astype(BF16)

    uc = modulate(ctx[...], 1, ctx.shape[0])
    craw = jnp.dot(uc, wall[:, 256:384], preferred_element_type=F32)
    lane = lax.broadcasted_iota(jnp.int32, craw.shape, 1)
    square = jnp.where(lane < HD, craw * craw, 0.0)
    mean = jnp.sum(square, axis=-1, keepdims=True) * (1.0 / HD)
    k_row = kg[...].astype(F32)
    keys = craw * lax.rsqrt(mean + EPS) * jnp.concatenate([k_row, jnp.ones((1, HD), F32)], axis=1)
    cbuf[pl.ds(0, 32), :] = jnp.where(lane < HD, keys, craw).astype(BF16)

    def project(x, first, to_row, between=None):
        @pl.loop(0, rows // 32)
        def _(i):
            at_rows = pl.ds(pl.multiple_of(i * 32, 32), 32)
            from_rows = pl.ds(pl.multiple_of(first + i * 32, 32), 32)
            ubuf[at_rows, :] = modulate(x[from_rows, :], 0, 32)

        if between is not None:
            between()
        raw[pl.ds(to_row, rows), :] = jnp.dot(ubuf[...], wall[...], preferred_element_type=F32)

    def column(ref):
        r = lax.broadcasted_iota(jnp.int32, (HD, HD), 0)
        c = lax.broadcasted_iota(jnp.int32, (HD, HD), 1)
        spread = jnp.broadcast_to(ref[...].astype(F32), (HD, HD))
        return jnp.sum(jnp.where(r == c, spread, 0.0), axis=1, keepdims=True)

    q_gain = column(qg)
    k_gain = column(kg)

    def turned(x, gain_column, g):
        square = jnp.sum(x * x, axis=0, keepdims=True) * (1.0 / HD)
        normed = x * lax.rsqrt(square + EPS) * gain_column
        up = pltpu.roll(normed, HD - 1, axis=0)
        down = pltpu.roll(normed, 1, axis=0)
        return normed * cosb[g] + jnp.where(even, up, down) * sinb[g]

    scale = LOG2E * HD ** (-0.5)

    def finish_kv(s):
        slot = s * N_SP
        for i in range(3):
            g = 3 * s + i
            side = raw[g * 128 : (g + 1) * 128, 256:384].T
            k = turned(side[0:HD], k_gain, g).T
            kvbuf[slot, i * 64 : (i + 1) * 64, :] = jnp.concatenate(
                [k[0:64], k[64:128]], axis=1
            ).astype(BF16)
        order = [(g, p) for p in range(2) for g in (3 * s, 3 * s + 1, 3 * s + 2)]
        for b in range(3):
            pieces = [
                raw[g * 128 + p * 64 : g * 128 + p * 64 + 64, 256:384]
                for g, p in order[2 * b : 2 * b + 2]
            ]
            side = jnp.concatenate(pieces, axis=0).T
            at_row = 192 + b * 64
            kvbuf[slot, at_row : at_row + 64, :] = side[HD : 2 * HD].astype(BF16)

    def finish_q(blocks):
        for g in blocks:
            block = raw[g * 128 : (g + 1) * 128, :]
            for pair in range(2):
                side = block[:, pair * 128 : (pair + 1) * 128].T
                for h in range(2):
                    q = turned(side[h * HD : (h + 1) * HD], q_gain, g)
                    at_lane = g * 512 + (pair * 2 + h) * 128
                    q_out[:, at_lane : at_lane + 128] = (q * scale).astype(BF16)

    kv_copies = [[], []]
    for s in range(2):
        for i, (here, there, dy, dz) in enumerate(SENDS):
            here, there = here + s * N_SP, there + s * N_SP
            kv_copies[s].append(
                send(
                    kvbuf.at[here], kvbuf.at[there],
                    kv_send.at[i + s * len(SENDS)], kv_recv.at[there], near(dy, dz),
                )
            )

    def start_from(s, slot):
        for copy, (here, _, _, _) in zip(kv_copies[s], SENDS):
            if here == slot:
                copy.start()

    def keep(s, slot):
        slot = slot + s * N_SP
        return pltpu.make_async_copy(kvbuf.at[slot], kv_all.at[slot], keep_sem.at[slot])

    def arrive(s, slot):
        if slot > 0:
            next(
                copy for copy, (_, there, _, _) in zip(kv_copies[s], SENDS) if there == slot
            ).wait_recv()
        start_from(s, slot)
        keep(s, slot).start()

    lifts = jnp.concatenate([jnp.full((1, 128), lift[h] * LOG2E, F32) for h in range(4)], axis=1)
    lifts = jnp.concatenate([lifts] * (TILE // 512), axis=1)
    ones = jnp.ones((VROWS - HD, 768), BF16)

    def lanes(t):
        if isinstance(t, int):
            return pl.ds(t * TILE, TILE)
        return pl.ds(pl.multiple_of(t * TILE, TILE), TILE)

    def narrow(t, n):
        start = t * TILE + n * NARROW
        return pl.ds(start if isinstance(t, int) else pl.multiple_of(start, NARROW), NARROW)

    def context(t):
        cv = cbuf[...].astype(F32).T[HD : 2 * HD].astype(BF16)
        cv = jnp.concatenate([cv, ones[:, 0:512]], axis=0)
        scores = jnp.dot(cbuf[...], tall(q_out[:, lanes(t)]), preferred_element_type=F32) + lifts
        top = jnp.max(scores, axis=0, keepdims=True)
        peak[:, lanes(t)] = top
        weights = jnp.exp2(scores - top).astype(BF16)
        acc[:, lanes(t)] = jnp.dot(cv, weights, preferred_element_type=F32)

    def query_forms(at_lanes):
        q = q_out[:, at_lanes]
        return tall(q), jnp.concatenate([jnp.zeros_like(q), q], axis=0)

    def values_of(pair):
        v = [kvbuf[pair * 2 + s, pl.ds(192 + i * 64, 64), :] for s in range(2) for i in range(3)]
        return jnp.concatenate([jnp.concatenate(v, axis=1), ones], axis=0)

    def work(now, then, read, write):
        if now is not None:
            v = values_of(now[0])
        for n in range(TILE // NARROW):
            cols = slice(n * NARROW, (n + 1) * NARROW)
            if then is not None:
                theirs = narrow(then[1], n)
                forms = query_forms(theirs)
                top = peak[:, theirs]
            total = None
            for i in range(4):
                if then is not None:
                    s, p = i % 2, i // 2
                    k = kvbuf[then[0] * 2 + s, pl.ds(0, 192), :]
                    x = jnp.dot(k, forms[p], preferred_element_type=F32)
                    write[pl.ds(s * 384 + p * 192, 192), cols] = jnp.exp2(x - top).astype(BF16)
                if now is not None and i < 3:
                    term = jnp.dot(
                        v[:, i * 256 : (i + 1) * 256], read[pl.ds(i * 256, 256), cols],
                        preferred_element_type=F32,
                    )
                    total = term if total is None else total + term
            if now is not None:
                acc[:, narrow(now[1], n)] += total

    def unit(j):
        pair = jnp.where(
            j < 2 * FIRST,
            j - FIRST,
            jnp.where(
                j < 16, FIRST + (j - 2 * FIRST) // 2, jnp.where(j < 24, j - 8, j - 16)
            ),
        )
        tile = jnp.where(
            j < 2 * FIRST, 1, jnp.where(j < 16, lax.rem(j, 2), jnp.where(j < 24, 1, 0))
        )
        return pair, tile

    c_copies = [
        send(
            cbuf.at[pl.ds(0, 32)], cbuf.at[pl.ds(32 * k, 32)],
            c_send.at[k - 1], c_recv.at[k - 1], sp_at(k),
        )
        for k in range(1, N_SP)
    ]

    def start_context():
        for copy in c_copies:
            copy.start()

    project(lat, 0, 0, start_context)
    ra.wait_recv()
    rb.wait_recv()
    rf.start()
    la.wait_recv()
    lb.wait_recv()
    lf.start()
    project(xbuf, 0, 192)
    finish_kv(0)
    finish_q((0,))
    arrive(0, 0)
    finish_q((1, 2))
    for copy in c_copies:
        copy.wait_recv()
    context(0)
    arrive(0, 1)
    work(None, (0, 0), None, p_even)

    def first_step(d, carry):
        for pair in range(1, FIRST):

            @pl.when(d == (pair - 1) // 2)
            def _(pair=pair):
                arrive(0, 2 * pair)
                arrive(0, 2 * pair + 1)

        work((2 * d, 0), (2 * d + 1, 0), p_even, p_odd)
        work((2 * d + 1, 0), (2 * d + 2, 0), p_odd, p_even)
        return carry

    lax.fori_loop(0, FIRST // 2, first_step, 0)
    work((FIRST - 1, 0), None, p_even, None)

    rc.wait_recv()
    lc.wait_recv()
    project(xbuf, 192, 384)
    rf.wait_recv()
    lf.wait_recv()
    project(xbuf, 384, 576)
    finish_kv(1)
    finish_q((3,))
    arrive(1, 0)
    finish_q((4, 5))
    context(1)
    keep_rest = [
        pltpu.make_async_copy(q_out, q_all, keep_sem.at[2 * N_SP]),
        pltpu.make_async_copy(cbuf, ctx_all, keep_sem.at[2 * N_SP + 1]),
    ]
    for copy in keep_rest:
        copy.start()
    work(None, (0, 1), None, p_even)

    events = [(0, 0, (5,)), (1, 0, (6,)), (2, 1, (0, 1)), (3, 0, (7,)), (3, 1, (2, 3)),
              (4, 1, (4,)), (5, 1, (5,)), (6, 1, (6,)), (8, 1, (7,))]

    def second_step(d, carry):
        for when, s, pairs in events:

            @pl.when(d == when)
            def _(s=s, pairs=pairs):
                for pair in pairs:
                    for slot in (2 * pair, 2 * pair + 1):
                        if slot > 0:
                            arrive(s, slot)

        j = FIRST + 2 * d
        work(unit(j), unit(j + 1), p_even, p_odd)
        work(unit(j + 1), unit(j + 2), p_odd, p_even)
        return carry

    returns = [
        send(
            o_out.at[pl.ds(here, count)], obuf.at[tp, pl.ds(there, count)],
            o_send.at[i], o_recv.at[i], tp_at(k),
        )
        for i, (k, here, there, count) in enumerate(RETURNS)
    ]

    def finish_o(blocks):
        for g in blocks:
            at_lanes = pl.ds(g * 512, 512)
            mean = acc[0:HD, at_lanes] / acc[HD : HD + 1, at_lanes]
            stack = jnp.concatenate([mean[:, h * 128 : (h + 1) * 128] for h in range(4)], axis=0)
            o_out[g * 128 : (g + 1) * 128, :] = stack.T.astype(BF16)

    steps = (UNITS - 1 - FIRST) // 2
    lax.fori_loop(0, steps - 3, second_step, 0)
    finish_o((3, 4, 5))
    lax.fori_loop(steps - 3, steps - 2, second_step, 0)
    for copy, (_, here, _, _) in zip(returns, RETURNS):
        if here >= 384:
            copy.start()
    lax.fori_loop(steps - 2, steps, second_step, 0)
    work((15, 0), None, p_even, None)
    finish_o((1, 2))
    l_out[...] = acc[HD : HD + 8, :]
    peaks = acc[HD : HD + 1, 0:128]
    for i in range(1, 24):
        peaks = jnp.maximum(peaks, acc[HD : HD + 1, i * 128 : (i + 1) * 128])
    flag[...] = jnp.broadcast_to(peaks, (8, 128))
    fbuf[tp] = flag[...]
    finish_o((0,))
    for copy, (_, here, _, _) in zip(returns, RETURNS):
        if here < 384:
            copy.start()
    flags = [
        send(flag, fbuf.at[tp], f_send.at[k - 1], f_recv.at[k - 1], tp_at(k))
        for k in range(1, N_TP)
    ]
    for copy in flags:
        copy.start()
    rows_out[tp] = o_out[0:rows, :]
    for copy in returns + flags:
        copy.wait_recv()
    for k in range(1, N_TP):
        source = lax.rem(tp + k, N_TP)
        rows_out[source] = obuf[source]
    flag_out[...] = fbuf[...]
    waiting = x_copies + p_copies + t_copies + c_copies + kv_copies[0] + kv_copies[1]
    for copy in waiting + returns + flags:
        copy.wait_send()
    for s in range(2):
        for slot in range(N_SP):
            keep(s, slot).wait()
    for copy in keep_rest:
        copy.wait()


def run_attention(lat, cond, condc, ctx, gain, ms, mc, mg, wq, wk, wv, qg, kg, lift):
    rows, width = lat.shape
    dma = pltpu.SemaphoreType.DMA
    loaded = (lat, ctx, ms, mc, mg, wq, wk, wv)
    return pl.pallas_call(
        attention_kernel,
        name="attention",
        out_shape=(
            jax.ShapeDtypeStruct((N_TP, rows, 256), BF16),
            jax.ShapeDtypeStruct((N_TP, 8, 128), F32),
            jax.ShapeDtypeStruct((768, 256), BF16),
            jax.ShapeDtypeStruct((8, 3072), F32),
            jax.ShapeDtypeStruct((HD, 3072), BF16),
            jax.ShapeDtypeStruct((2 * N_SP, 384, 128), BF16),
            jax.ShapeDtypeStruct((512, 128), BF16),
            jax.ShapeDtypeStruct((1, width), F32),
        ),
        in_specs=[HBM] * 8 + [VMEM] * 6 + [SMEM],
        out_specs=(VMEM, VMEM, VMEM, VMEM, HBM, HBM, HBM, VMEM),
        scratch_shapes=[
            pltpu.VMEM((3 * rows, width), BF16),
            pltpu.VMEM((24, 128), F32),
            pltpu.VMEM((N_SP - 1, 24, 128), F32),
            pltpu.VMEM((24, 128), F32),
            pltpu.VMEM((N_TP, 24, 128), F32),
            pltpu.VMEM((width, 384), BF16),
            pltpu.VMEM((rows, width), BF16),
            pltpu.VMEM((768, 384), F32),
            pltpu.VMEM((6, HD, GRID_W), F32),
            pltpu.VMEM((6, HD, GRID_W), F32),
            pltpu.VMEM((2, 8, width), F32),
            pltpu.VMEM((2, 8, width), F32),
            pltpu.VMEM((512, 128), BF16),
            pltpu.VMEM((HD, 3072), BF16),
            pltpu.VMEM((2 * N_SP, 384, 128), BF16),
            pltpu.VMEM((VROWS, 3072), F32),
            pltpu.VMEM((1, 3072), F32),
            pltpu.VMEM((768, TILE), BF16),
            pltpu.VMEM((768, TILE), BF16),
            *[pltpu.VMEM(a.shape, BF16) for a in loaded],
            dma((len(loaded),)),
            dma((8,)), dma((8,)), dma((15,)), dma((15,)),
            dma((3,)), dma((3,)), dma((15,)), dma((15,)),
            dma((2 * len(SENDS),)), dma((2 * N_SP,)), dma((2 * N_SP + 2,)),
            pltpu.VMEM((N_TP, rows, 256), BF16),
            pltpu.VMEM((N_TP, 8, 128), F32),
            pltpu.VMEM((8, 128), F32),
            dma((len(RETURNS),)), dma((len(RETURNS),)), dma((N_TP - 1,)), dma((N_TP - 1,)),
        ],
        compiler_params=pltpu.CompilerParams(
            collective_id=0, has_side_effects=True, vmem_limit_bytes=67043328
        ),
        cost_estimate=pl.CostEstimate(
            flops=2 * 10**10, bytes_accessed=10**7, transcendentals=4 * 10**7
        ),
    )(
        *loaded, cond, condc, gain, qg, kg, jnp.asarray(angle_table()), lift,
    )


def repair_kernel(
    l_ref, o_in, q_hbm, kv_hbm, ctx_hbm, lift, o_out,
    q_ref, kvbuf, ctx, acc, peak, sem,
):
    safe = jnp.all(l_ref[...] < 2.0**100)
    o_out[...] = o_in[...]

    @pl.when(jnp.logical_not(safe))
    def _():
        for src, dst in ((q_hbm, q_ref), (kv_hbm, kvbuf), (ctx_hbm, ctx)):
            copy = pltpu.make_async_copy(src, dst, sem)
            copy.start()
            copy.wait()
        wide = 512
        ones = jnp.ones((VROWS - HD, 768), BF16)
        lifts = jnp.concatenate(
            [jnp.full((1, 128), lift[h] * LOG2E, F32) for h in range(4)], axis=1
        )
        cv = ctx[...].astype(F32).T[HD : 2 * HD].astype(BF16)
        cv = jnp.concatenate([cv, ones[:, 0:512]], axis=0)

        @pl.loop(0, q_ref.shape[1] // wide)
        def _(t):
            lanes = pl.ds(pl.multiple_of(t * wide, wide), wide)
            q = q_ref[:, lanes]
            left = tall(q)
            right = jnp.concatenate([jnp.zeros_like(q), q], axis=0)
            scores = jnp.dot(ctx[...], left, preferred_element_type=F32) + lifts
            top = jnp.max(scores, axis=0, keepdims=True)
            peak[...] = top
            weights = jnp.exp2(scores - top).astype(BF16)
            acc[...] = jnp.dot(cv, weights, preferred_element_type=F32)

            @pl.loop(0, N_SP)
            def _(b):
                parts = []
                for s in range(2):
                    k = kvbuf[b * 2 + s, pl.ds(0, 192), :]
                    for query in (left, right):
                        parts.append(jnp.dot(k, query, preferred_element_type=F32))
                x = jnp.concatenate(parts, axis=0)
                old = peak[...]
                new = jnp.maximum(old, jnp.max(x, axis=0, keepdims=True))
                peak[...] = new
                v = [
                    kvbuf[b * 2 + s, pl.ds(192 + i * 64, 64), :] for s in range(2) for i in range(3)
                ]
                v = jnp.concatenate([jnp.concatenate(v, axis=1), ones], axis=0)
                weights = jnp.exp2(x - new).astype(BF16)
                acc[...] = acc[...] * jnp.exp2(old - new) + jnp.dot(
                    v, weights, preferred_element_type=F32
                )

            mean = acc[0:HD, :] / acc[HD : HD + 1, :]
            stack = jnp.concatenate([mean[:, h * 128 : (h + 1) * 128] for h in range(4)], axis=0)
            rows = pl.ds(pl.multiple_of(t * 128, 128), 128)
            o_out[rows, :] = stack.T.astype(BF16)


def run_repair(l, o, q, kv_all, ctx, lift):
    return pl.pallas_call(
        repair_kernel,
        name="repair",
        out_shape=jax.ShapeDtypeStruct(o.shape, o.dtype),
        in_specs=[VMEM, VMEM, HBM, HBM, HBM, SMEM],
        out_specs=VMEM,
        scratch_shapes=[
            pltpu.VMEM((HD, 3072), BF16),
            pltpu.VMEM((2 * N_SP, 384, 128), BF16),
            pltpu.VMEM((512, 128), BF16),
            pltpu.VMEM((VROWS, 512), F32),
            pltpu.VMEM((1, 512), F32),
            pltpu.SemaphoreType.DMA(()),
        ],
        compiler_params=pltpu.CompilerParams(vmem_limit_bytes=67043328),
    )(l, o, q, kv_all, ctx, lift)


def exchange_kernel(o_ref, out, obuf, send_sem, recv_sem):
    tp = lax.axis_index("tp")
    rows = o_ref.shape[0] // N_TP

    def tp_at(k):
        return {"tp": lax.rem(tp + k, N_TP)}

    barrier = pltpu.get_barrier_semaphore()
    for k in range(1, N_TP):
        pl.semaphore_signal(barrier, inc=1, device_id=tp_at(k), device_id_type=MESH)
    pl.semaphore_wait(barrier, N_TP - 1)
    copies = []
    for i, (k, here, there, count) in enumerate(RETURNS):
        copies.append(
            pltpu.make_async_remote_copy(
                src_ref=o_ref.at[pl.ds(here, count)],
                dst_ref=obuf.at[tp, pl.ds(there, count)],
                send_sem=send_sem.at[i], recv_sem=recv_sem.at[i],
                device_id=tp_at(k), device_id_type=MESH,
            )
        )
        copies[-1].start()
    out[tp] = o_ref[0:rows, :]
    for copy in copies:
        copy.wait_recv()
    for k in range(1, N_TP):
        source = lax.rem(tp + k, N_TP)
        out[source] = obuf[source]
    for copy in copies:
        copy.wait_send()


def run_exchange(o):
    rows = o.shape[0] // N_TP
    dma = pltpu.SemaphoreType.DMA
    return pl.pallas_call(
        exchange_kernel,
        name="exchange",
        out_shape=jax.ShapeDtypeStruct((N_TP, rows, 256), BF16),
        in_specs=[VMEM],
        out_specs=VMEM,
        scratch_shapes=[pltpu.VMEM((N_TP, rows, 256), BF16), dma((5,)), dma((5,))],
        compiler_params=pltpu.CompilerParams(
            collective_id=2, has_side_effects=True, vmem_limit_bytes=4 * 2**20
        ),
        cost_estimate=pl.CostEstimate(flops=0, bytes_accessed=25 * 10**6, transcendentals=0),
    )(o)


def output_kernel(o_ref, w_hbm, lat, gate, out, w, sem):
    wide = 512
    count = out.shape[1] // wide
    loads = [
        pltpu.make_async_copy(w_hbm.at[:, pl.ds(n * wide, wide)], w.at[n], sem.at[n])
        for n in range(count)
    ]
    for load in loads:
        load.start()
    for n in range(count):
        cols = slice(n * wide, (n + 1) * wide)
        loads[n].wait()
        total = None
        for t in range(N_TP):
            term = jnp.dot(o_ref[t], w[n, t * 256 : (t + 1) * 256, :], preferred_element_type=F32)
            total = term if total is None else total + term
        out[:, cols] = (lat[:, cols].astype(F32) + gate[:, cols] * total).astype(BF16)


def run_output(o, w_out, lat, gate):
    return pl.pallas_call(
        output_kernel,
        name="output",
        out_shape=jax.ShapeDtypeStruct(lat.shape, BF16),
        in_specs=[VMEM, HBM, VMEM, VMEM],
        out_specs=VMEM,
        scratch_shapes=[
            pltpu.VMEM((4, w_out.shape[0], w_out.shape[1] // 4), BF16),
            pltpu.SemaphoreType.DMA((4,)),
        ],
        compiler_params=pltpu.CompilerParams(vmem_limit_bytes=67043328),
    )(o, w_out, lat, gate)


def on_device(
    latent, cond, cond_ctx, context, norm_gain, mod_shift, mod_scale, mod_gate,
    w_query, w_key, w_value, q_gain, k_gain, ctx_lift, w_out,
):
    lat = latent[0]
    at_owner, flags, o, l, q, kv_all, ctx, gate = run_attention(
        lat, cond, cond_ctx[None, :], context[0], norm_gain.reshape(-1, 128),
        mod_shift, mod_scale, mod_gate, w_query, w_key.T, w_value.T,
        q_gain[None, :], k_gain[None, :], ctx_lift,
    )

    def again(at_owner, o, l, q, kv_all, ctx):
        return run_exchange(run_repair(l, o, q, kv_all, ctx, ctx_lift))

    def keep(at_owner, *rest):
        return at_owner

    safe = jnp.max(flags) < 2.0**100
    at_owner = lax.cond(safe, keep, again, at_owner, o, l, q, kv_all, ctx)
    return run_output(at_owner, w_out, lat, gate)[None]


def solution(mesh):
    in_specs = (
        P("dp", ("sp", "tp"), None),
        P("dp", "sp"),
        P("sp"),
        P("dp", "sp", None),
        P(),
        P("sp", "tp"),
        P("sp", "tp"),
        P("sp", "tp"),
        P(None, "tp"),
        P(None, "tp"),
        P(None, "tp"),
        P(),
        P(),
        P("tp"),
        P(),
    )
    return jax.shard_map(
        on_device, mesh=mesh, in_specs=in_specs,
        out_specs=P("dp", ("sp", "tp"), None), check_vma=False,
    )
```

```python
import functools

import jax
import jax.numpy as jnp
import numpy as np
from jax import lax
from jax.experimental import pallas as pl
from jax.experimental.pallas import tpu as pltpu
from jax.sharding import PartitionSpec as P

MESH = pl.DeviceIdType.MESH
HD = 64
GRID_W = 128
EPS = 1e-06
THETA = 10000.0
LOG2E = 1.4426950408889634
N_SP = 16
N_TP = 4
F32 = jnp.float32
BF16 = jnp.bfloat16
VMEM = pl.BlockSpec(memory_space=pltpu.VMEM)
HBM = pl.BlockSpec(memory_space=pltpu.HBM)
SMEM = pl.BlockSpec(memory_space=pltpu.SMEM)


def angle_table():
    i = (np.arange(HD) // 2) % 16
    f = (THETA ** (-(i.astype(np.float32)) / np.float32(16))).astype(np.float32)
    return np.repeat(f[:, None], GRID_W, axis=1)


def tall(x):
    return jnp.concatenate([x, jnp.zeros_like(x)], axis=0)


PLACES = [
    (0, 0), (-1, 0), (1, 0), (0, -1), (0, 1), (2, 0), (-1, -1), (-1, 1),
    (1, -1), (1, 1), (0, 2), (2, -1), (2, 1), (-1, 2), (1, 2), (2, 2),
]
SENDS = [
    (0, 1, 1, 0), (0, 2, -1, 0), (0, 3, 0, 1), (0, 4, 0, -1),
    (1, 5, 1, 0), (1, 6, 0, 1), (1, 7, 0, -1),
    (2, 8, 0, 1), (2, 9, 0, -1),
    (3, 10, 0, 1),
    (5, 11, 0, 1), (5, 12, 0, -1),
    (7, 13, 0, -1), (8, 14, 0, 1), (12, 15, 0, -1),
]
MIRROR = [
    next(i for i, q in enumerate(PLACES) if (q[0] % 4, q[1] % 4) == (p[1] % 4, p[0] % 4))
    for p in PLACES
]
SENDS = [(h, t, dy, dz, 0) for h, t, dy, dz in SENDS] + [
    (MIRROR[h], MIRROR[t], dz, dy, 1) for h, t, dy, dz in SENDS
]
TILE = 1536
NARROW = 512
VROWS = 80
FIRST = 7
UNITS = 32
RETURNS = [(2, 576, 0, 192), (3, 384, 96, 96), (1, 480, 0, 96), (3, 192, 0, 96), (1, 288, 96, 96)]


def attention_kernel(
    lat_hbm, ctx_hbm, ms_hbm, mc_hbm, mg_hbm, wq_hbm, wk_hbm, wv_hbm,
    cond, condc, gain, qg, kg, table, lift,
    rows_out, flag_out, o_out, l_out, q_all, kv_all, ctx_all, gate_out,
    xbuf, part, psum_in, mine, full, wall, ubuf, raw, cosb, sinb, scl, sft, cbuf,
    q_out, kvbuf, acc, peak, p_even, p_odd, lat, ctx, m_shift, m_scale, m_gate, wq, wk, wv, load_sem,
    x_send, x_recv, p_send, p_recv, t_send, t_recv, c_send, c_recv, kv_send, kv_recv, keep_sem,
    obuf, fbuf, flag, o_send, o_recv, f_send, f_recv,
):
    sp = lax.axis_index("sp")
    tp = lax.axis_index("tp")
    y, z = lax.rem(sp, 4), lax.div(sp, 4)
    rows, width = lat.shape
    half = rows // 2

    def sp_at(k):
        return {"sp": lax.rem(sp + k, N_SP)}

    def tp_at(k):
        return {"tp": lax.rem(tp + k, N_TP)}

    def near(dy, dz):
        return {"sp": lax.rem(z + dz + 4, 4) * 4 + lax.rem(y + dy + 4, 4)}

    barrier = pltpu.get_barrier_semaphore()
    for k in range(1, N_SP):
        pl.semaphore_signal(barrier, inc=1, device_id=sp_at(k), device_id_type=MESH)
    for k in range(1, N_TP):
        pl.semaphore_signal(barrier, inc=1, device_id=tp_at(k), device_id_type=MESH)
    pairs = zip(
        (ms_hbm, mc_hbm, mg_hbm, lat_hbm, ctx_hbm, wq_hbm, wk_hbm, wv_hbm),
        (m_shift, m_scale, m_gate, lat, ctx, wq, wk, wv),
    )
    loads = [pltpu.make_async_copy(a, b, load_sem.at[i]) for i, (a, b) in enumerate(pairs)]
    for load in loads:
        load.start()
    pl.semaphore_wait(barrier, N_SP - 1 + N_TP - 1)

    def send(src, dst, s_sem, r_sem, target):
        return pltpu.make_async_remote_copy(
            src_ref=src, dst_ref=dst, send_sem=s_sem, recv_sem=r_sem,
            device_id=target, device_id_type=MESH,
        )

    def x_copy(i, src, to_row, count, k):
        return send(src, xbuf.at[pl.ds(to_row, count)], x_send.at[i], x_recv.at[i], tp_at(k))

    ra = x_copy(0, lat_hbm.at[pl.ds(0, 64)], 0, 64, 1)
    la = x_copy(1, lat_hbm.at[pl.ds(half, 64)], 96, 64, 3)
    rb = x_copy(2, lat_hbm.at[pl.ds(64, 32)], 64, 32, 1)
    lb = x_copy(3, lat_hbm.at[pl.ds(half + 64, 32)], 160, 32, 3)
    rc = x_copy(4, lat_hbm.at[pl.ds(half, half)], 192, half, 1)
    lc = x_copy(5, lat_hbm.at[pl.ds(0, half)], 288, half, 3)
    rf = x_copy(6, xbuf.at[pl.ds(0, half)], 384, half, 1)
    lf = x_copy(7, xbuf.at[pl.ds(half, half)], 480, half, 3)
    x_copies = [ra, la, rb, lb, rc, lc, rf, lf]
    ra.start()
    la.start()

    at = lax.broadcasted_iota(jnp.int32, (16, 128), 0)
    given = jnp.where(
        at == 0,
        jnp.broadcast_to(cond[...].astype(F32), (16, 128)),
        jnp.where(at == 1, jnp.broadcast_to(condc[...].astype(F32), (16, 128)), 0.0),
    )
    for load in loads[0:3]:
        load.wait()
    active = (given / (1.0 + jnp.exp(-given))).astype(BF16)
    for k, weight in enumerate((m_shift, m_scale, m_gate)):
        product = jnp.dot(active, weight[...], preferred_element_type=F32)
        for r in range(2):
            for c in range(4):
                i = r * 12 + k * 4 + c
                part[i : i + 1, :] = product[r : r + 1, c * 128 : (c + 1) * 128]
    p_copies = [
        send(part, psum_in.at[k - 1], p_send.at[k - 1], p_recv.at[k - 1], sp_at(k))
        for k in range(1, N_SP)
    ]
    for copy in p_copies:
        copy.start()

    for load in loads[3:]:
        load.wait()
    wall[:, 0:256] = wq[...]
    wall[:, 256:384] = jnp.concatenate([wk[...], wv[...]], axis=0).T

    for copy in p_copies:
        copy.wait_recv()
    total = part[...]
    for k in range(N_SP - 1):
        total = total + psum_in[k]
    mine[...] = total
    full[tp] = total
    t_copies = [
        send(mine, full.at[tp], t_send.at[k - 1], t_recv.at[k - 1], tp_at(k))
        for k in range(1, N_TP)
    ]
    for copy in t_copies:
        copy.start()
    for copy in (rb, lb, rc, lc):
        copy.start()

    row_id = lax.broadcasted_iota(jnp.int32, (HD, GRID_W), 0)
    lane_id = lax.broadcasted_iota(jnp.int32, (HD, GRID_W), 1)
    even = lax.rem(row_id, 2) == 0
    left, right, opposite = (lax.rem(tp + k, N_TP) * rows for k in (3, 1, 2))
    for g in range(6):
        n = lane_id + g * 128
        shift = jnp.where(
            n < 192,
            tp * rows,
            jnp.where(
                n < 288,
                left - 192,
                jnp.where(
                    n < 384,
                    right - 192,
                    jnp.where(
                        n < 480,
                        left - 288,
                        jnp.where(n < 576, right - 480, opposite - 576),
                    ),
                ),
            ),
        )
        at_token = n + shift + sp * 768
        grid_at = jnp.where(row_id < 32, at_token >> 7, at_token & 127)
        angle = table[...] * grid_at.astype(F32)
        cosb[g] = jnp.cos(angle)
        sine = jnp.sin(angle)
        sinb[g] = jnp.where(even, -sine, sine)

    for copy in t_copies:
        copy.wait_recv()

    def vector(r, k):
        pieces = [
            full[t, r * 12 + k * 4 + c : r * 12 + k * 4 + c + 1, :]
            for t in range(N_TP)
            for c in range(4)
        ]
        return jnp.concatenate(pieces, axis=1)

    gains = gain[...].astype(F32)
    gains = jnp.concatenate([gains[i : i + 1, :] for i in range(width // 128)], axis=1)
    for r in range(2):
        scl[r] = jnp.broadcast_to(gains * (1.0 + vector(r, 1)), (8, width))
        sft[r] = jnp.broadcast_to(vector(r, 0), (8, width))
    gate_out[...] = vector(0, 2)

    def modulate(src, r, count):
        values = src.astype(F32)
        inverse = lax.rsqrt(jnp.mean(values * values, axis=-1, keepdims=True) + EPS)
        normed = (values * inverse).reshape(count // 8, 8, width)
        return (normed * scl[r][None] + sft[r][None]).reshape(count, width).astype(BF16)

    uc = modulate(ctx[...], 1, ctx.shape[0])
    craw = jnp.dot(uc, wall[:, 256:384], preferred_element_type=F32)
    lane = lax.broadcasted_iota(jnp.int32, craw.shape, 1)
    square = jnp.where(lane < HD, craw * craw, 0.0)
    mean = jnp.sum(square, axis=-1, keepdims=True) * (1.0 / HD)
    k_row = kg[...].astype(F32)
    keys = craw * lax.rsqrt(mean + EPS) * jnp.concatenate([k_row, jnp.ones((1, HD), F32)], axis=1)
    cbuf[pl.ds(0, 32), :] = jnp.where(lane < HD, keys, craw).astype(BF16)

    def project(x, first, to_row, between=None):
        @pl.loop(0, rows // 32)
        def _(i):
            at_rows = pl.ds(pl.multiple_of(i * 32, 32), 32)
            from_rows = pl.ds(pl.multiple_of(first + i * 32, 32), 32)
            ubuf[at_rows, :] = modulate(x[from_rows, :], 0, 32)

        if between is not None:
            between()
        raw[pl.ds(to_row, rows), :] = jnp.dot(ubuf[...], wall[...], preferred_element_type=F32)

    def column(ref):
        r = lax.broadcasted_iota(jnp.int32, (HD, HD), 0)
        c = lax.broadcasted_iota(jnp.int32, (HD, HD), 1)
        spread = jnp.broadcast_to(ref[...].astype(F32), (HD, HD))
        return jnp.sum(jnp.where(r == c, spread, 0.0), axis=1, keepdims=True)

    q_gain = column(qg)
    k_gain = column(kg)

    def turned(x, gain_column, g):
        square = jnp.sum(x * x, axis=0, keepdims=True) * (1.0 / HD)
        normed = x * lax.rsqrt(square + EPS) * gain_column
        up = pltpu.roll(normed, HD - 1, axis=0)
        down = pltpu.roll(normed, 1, axis=0)
        return normed * cosb[g] + jnp.where(even, up, down) * sinb[g]

    scale = LOG2E * HD ** (-0.5)

    def finish_kv(s):
        slot = s * N_SP
        for i in range(3):
            g = 3 * s + i
            side = raw[g * 128 : (g + 1) * 128, 256:384].T
            k = turned(side[0:HD], k_gain, g).T
            kvbuf[slot, i * 64 : (i + 1) * 64, :] = jnp.concatenate(
                [k[0:64], k[64:128]], axis=1
            ).astype(BF16)
        order = [(g, p) for p in range(2) for g in (3 * s, 3 * s + 1, 3 * s + 2)]
        for b in range(3):
            pieces = [
                raw[g * 128 + p * 64 : g * 128 + p * 64 + 64, 256:384]
                for g, p in order[2 * b : 2 * b + 2]
            ]
            side = jnp.concatenate(pieces, axis=0).T
            at_row = 192 + b * 64
            kvbuf[slot, at_row : at_row + 64, :] = side[HD : 2 * HD].astype(BF16)

    def finish_q(blocks):
        for g in blocks:
            block = raw[g * 128 : (g + 1) * 128, :]
            for pair in range(2):
                side = block[:, pair * 128 : (pair + 1) * 128].T
                for h in range(2):
                    q = turned(side[h * HD : (h + 1) * HD], q_gain, g)
                    at_lane = g * 512 + (pair * 2 + h) * 128
                    q_out[:, at_lane : at_lane + 128] = (q * scale).astype(BF16)

    kv_copies = [[], []]
    for s in range(2):
        for i, (here, there, dy, dz, part_of) in enumerate(SENDS):
            here, there = here + s * N_SP, there + s * N_SP
            half_of = pl.ds(192 * part_of, 192)
            kv_copies[s].append(
                send(
                    kvbuf.at[here, half_of], kvbuf.at[there, half_of],
                    kv_send.at[i + s * len(SENDS)], kv_recv.at[2 * there + part_of], near(dy, dz),
                )
            )

    def start_from(s, slot):
        for copy, (here, _, _, _, _) in zip(kv_copies[s], SENDS):
            if here == slot:
                copy.start()

    def keep(s, slot):
        slot = slot + s * N_SP
        return pltpu.make_async_copy(kvbuf.at[slot], kv_all.at[slot], keep_sem.at[slot])

    def arrive(s, slot):
        for copy, (_, there, _, _, _) in zip(kv_copies[s], SENDS):
            if there == slot:
                copy.wait_recv()
        start_from(s, slot)
        keep(s, slot).start()

    lifts = jnp.concatenate([jnp.full((1, 128), lift[h] * LOG2E, F32) for h in range(4)], axis=1)
    lifts = jnp.concatenate([lifts] * (TILE // 512), axis=1)
    ones = jnp.ones((VROWS - HD, 768), BF16)

    def lanes(t):
        if isinstance(t, int):
            return pl.ds(t * TILE, TILE)
        return pl.ds(pl.multiple_of(t * TILE, TILE), TILE)

    def narrow(t, n):
        start = t * TILE + n * NARROW
        return pl.ds(start if isinstance(t, int) else pl.multiple_of(start, NARROW), NARROW)

    def context(t):
        cv = cbuf[...].astype(F32).T[HD : 2 * HD].astype(BF16)
        cv = jnp.concatenate([cv, ones[:, 0:512]], axis=0)
        scores = jnp.dot(cbuf[...], tall(q_out[:, lanes(t)]), preferred_element_type=F32) + lifts
        top = jnp.max(scores, axis=0, keepdims=True)
        peak[:, lanes(t)] = top
        weights = jnp.exp2(scores - top).astype(BF16)
        acc[:, lanes(t)] = jnp.dot(cv, weights, preferred_element_type=F32)

    def query_forms(at_lanes):
        q = q_out[:, at_lanes]
        return tall(q), jnp.concatenate([jnp.zeros_like(q), q], axis=0)

    def values_of(pair):
        v = [kvbuf[pair * 2 + s, pl.ds(192 + i * 64, 64), :] for s in range(2) for i in range(3)]
        return jnp.concatenate([jnp.concatenate(v, axis=1), ones], axis=0)

    def work(now, then, read, write):
        if now is not None:
            v = values_of(now[0])
        for n in range(TILE // NARROW):
            cols = slice(n * NARROW, (n + 1) * NARROW)
            if then is not None:
                theirs = narrow(then[1], n)
                forms = query_forms(theirs)
                top = peak[:, theirs]
            total = None
            for i in range(4):
                if then is not None:
                    s, p = i % 2, i // 2
                    k = kvbuf[then[0] * 2 + s, pl.ds(0, 192), :]
                    x = jnp.dot(k, forms[p], preferred_element_type=F32)
                    write[pl.ds(s * 384 + p * 192, 192), cols] = jnp.exp2(x - top).astype(BF16)
                if now is not None and i < 3:
                    term = jnp.dot(
                        v[:, i * 256 : (i + 1) * 256], read[pl.ds(i * 256, 256), cols],
                        preferred_element_type=F32,
                    )
                    total = term if total is None else total + term
            if now is not None:
                acc[:, narrow(now[1], n)] += total

    def unit(j):
        pair = jnp.where(
            j < 2 * FIRST,
            j - FIRST,
            jnp.where(
                j < 16, FIRST + (j - 2 * FIRST) // 2, jnp.where(j < 24, j - 8, j - 16)
            ),
        )
        tile = jnp.where(
            j < 2 * FIRST, 1, jnp.where(j < 16, lax.rem(j, 2), jnp.where(j < 24, 1, 0))
        )
        return pair, tile

    c_copies = [
        send(
            cbuf.at[pl.ds(0, 32)], cbuf.at[pl.ds(32 * k, 32)],
            c_send.at[k - 1], c_recv.at[k - 1], sp_at(k),
        )
        for k in range(1, N_SP)
    ]

    def start_context():
        for copy in c_copies:
            copy.start()

    project(lat, 0, 0, start_context)
    ra.wait_recv()
    rb.wait_recv()
    rf.start()
    la.wait_recv()
    lb.wait_recv()
    lf.start()
    project(xbuf, 0, 192)
    finish_kv(0)
    finish_q((0,))
    arrive(0, 0)
    finish_q((1, 2))
    for copy in c_copies:
        copy.wait_recv()
    context(0)
    arrive(0, 1)
    work(None, (0, 0), None, p_even)

    def first_step(d, carry):
        for pair in range(1, FIRST):

            @pl.when(d == (pair - 1) // 2)
            def _(pair=pair):
                arrive(0, 2 * pair)
                arrive(0, 2 * pair + 1)

        work((2 * d, 0), (2 * d + 1, 0), p_even, p_odd)
        work((2 * d + 1, 0), (2 * d + 2, 0), p_odd, p_even)
        return carry

    lax.fori_loop(0, FIRST // 2, first_step, 0)
    work((FIRST - 1, 0), None, p_even, None)

    rc.wait_recv()
    lc.wait_recv()
    project(xbuf, 192, 384)
    rf.wait_recv()
    lf.wait_recv()
    project(xbuf, 384, 576)
    finish_kv(1)
    finish_q((3,))
    arrive(1, 0)
    finish_q((4, 5))
    context(1)
    keep_rest = [
        pltpu.make_async_copy(q_out, q_all, keep_sem.at[2 * N_SP]),
        pltpu.make_async_copy(cbuf, ctx_all, keep_sem.at[2 * N_SP + 1]),
    ]
    for copy in keep_rest:
        copy.start()
    work(None, (0, 1), None, p_even)

    events = [(1, 0, (7,)), (2, 1, (0, 1)), (3, 1, (2,)), (4, 1, (3, 4)), (5, 1, (5,)),
              (6, 1, (6,)), (7, 1, (7,))]

    def second_step(d, carry):
        for when, s, pairs in events:

            @pl.when(d == when)
            def _(s=s, pairs=pairs):
                for pair in pairs:
                    for slot in (2 * pair, 2 * pair + 1):
                        if slot > 0:
                            arrive(s, slot)

        j = FIRST + 2 * d
        work(unit(j), unit(j + 1), p_even, p_odd)
        work(unit(j + 1), unit(j + 2), p_odd, p_even)
        return carry

    returns = [
        send(
            o_out.at[pl.ds(here, count)], obuf.at[tp, pl.ds(there, count)],
            o_send.at[i], o_recv.at[i], tp_at(k),
        )
        for i, (k, here, there, count) in enumerate(RETURNS)
    ]

    def finish_o(blocks):
        for g in blocks:
            at_lanes = pl.ds(g * 512, 512)
            mean = acc[0:HD, at_lanes] / acc[HD : HD + 1, at_lanes]
            stack = jnp.concatenate([mean[:, h * 128 : (h + 1) * 128] for h in range(4)], axis=0)
            o_out[g * 128 : (g + 1) * 128, :] = stack.T.astype(BF16)

    steps = (UNITS - 1 - FIRST) // 2
    lax.fori_loop(0, steps - 3, second_step, 0)
    finish_o((3, 4, 5))
    lax.fori_loop(steps - 3, steps - 2, second_step, 0)
    for copy, (_, here, _, _) in zip(returns, RETURNS):
        if here >= 384:
            copy.start()
    lax.fori_loop(steps - 2, steps, second_step, 0)
    work((15, 0), None, p_even, None)
    finish_o((1, 2))
    l_out[...] = acc[HD : HD + 8, :]
    peaks = acc[HD : HD + 1, 0:128]
    for i in range(1, 24):
        peaks = jnp.maximum(peaks, acc[HD : HD + 1, i * 128 : (i + 1) * 128])
    flag[...] = jnp.broadcast_to(peaks, (8, 128))
    fbuf[tp] = flag[...]
    finish_o((0,))
    for copy, (_, here, _, _) in zip(returns, RETURNS):
        if here < 384:
            copy.start()
    flags = [
        send(flag, fbuf.at[tp], f_send.at[k - 1], f_recv.at[k - 1], tp_at(k))
        for k in range(1, N_TP)
    ]
    for copy in flags:
        copy.start()
    rows_out[tp] = o_out[0:rows, :]
    for copy in returns + flags:
        copy.wait_recv()
    for k in range(1, N_TP):
        source = lax.rem(tp + k, N_TP)
        rows_out[source] = obuf[source]
    flag_out[0] = (jnp.max(fbuf[...]) < 2.0**100).astype(jnp.int32)
    waiting = x_copies + p_copies + t_copies + c_copies + kv_copies[0] + kv_copies[1]
    for copy in waiting + returns + flags:
        copy.wait_send()
    for s in range(2):
        for slot in range(N_SP):
            keep(s, slot).wait()
    for copy in keep_rest:
        copy.wait()


def run_attention(lat, cond, condc, ctx, gain, ms, mc, mg, wq, wk, wv, qg, kg, lift):
    rows, width = lat.shape
    dma = pltpu.SemaphoreType.DMA
    loaded = (lat, ctx, ms, mc, mg, wq, wk, wv)
    return pl.pallas_call(
        attention_kernel,
        name="attention",
        out_shape=(
            jax.ShapeDtypeStruct((N_TP, rows, 256), BF16),
            jax.ShapeDtypeStruct((1,), jnp.int32),
            jax.ShapeDtypeStruct((768, 256), BF16),
            jax.ShapeDtypeStruct((8, 3072), F32),
            jax.ShapeDtypeStruct((HD, 3072), BF16),
            jax.ShapeDtypeStruct((2 * N_SP, 384, 128), BF16),
            jax.ShapeDtypeStruct((512, 128), BF16),
            jax.ShapeDtypeStruct((1, width), F32),
        ),
        in_specs=[HBM] * 8 + [VMEM] * 6 + [SMEM],
        out_specs=(VMEM, SMEM, VMEM, VMEM, HBM, HBM, HBM, VMEM),
        scratch_shapes=[
            pltpu.VMEM((3 * rows, width), BF16),
            pltpu.VMEM((24, 128), F32),
            pltpu.VMEM((N_SP - 1, 24, 128), F32),
            pltpu.VMEM((24, 128), F32),
            pltpu.VMEM((N_TP, 24, 128), F32),
            pltpu.VMEM((width, 384), BF16),
            pltpu.VMEM((rows, width), BF16),
            pltpu.VMEM((768, 384), F32),
            pltpu.VMEM((6, HD, GRID_W), F32),
            pltpu.VMEM((6, HD, GRID_W), F32),
            pltpu.VMEM((2, 8, width), F32),
            pltpu.VMEM((2, 8, width), F32),
            pltpu.VMEM((512, 128), BF16),
            pltpu.VMEM((HD, 3072), BF16),
            pltpu.VMEM((2 * N_SP, 384, 128), BF16),
            pltpu.VMEM((VROWS, 3072), F32),
            pltpu.VMEM((1, 3072), F32),
            pltpu.VMEM((768, TILE), BF16),
            pltpu.VMEM((768, TILE), BF16),
            *[pltpu.VMEM(a.shape, BF16) for a in loaded],
            dma((len(loaded),)),
            dma((8,)), dma((8,)), dma((15,)), dma((15,)),
            dma((3,)), dma((3,)), dma((15,)), dma((15,)),
            dma((2 * len(SENDS),)), dma((4 * N_SP,)), dma((2 * N_SP + 2,)),
            pltpu.VMEM((N_TP, rows, 256), BF16),
            pltpu.VMEM((N_TP, 8, 128), F32),
            pltpu.VMEM((8, 128), F32),
            dma((len(RETURNS),)), dma((len(RETURNS),)), dma((N_TP - 1,)), dma((N_TP - 1,)),
        ],
        compiler_params=pltpu.CompilerParams(
            collective_id=0, has_side_effects=True, vmem_limit_bytes=67043328
        ),
        cost_estimate=pl.CostEstimate(
            flops=2 * 10**10, bytes_accessed=10**7, transcendentals=4 * 10**7
        ),
    )(
        *loaded, cond, condc, gain, qg, kg, jnp.asarray(angle_table()), lift,
    )


def repair_kernel(
    l_ref, o_in, q_hbm, kv_hbm, ctx_hbm, lift, o_out,
    q_ref, kvbuf, ctx, acc, peak, sem,
):
    safe = jnp.all(l_ref[...] < 2.0**100)
    o_out[...] = o_in[...]

    @pl.when(jnp.logical_not(safe))
    def _():
        for src, dst in ((q_hbm, q_ref), (kv_hbm, kvbuf), (ctx_hbm, ctx)):
            copy = pltpu.make_async_copy(src, dst, sem)
            copy.start()
            copy.wait()
        wide = 512
        ones = jnp.ones((VROWS - HD, 768), BF16)
        lifts = jnp.concatenate(
            [jnp.full((1, 128), lift[h] * LOG2E, F32) for h in range(4)], axis=1
        )
        cv = ctx[...].astype(F32).T[HD : 2 * HD].astype(BF16)
        cv = jnp.concatenate([cv, ones[:, 0:512]], axis=0)

        @pl.loop(0, q_ref.shape[1] // wide)
        def _(t):
            lanes = pl.ds(pl.multiple_of(t * wide, wide), wide)
            q = q_ref[:, lanes]
            left = tall(q)
            right = jnp.concatenate([jnp.zeros_like(q), q], axis=0)
            scores = jnp.dot(ctx[...], left, preferred_element_type=F32) + lifts
            top = jnp.max(scores, axis=0, keepdims=True)
            peak[...] = top
            weights = jnp.exp2(scores - top).astype(BF16)
            acc[...] = jnp.dot(cv, weights, preferred_element_type=F32)

            @pl.loop(0, N_SP)
            def _(b):
                parts = []
                for s in range(2):
                    k = kvbuf[b * 2 + s, pl.ds(0, 192), :]
                    for query in (left, right):
                        parts.append(jnp.dot(k, query, preferred_element_type=F32))
                x = jnp.concatenate(parts, axis=0)
                old = peak[...]
                new = jnp.maximum(old, jnp.max(x, axis=0, keepdims=True))
                peak[...] = new
                v = [
                    kvbuf[b * 2 + s, pl.ds(192 + i * 64, 64), :] for s in range(2) for i in range(3)
                ]
                v = jnp.concatenate([jnp.concatenate(v, axis=1), ones], axis=0)
                weights = jnp.exp2(x - new).astype(BF16)
                acc[...] = acc[...] * jnp.exp2(old - new) + jnp.dot(
                    v, weights, preferred_element_type=F32
                )

            mean = acc[0:HD, :] / acc[HD : HD + 1, :]
            stack = jnp.concatenate([mean[:, h * 128 : (h + 1) * 128] for h in range(4)], axis=0)
            rows = pl.ds(pl.multiple_of(t * 128, 128), 128)
            o_out[rows, :] = stack.T.astype(BF16)


def run_repair(l, o, q, kv_all, ctx, lift):
    return pl.pallas_call(
        repair_kernel,
        name="repair",
        out_shape=jax.ShapeDtypeStruct(o.shape, o.dtype),
        in_specs=[VMEM, VMEM, HBM, HBM, HBM, SMEM],
        out_specs=VMEM,
        scratch_shapes=[
            pltpu.VMEM((HD, 3072), BF16),
            pltpu.VMEM((2 * N_SP, 384, 128), BF16),
            pltpu.VMEM((512, 128), BF16),
            pltpu.VMEM((VROWS, 512), F32),
            pltpu.VMEM((1, 512), F32),
            pltpu.SemaphoreType.DMA(()),
        ],
        compiler_params=pltpu.CompilerParams(vmem_limit_bytes=67043328),
    )(l, o, q, kv_all, ctx, lift)


def exchange_kernel(o_ref, out, obuf, send_sem, recv_sem):
    tp = lax.axis_index("tp")
    rows = o_ref.shape[0] // N_TP

    def tp_at(k):
        return {"tp": lax.rem(tp + k, N_TP)}

    barrier = pltpu.get_barrier_semaphore()
    for k in range(1, N_TP):
        pl.semaphore_signal(barrier, inc=1, device_id=tp_at(k), device_id_type=MESH)
    pl.semaphore_wait(barrier, N_TP - 1)
    copies = []
    for i, (k, here, there, count) in enumerate(RETURNS):
        copies.append(
            pltpu.make_async_remote_copy(
                src_ref=o_ref.at[pl.ds(here, count)],
                dst_ref=obuf.at[tp, pl.ds(there, count)],
                send_sem=send_sem.at[i], recv_sem=recv_sem.at[i],
                device_id=tp_at(k), device_id_type=MESH,
            )
        )
        copies[-1].start()
    out[tp] = o_ref[0:rows, :]
    for copy in copies:
        copy.wait_recv()
    for k in range(1, N_TP):
        source = lax.rem(tp + k, N_TP)
        out[source] = obuf[source]
    for copy in copies:
        copy.wait_send()


def run_exchange(o):
    rows = o.shape[0] // N_TP
    dma = pltpu.SemaphoreType.DMA
    return pl.pallas_call(
        exchange_kernel,
        name="exchange",
        out_shape=jax.ShapeDtypeStruct((N_TP, rows, 256), BF16),
        in_specs=[VMEM],
        out_specs=VMEM,
        scratch_shapes=[pltpu.VMEM((N_TP, rows, 256), BF16), dma((5,)), dma((5,))],
        compiler_params=pltpu.CompilerParams(
            collective_id=2, has_side_effects=True, vmem_limit_bytes=4 * 2**20
        ),
        cost_estimate=pl.CostEstimate(flops=0, bytes_accessed=25 * 10**6, transcendentals=0),
    )(o)


def output_kernel(o_hbm, w_hbm, lat_hbm, gate, out, o, w, lat, total, sem):
    pairs = [(o_hbm, o)]
    pairs += [(w_hbm.at[pl.ds(t * 256, 256)], w.at[t]) for t in range(N_TP)]
    pairs += [(lat_hbm, lat)]
    loads = [pltpu.make_async_copy(a, b, sem.at[i]) for i, (a, b) in enumerate(pairs)]
    for load in loads:
        load.start()
    loads[0].wait()
    wide = 512
    for t in range(N_TP):
        loads[1 + t].wait()
        if t == N_TP - 1:
            loads[-1].wait()
        for n in range(out.shape[1] // wide):
            cols = slice(n * wide, (n + 1) * wide)
            term = jnp.dot(o[t], w[t, :, cols], preferred_element_type=F32)
            if t == 0:
                total[:, cols] = term
            elif t < N_TP - 1:
                total[:, cols] += term
            else:
                term = total[:, cols] + term
                out[:, cols] = (lat[:, cols].astype(F32) + gate[:, cols] * term).astype(BF16)


def run_output(o, w_out, lat, gate):
    return pl.pallas_call(
        output_kernel,
        name="output",
        out_shape=jax.ShapeDtypeStruct(lat.shape, BF16),
        in_specs=[HBM, HBM, HBM, VMEM],
        out_specs=VMEM,
        scratch_shapes=[
            pltpu.VMEM(o.shape, BF16),
            pltpu.VMEM((N_TP, 256, w_out.shape[1]), BF16),
            pltpu.VMEM(lat.shape, BF16),
            pltpu.VMEM(lat.shape, F32),
            pltpu.SemaphoreType.DMA((N_TP + 2,)),
        ],
        compiler_params=pltpu.CompilerParams(vmem_limit_bytes=67043328),
    )(o, w_out, lat, gate)


def on_device(
    latent, cond, cond_ctx, context, norm_gain, mod_shift, mod_scale, mod_gate,
    w_query, w_key, w_value, q_gain, k_gain, ctx_lift, w_out,
):
    lat = latent[0]
    at_owner, safe, o, l, q, kv_all, ctx, gate = run_attention(
        lat, cond, cond_ctx[None, :], context[0], norm_gain.reshape(-1, 128),
        mod_shift, mod_scale, mod_gate, w_query, w_key.T, w_value.T,
        q_gain[None, :], k_gain[None, :], ctx_lift,
    )

    def again(at_owner, o, l, q, kv_all, ctx):
        return run_exchange(run_repair(l, o, q, kv_all, ctx, ctx_lift))

    def keep(at_owner, *rest):
        return at_owner

    at_owner = lax.cond(safe[0] > 0, keep, again, at_owner, o, l, q, kv_all, ctx)
    return run_output(at_owner, w_out, lat, gate)[None]


def solution(mesh):
    in_specs = (
        P("dp", ("sp", "tp"), None),
        P("dp", "sp"),
        P("sp"),
        P("dp", "sp", None),
        P(),
        P("sp", "tp"),
        P("sp", "tp"),
        P("sp", "tp"),
        P(None, "tp"),
        P(None, "tp"),
        P(None, "tp"),
        P(),
        P(),
        P("tp"),
        P(),
    )
    return jax.shard_map(
        on_device, mesh=mesh, in_specs=in_specs,
        out_specs=P("dp", ("sp", "tp"), None), check_vma=False,
    )
```

```python
import functools

import jax
import jax.numpy as jnp
import numpy as np
from jax import lax
from jax.experimental import pallas as pl
from jax.experimental.pallas import tpu as pltpu
from jax.sharding import PartitionSpec as P

MESH = pl.DeviceIdType.MESH
HD = 64
GRID_W = 128
EPS = 1e-06
THETA = 10000.0
LOG2E = 1.4426950408889634
N_SP = 16
N_TP = 4
F32 = jnp.float32
BF16 = jnp.bfloat16
VMEM = pl.BlockSpec(memory_space=pltpu.VMEM)
HBM = pl.BlockSpec(memory_space=pltpu.HBM)
SMEM = pl.BlockSpec(memory_space=pltpu.SMEM)


def angle_table():
    i = (np.arange(HD) // 2) % 16
    f = (THETA ** (-(i.astype(np.float32)) / np.float32(16))).astype(np.float32)
    return np.repeat(f[:, None], GRID_W, axis=1)


def tall(x):
    return jnp.concatenate([x, jnp.zeros_like(x)], axis=0)


PLACES = [
    (0, 0), (-1, 0), (1, 0), (0, -1), (0, 1), (2, 0), (0, 2), (-1, -1),
    (-1, 1), (1, -1), (1, 1), (2, 1), (1, 2), (2, -1), (-1, 2), (2, 2),
]
SENDS = [
    (0, 1, 1, 0), (0, 2, -1, 0), (0, 3, 0, 1), (0, 4, 0, -1),
    (1, 5, 1, 0), (1, 7, 0, 1), (1, 8, 0, -1),
    (2, 9, 0, 1), (2, 10, 0, -1),
    (3, 6, 0, 1),
    (5, 11, 0, -1), (5, 13, 0, 1),
    (8, 14, 0, -1), (9, 12, 0, 1), (11, 15, 0, -1),
]
MIRROR = [
    next(i for i, q in enumerate(PLACES) if (q[0] % 4, q[1] % 4) == (p[1] % 4, p[0] % 4))
    for p in PLACES
]
SENDS = [(h, t, dy, dz, 0) for h, t, dy, dz in SENDS] + [
    (MIRROR[h], MIRROR[t], dz, dy, 1) for h, t, dy, dz in SENDS
]
TILE = 1536
NARROW = 512
VROWS = 80
FIRST = 7
UNITS = 32
RETURNS = [(2, 576, 0, 192), (3, 384, 96, 96), (1, 480, 0, 96), (3, 192, 0, 96), (1, 288, 96, 96)]


def attention_kernel(
    lat_hbm, ctx_hbm, ms_hbm, mc_hbm, mg_hbm, wq_hbm, wk_hbm, wv_hbm, w_hbm,
    cond, condc, gain, qg, kg, table, lift,
    mixed_out, flag_out, o_out, l_out, q_all, kv_all, ctx_all, gate_out,
    xbuf, part, psum_in, mine, full, wall, ubuf, raw, cosb, sinb, scl, sft, cbuf,
    q_out, kvbuf, acc, peak, p_even, p_odd, lat, ctx, m_shift, m_scale, m_gate, wq, wk, wv, load_sem,
    x_send, x_recv, p_send, p_recv, t_send, t_recv, c_send, c_recv, kv_send, kv_recv, keep_sem,
    obuf, fbuf, flag, w, w_sem, summed, o_send, o_recv, f_send, f_recv,
):
    sp = lax.axis_index("sp")
    tp = lax.axis_index("tp")
    y, z = lax.rem(sp, 4), lax.div(sp, 4)
    rows, width = lat.shape
    half = rows // 2

    def sp_at(k):
        return {"sp": lax.rem(sp + k, N_SP)}

    def tp_at(k):
        return {"tp": lax.rem(tp + k, N_TP)}

    def near(dy, dz):
        return {"sp": lax.rem(z + dz + 4, 4) * 4 + lax.rem(y + dy + 4, 4)}

    barrier = pltpu.get_barrier_semaphore()
    for k in range(1, N_SP):
        pl.semaphore_signal(barrier, inc=1, device_id=sp_at(k), device_id_type=MESH)
    for k in range(1, N_TP):
        pl.semaphore_signal(barrier, inc=1, device_id=tp_at(k), device_id_type=MESH)
    pairs = zip(
        (ms_hbm, mc_hbm, mg_hbm, lat_hbm, ctx_hbm, wq_hbm, wk_hbm, wv_hbm),
        (m_shift, m_scale, m_gate, lat, ctx, wq, wk, wv),
    )
    loads = [pltpu.make_async_copy(a, b, load_sem.at[i]) for i, (a, b) in enumerate(pairs)]
    for load in loads:
        load.start()
    pl.semaphore_wait(barrier, N_SP - 1 + N_TP - 1)

    def send(src, dst, s_sem, r_sem, target):
        return pltpu.make_async_remote_copy(
            src_ref=src, dst_ref=dst, send_sem=s_sem, recv_sem=r_sem,
            device_id=target, device_id_type=MESH,
        )

    def x_copy(i, src, to_row, count, k):
        return send(src, xbuf.at[pl.ds(to_row, count)], x_send.at[i], x_recv.at[i], tp_at(k))

    ra = x_copy(0, lat_hbm.at[pl.ds(0, 64)], 0, 64, 1)
    la = x_copy(1, lat_hbm.at[pl.ds(half, 64)], 96, 64, 3)
    rb = x_copy(2, lat_hbm.at[pl.ds(64, 32)], 64, 32, 1)
    lb = x_copy(3, lat_hbm.at[pl.ds(half + 64, 32)], 160, 32, 3)
    rc = x_copy(4, lat_hbm.at[pl.ds(half, half)], 192, half, 1)
    lc = x_copy(5, lat_hbm.at[pl.ds(0, half)], 288, half, 3)
    rf = x_copy(6, xbuf.at[pl.ds(0, half)], 384, half, 1)
    lf = x_copy(7, xbuf.at[pl.ds(half, half)], 480, half, 3)
    x_copies = [ra, la, rb, lb, rc, lc, rf, lf]
    ra.start()
    la.start()

    at = lax.broadcasted_iota(jnp.int32, (16, 128), 0)
    given = jnp.where(
        at == 0,
        jnp.broadcast_to(cond[...].astype(F32), (16, 128)),
        jnp.where(at == 1, jnp.broadcast_to(condc[...].astype(F32), (16, 128)), 0.0),
    )
    for load in loads[0:3]:
        load.wait()
    active = (given / (1.0 + jnp.exp(-given))).astype(BF16)
    for k, weight in enumerate((m_shift, m_scale, m_gate)):
        product = jnp.dot(active, weight[...], preferred_element_type=F32)
        for r in range(2):
            for c in range(4):
                i = r * 12 + k * 4 + c
                part[i : i + 1, :] = product[r : r + 1, c * 128 : (c + 1) * 128]
    p_copies = [
        send(part, psum_in.at[k - 1], p_send.at[k - 1], p_recv.at[k - 1], sp_at(k))
        for k in range(1, N_SP)
    ]
    for copy in p_copies:
        copy.start()

    for load in loads[3:]:
        load.wait()
    wall[:, 0:256] = wq[...]
    wall[:, 256:384] = jnp.concatenate([wk[...], wv[...]], axis=0).T

    for copy in p_copies:
        copy.wait_recv()
    total = part[...]
    for k in range(N_SP - 1):
        total = total + psum_in[k]
    mine[...] = total
    full[tp] = total
    t_copies = [
        send(mine, full.at[tp], t_send.at[k - 1], t_recv.at[k - 1], tp_at(k))
        for k in range(1, N_TP)
    ]
    for copy in t_copies:
        copy.start()
    for copy in (rb, lb, rc, lc):
        copy.start()

    row_id = lax.broadcasted_iota(jnp.int32, (HD, GRID_W), 0)
    lane_id = lax.broadcasted_iota(jnp.int32, (HD, GRID_W), 1)
    even = lax.rem(row_id, 2) == 0
    left, right, opposite = (lax.rem(tp + k, N_TP) * rows for k in (3, 1, 2))
    for g in range(6):
        n = lane_id + g * 128
        shift = jnp.where(
            n < 192,
            tp * rows,
            jnp.where(
                n < 288,
                left - 192,
                jnp.where(
                    n < 384,
                    right - 192,
                    jnp.where(
                        n < 480,
                        left - 288,
                        jnp.where(n < 576, right - 480, opposite - 576),
                    ),
                ),
            ),
        )
        at_token = n + shift + sp * 768
        grid_at = jnp.where(row_id < 32, at_token >> 7, at_token & 127)
        angle = table[...] * grid_at.astype(F32)
        cosb[g] = jnp.cos(angle)
        sine = jnp.sin(angle)
        sinb[g] = jnp.where(even, -sine, sine)

    w_load = pltpu.make_async_copy(w_hbm, w, w_sem)
    w_load.start()
    for copy in t_copies:
        copy.wait_recv()

    def vector(r, k):
        pieces = [
            full[t, r * 12 + k * 4 + c : r * 12 + k * 4 + c + 1, :]
            for t in range(N_TP)
            for c in range(4)
        ]
        return jnp.concatenate(pieces, axis=1)

    gains = gain[...].astype(F32)
    gains = jnp.concatenate([gains[i : i + 1, :] for i in range(width // 128)], axis=1)
    for r in range(2):
        scl[r] = jnp.broadcast_to(gains * (1.0 + vector(r, 1)), (8, width))
        sft[r] = jnp.broadcast_to(vector(r, 0), (8, width))
    gate_out[...] = vector(0, 2)

    def modulate(src, r, count):
        values = src.astype(F32)
        inverse = lax.rsqrt(jnp.mean(values * values, axis=-1, keepdims=True) + EPS)
        normed = (values * inverse).reshape(count // 8, 8, width)
        return (normed * scl[r][None] + sft[r][None]).reshape(count, width).astype(BF16)

    uc = modulate(ctx[...], 1, ctx.shape[0])
    craw = jnp.dot(uc, wall[:, 256:384], preferred_element_type=F32)
    lane = lax.broadcasted_iota(jnp.int32, craw.shape, 1)
    square = jnp.where(lane < HD, craw * craw, 0.0)
    mean = jnp.sum(square, axis=-1, keepdims=True) * (1.0 / HD)
    k_row = kg[...].astype(F32)
    keys = craw * lax.rsqrt(mean + EPS) * jnp.concatenate([k_row, jnp.ones((1, HD), F32)], axis=1)
    cbuf[pl.ds(0, 32), :] = jnp.where(lane < HD, keys, craw).astype(BF16)

    def project(x, first, to_row, between=None):
        @pl.loop(0, rows // 32)
        def _(i):
            at_rows = pl.ds(pl.multiple_of(i * 32, 32), 32)
            from_rows = pl.ds(pl.multiple_of(first + i * 32, 32), 32)
            ubuf[at_rows, :] = modulate(x[from_rows, :], 0, 32)

        if between is not None:
            between()
        raw[pl.ds(to_row, rows), :] = jnp.dot(ubuf[...], wall[...], preferred_element_type=F32)

    def column(ref):
        r = lax.broadcasted_iota(jnp.int32, (HD, HD), 0)
        c = lax.broadcasted_iota(jnp.int32, (HD, HD), 1)
        spread = jnp.broadcast_to(ref[...].astype(F32), (HD, HD))
        return jnp.sum(jnp.where(r == c, spread, 0.0), axis=1, keepdims=True)

    q_gain = column(qg)
    k_gain = column(kg)

    def turned(x, gain_column, g):
        square = jnp.sum(x * x, axis=0, keepdims=True) * (1.0 / HD)
        normed = x * lax.rsqrt(square + EPS) * gain_column
        up = pltpu.roll(normed, HD - 1, axis=0)
        down = pltpu.roll(normed, 1, axis=0)
        return normed * cosb[g] + jnp.where(even, up, down) * sinb[g]

    scale = LOG2E * HD ** (-0.5)

    def finish_kv(s):
        slot = s * N_SP
        for i in range(3):
            g = 3 * s + i
            side = raw[g * 128 : (g + 1) * 128, 256:384].T
            k = turned(side[0:HD], k_gain, g).T
            kvbuf[slot, i * 64 : (i + 1) * 64, :] = jnp.concatenate(
                [k[0:64], k[64:128]], axis=1
            ).astype(BF16)
        order = [(g, p) for p in range(2) for g in (3 * s, 3 * s + 1, 3 * s + 2)]
        for b in range(3):
            pieces = [
                raw[g * 128 + p * 64 : g * 128 + p * 64 + 64, 256:384]
                for g, p in order[2 * b : 2 * b + 2]
            ]
            side = jnp.concatenate(pieces, axis=0).T
            at_row = 192 + b * 64
            kvbuf[slot, at_row : at_row + 64, :] = side[HD : 2 * HD].astype(BF16)

    def finish_q(blocks):
        for g in blocks:
            block = raw[g * 128 : (g + 1) * 128, :]
            for pair in range(2):
                side = block[:, pair * 128 : (pair + 1) * 128].T
                for h in range(2):
                    q = turned(side[h * HD : (h + 1) * HD], q_gain, g)
                    at_lane = g * 512 + (pair * 2 + h) * 128
                    q_out[:, at_lane : at_lane + 128] = (q * scale).astype(BF16)

    kv_copies = [[], []]
    for s in range(2):
        for i, (here, there, dy, dz, part_of) in enumerate(SENDS):
            here, there = here + s * N_SP, there + s * N_SP
            half_of = pl.ds(192 * part_of, 192)
            kv_copies[s].append(
                send(
                    kvbuf.at[here, half_of], kvbuf.at[there, half_of],
                    kv_send.at[i + s * len(SENDS)], kv_recv.at[2 * there + part_of], near(dy, dz),
                )
            )

    def start_from(s, slot):
        for copy, (here, _, _, _, _) in zip(kv_copies[s], SENDS):
            if here == slot:
                copy.start()

    def keep(s, slot):
        slot = slot + s * N_SP
        return pltpu.make_async_copy(kvbuf.at[slot], kv_all.at[slot], keep_sem.at[slot])

    def arrive(s, slot):
        for copy, (_, there, _, _, _) in zip(kv_copies[s], SENDS):
            if there == slot:
                copy.wait_recv()
        start_from(s, slot)
        keep(s, slot).start()

    lifts = jnp.concatenate([jnp.full((1, 128), lift[h] * LOG2E, F32) for h in range(4)], axis=1)
    lifts = jnp.concatenate([lifts] * (TILE // 512), axis=1)
    ones = jnp.ones((VROWS - HD, 768), BF16)

    def lanes(t):
        if isinstance(t, int):
            return pl.ds(t * TILE, TILE)
        return pl.ds(pl.multiple_of(t * TILE, TILE), TILE)

    def narrow(t, n):
        start = t * TILE + n * NARROW
        return pl.ds(start if isinstance(t, int) else pl.multiple_of(start, NARROW), NARROW)

    def context(t):
        cv = cbuf[...].astype(F32).T[HD : 2 * HD].astype(BF16)
        cv = jnp.concatenate([cv, ones[:, 0:512]], axis=0)
        scores = jnp.dot(cbuf[...], tall(q_out[:, lanes(t)]), preferred_element_type=F32) + lifts
        top = jnp.max(scores, axis=0, keepdims=True)
        peak[:, lanes(t)] = top
        weights = jnp.exp2(scores - top).astype(BF16)
        acc[:, lanes(t)] = jnp.dot(cv, weights, preferred_element_type=F32)

    def query_forms(at_lanes):
        q = q_out[:, at_lanes]
        return tall(q), jnp.concatenate([jnp.zeros_like(q), q], axis=0)

    def values_of(pair):
        v = [kvbuf[pair * 2 + s, pl.ds(192 + i * 64, 64), :] for s in range(2) for i in range(3)]
        return jnp.concatenate([jnp.concatenate(v, axis=1), ones], axis=0)

    def work(now, then, read, write):
        if now is not None:
            v = values_of(now[0])
        for n in range(TILE // NARROW):
            cols = slice(n * NARROW, (n + 1) * NARROW)
            if then is not None:
                theirs = narrow(then[1], n)
                forms = query_forms(theirs)
                top = peak[:, theirs]
            total = None
            for i in range(4):
                if then is not None:
                    s, p = i % 2, i // 2
                    k = kvbuf[then[0] * 2 + s, pl.ds(0, 192), :]
                    x = jnp.dot(k, forms[p], preferred_element_type=F32)
                    write[pl.ds(s * 384 + p * 192, 192), cols] = jnp.exp2(x - top).astype(BF16)
                if now is not None and i < 3:
                    term = jnp.dot(
                        v[:, i * 256 : (i + 1) * 256], read[pl.ds(i * 256, 256), cols],
                        preferred_element_type=F32,
                    )
                    total = term if total is None else total + term
            if now is not None:
                acc[:, narrow(now[1], n)] += total

    def unit(j):
        i = j - 16
        late = jnp.where(i < 6, i + 8, jnp.where(i == 6, 8, jnp.where(i < 9, i + 7, i)))
        pair = jnp.where(
            j < 2 * FIRST, j - FIRST, jnp.where(j < 16, FIRST + (j - 2 * FIRST) // 2, late)
        )
        late = jnp.where(i < 6, 1, jnp.where(i == 6, 0, jnp.where(i < 9, 1, 0)))
        tile = jnp.where(j < 2 * FIRST, 1, jnp.where(j < 16, lax.rem(j, 2), late))
        return pair, tile

    c_copies = [
        send(
            cbuf.at[pl.ds(0, 32)], cbuf.at[pl.ds(32 * k, 32)],
            c_send.at[k - 1], c_recv.at[k - 1], sp_at(k),
        )
        for k in range(1, N_SP)
    ]

    def start_context():
        for copy in c_copies:
            copy.start()

    project(lat, 0, 0, start_context)
    ra.wait_recv()
    rb.wait_recv()
    rf.start()
    la.wait_recv()
    lb.wait_recv()
    lf.start()
    project(xbuf, 0, 192)
    finish_kv(0)
    finish_q((0,))
    arrive(0, 0)
    finish_q((1, 2))
    for copy in c_copies:
        copy.wait_recv()
    context(0)
    arrive(0, 1)
    work(None, (0, 0), None, p_even)

    def first_step(d, carry):
        for pair in range(1, FIRST):

            @pl.when(d == (pair - 1) // 2)
            def _(pair=pair):
                arrive(0, 2 * pair)
                arrive(0, 2 * pair + 1)

        work((2 * d, 0), (2 * d + 1, 0), p_even, p_odd)
        work((2 * d + 1, 0), (2 * d + 2, 0), p_odd, p_even)
        return carry

    lax.fori_loop(0, 1, first_step, 0)
    rc.wait_recv()
    lc.wait_recv()
    project(xbuf, 192, 384)
    lax.fori_loop(1, FIRST // 2, first_step, 0)
    work((FIRST - 1, 0), None, p_even, None)

    rf.wait_recv()
    lf.wait_recv()
    project(xbuf, 384, 576)
    finish_kv(1)
    finish_q((3,))
    arrive(1, 0)
    finish_q((4, 5))
    context(1)
    keep_rest = [
        pltpu.make_async_copy(q_out, q_all, keep_sem.at[2 * N_SP]),
        pltpu.make_async_copy(cbuf, ctx_all, keep_sem.at[2 * N_SP + 1]),
    ]
    for copy in keep_rest:
        copy.start()
    work(None, (0, 1), None, p_even)

    events = [(1, 0, (14, 15)), (1, 1, (1, 2, 3)), (3, 1, (4, 5)), (4, 1, (6, 7, 8, 9)),
              (5, 1, (10,)), (6, 1, (11, 12)), (7, 1, (13, 14)), (8, 1, (15,))]

    def second_step(d, carry):
        for when, s, slots in events:

            @pl.when(d == when)
            def _(s=s, slots=slots):
                for slot in slots:
                    arrive(s, slot)

        j = FIRST + 2 * d
        work(unit(j), unit(j + 1), p_even, p_odd)
        work(unit(j + 1), unit(j + 2), p_odd, p_even)
        return carry

    returns = [
        send(
            o_out.at[pl.ds(here, count)], obuf.at[tp, pl.ds(there, count)],
            o_send.at[i], o_recv.at[i], tp_at(k),
        )
        for i, (k, here, there, count) in enumerate(RETURNS)
    ]

    def finish_o(blocks):
        for g in blocks:
            at_lanes = pl.ds(g * 512, 512)
            mean = acc[0:HD, at_lanes] / acc[HD : HD + 1, at_lanes]
            stack = jnp.concatenate([mean[:, h * 128 : (h + 1) * 128] for h in range(4)], axis=0)
            o_out[g * 128 : (g + 1) * 128, :] = stack.T.astype(BF16)

    steps = (UNITS - 1 - FIRST) // 2
    lax.fori_loop(0, steps - 3, second_step, 0)
    finish_o((3, 4, 5))
    lax.fori_loop(steps - 3, steps - 2, second_step, 0)
    for copy, (_, here, _, _) in zip(returns, RETURNS):
        if here >= 384:
            copy.start()
    lax.fori_loop(steps - 2, steps, second_step, 0)
    work((15, 0), None, p_even, None)
    finish_o((1, 2))
    l_out[...] = acc[HD : HD + 8, :]
    peaks = acc[HD : HD + 1, 0:128]
    for i in range(1, 24):
        peaks = jnp.maximum(peaks, acc[HD : HD + 1, i * 128 : (i + 1) * 128])
    flag[...] = jnp.broadcast_to(peaks, (8, 128))
    fbuf[tp] = flag[...]
    finish_o((0,))
    for copy, (_, here, _, _) in zip(returns, RETURNS):
        if here < 384:
            copy.start()
    flags = [
        send(flag, fbuf.at[tp], f_send.at[k - 1], f_recv.at[k - 1], tp_at(k))
        for k in range(1, N_TP)
    ]
    for copy in flags:
        copy.start()
    obuf[tp] = o_out[0:rows, :]
    w_load.wait()
    wide = 512

    def heads(source, cols):
        feature = pl.ds(pl.multiple_of(source * 256, 256), 256)
        return jnp.dot(obuf[source], w[feature, cols], preferred_element_type=F32)

    for n in range(width // wide):
        cols = slice(n * wide, (n + 1) * wide)
        summed[:, cols] = heads(tp, cols)
    for copy in returns + flags:
        copy.wait_recv()
    for n in range(width // wide):
        cols = slice(n * wide, (n + 1) * wide)
        others = sum(heads(lax.rem(tp + k, N_TP), cols) for k in range(1, N_TP))
        mixed_out[:, cols] = (
            lat[:, cols].astype(F32) + gate_out[:, cols] * (summed[:, cols] + others)
        ).astype(BF16)
    flag_out[0] = (jnp.max(fbuf[...]) < 2.0**100).astype(jnp.int32)
    waiting = x_copies + p_copies + t_copies + c_copies + kv_copies[0] + kv_copies[1]
    for copy in waiting + returns + flags:
        copy.wait_send()
    for s in range(2):
        for slot in range(N_SP):
            keep(s, slot).wait()
    for copy in keep_rest:
        copy.wait()


def run_attention(lat, cond, condc, ctx, gain, ms, mc, mg, wq, wk, wv, qg, kg, lift, w_out):
    rows, width = lat.shape
    dma = pltpu.SemaphoreType.DMA
    loaded = (lat, ctx, ms, mc, mg, wq, wk, wv)
    return pl.pallas_call(
        attention_kernel,
        name="attention",
        out_shape=(
            jax.ShapeDtypeStruct((rows, width), BF16),
            jax.ShapeDtypeStruct((1,), jnp.int32),
            jax.ShapeDtypeStruct((768, 256), BF16),
            jax.ShapeDtypeStruct((8, 3072), F32),
            jax.ShapeDtypeStruct((HD, 3072), BF16),
            jax.ShapeDtypeStruct((2 * N_SP, 384, 128), BF16),
            jax.ShapeDtypeStruct((512, 128), BF16),
            jax.ShapeDtypeStruct((1, width), F32),
        ),
        in_specs=[HBM] * 9 + [VMEM] * 6 + [SMEM],
        out_specs=(VMEM, SMEM, VMEM, VMEM, HBM, HBM, HBM, VMEM),
        scratch_shapes=[
            pltpu.VMEM((3 * rows, width), BF16),
            pltpu.VMEM((24, 128), F32),
            pltpu.VMEM((N_SP - 1, 24, 128), F32),
            pltpu.VMEM((24, 128), F32),
            pltpu.VMEM((N_TP, 24, 128), F32),
            pltpu.VMEM((width, 384), BF16),
            pltpu.VMEM((rows, width), BF16),
            pltpu.VMEM((768, 384), F32),
            pltpu.VMEM((6, HD, GRID_W), F32),
            pltpu.VMEM((6, HD, GRID_W), F32),
            pltpu.VMEM((2, 8, width), F32),
            pltpu.VMEM((2, 8, width), F32),
            pltpu.VMEM((512, 128), BF16),
            pltpu.VMEM((HD, 3072), BF16),
            pltpu.VMEM((2 * N_SP, 384, 128), BF16),
            pltpu.VMEM((VROWS, 3072), F32),
            pltpu.VMEM((1, 3072), F32),
            pltpu.VMEM((768, TILE), BF16),
            pltpu.VMEM((768, TILE), BF16),
            *[pltpu.VMEM(a.shape, BF16) for a in loaded],
            dma((len(loaded),)),
            dma((8,)), dma((8,)), dma((15,)), dma((15,)),
            dma((3,)), dma((3,)), dma((15,)), dma((15,)),
            dma((2 * len(SENDS),)), dma((4 * N_SP,)), dma((2 * N_SP + 2,)),
            pltpu.VMEM((N_TP, rows, 256), BF16),
            pltpu.VMEM((N_TP, 8, 128), F32),
            pltpu.VMEM((8, 128), F32),
            pltpu.VMEM(w_out.shape, BF16),
            dma(()),
            pltpu.VMEM((rows, width), F32),
            dma((len(RETURNS),)), dma((len(RETURNS),)), dma((N_TP - 1,)), dma((N_TP - 1,)),
        ],
        compiler_params=pltpu.CompilerParams(
            collective_id=0, has_side_effects=True, vmem_limit_bytes=67043328
        ),
        cost_estimate=pl.CostEstimate(
            flops=2 * 10**10, bytes_accessed=10**7, transcendentals=4 * 10**7
        ),
    )(
        *loaded, w_out, cond, condc, gain, qg, kg, jnp.asarray(angle_table()), lift,
    )


def repair_kernel(
    l_ref, o_in, q_hbm, kv_hbm, ctx_hbm, lift, o_out,
    q_ref, kvbuf, ctx, acc, peak, sem,
):
    safe = jnp.all(l_ref[...] < 2.0**100)
    o_out[...] = o_in[...]

    @pl.when(jnp.logical_not(safe))
    def _():
        for src, dst in ((q_hbm, q_ref), (kv_hbm, kvbuf), (ctx_hbm, ctx)):
            copy = pltpu.make_async_copy(src, dst, sem)
            copy.start()
            copy.wait()
        wide = 512
        ones = jnp.ones((VROWS - HD, 768), BF16)
        lifts = jnp.concatenate(
            [jnp.full((1, 128), lift[h] * LOG2E, F32) for h in range(4)], axis=1
        )
        cv = ctx[...].astype(F32).T[HD : 2 * HD].astype(BF16)
        cv = jnp.concatenate([cv, ones[:, 0:512]], axis=0)

        @pl.loop(0, q_ref.shape[1] // wide)
        def _(t):
            lanes = pl.ds(pl.multiple_of(t * wide, wide), wide)
            q = q_ref[:, lanes]
            left = tall(q)
            right = jnp.concatenate([jnp.zeros_like(q), q], axis=0)
            scores = jnp.dot(ctx[...], left, preferred_element_type=F32) + lifts
            top = jnp.max(scores, axis=0, keepdims=True)
            peak[...] = top
            weights = jnp.exp2(scores - top).astype(BF16)
            acc[...] = jnp.dot(cv, weights, preferred_element_type=F32)

            @pl.loop(0, N_SP)
            def _(b):
                parts = []
                for s in range(2):
                    k = kvbuf[b * 2 + s, pl.ds(0, 192), :]
                    for query in (left, right):
                        parts.append(jnp.dot(k, query, preferred_element_type=F32))
                x = jnp.concatenate(parts, axis=0)
                old = peak[...]
                new = jnp.maximum(old, jnp.max(x, axis=0, keepdims=True))
                peak[...] = new
                v = [
                    kvbuf[b * 2 + s, pl.ds(192 + i * 64, 64), :] for s in range(2) for i in range(3)
                ]
                v = jnp.concatenate([jnp.concatenate(v, axis=1), ones], axis=0)
                weights = jnp.exp2(x - new).astype(BF16)
                acc[...] = acc[...] * jnp.exp2(old - new) + jnp.dot(
                    v, weights, preferred_element_type=F32
                )

            mean = acc[0:HD, :] / acc[HD : HD + 1, :]
            stack = jnp.concatenate([mean[:, h * 128 : (h + 1) * 128] for h in range(4)], axis=0)
            rows = pl.ds(pl.multiple_of(t * 128, 128), 128)
            o_out[rows, :] = stack.T.astype(BF16)


def run_repair(l, o, q, kv_all, ctx, lift):
    return pl.pallas_call(
        repair_kernel,
        name="repair",
        out_shape=jax.ShapeDtypeStruct(o.shape, o.dtype),
        in_specs=[VMEM, VMEM, HBM, HBM, HBM, SMEM],
        out_specs=VMEM,
        scratch_shapes=[
            pltpu.VMEM((HD, 3072), BF16),
            pltpu.VMEM((2 * N_SP, 384, 128), BF16),
            pltpu.VMEM((512, 128), BF16),
            pltpu.VMEM((VROWS, 512), F32),
            pltpu.VMEM((1, 512), F32),
            pltpu.SemaphoreType.DMA(()),
        ],
        compiler_params=pltpu.CompilerParams(vmem_limit_bytes=67043328),
    )(l, o, q, kv_all, ctx, lift)


def exchange_kernel(o_ref, out, obuf, send_sem, recv_sem):
    tp = lax.axis_index("tp")
    rows = o_ref.shape[0] // N_TP

    def tp_at(k):
        return {"tp": lax.rem(tp + k, N_TP)}

    barrier = pltpu.get_barrier_semaphore()
    for k in range(1, N_TP):
        pl.semaphore_signal(barrier, inc=1, device_id=tp_at(k), device_id_type=MESH)
    pl.semaphore_wait(barrier, N_TP - 1)
    copies = []
    for i, (k, here, there, count) in enumerate(RETURNS):
        copies.append(
            pltpu.make_async_remote_copy(
                src_ref=o_ref.at[pl.ds(here, count)],
                dst_ref=obuf.at[tp, pl.ds(there, count)],
                send_sem=send_sem.at[i], recv_sem=recv_sem.at[i],
                device_id=tp_at(k), device_id_type=MESH,
            )
        )
        copies[-1].start()
    out[tp] = o_ref[0:rows, :]
    for copy in copies:
        copy.wait_recv()
    for k in range(1, N_TP):
        source = lax.rem(tp + k, N_TP)
        out[source] = obuf[source]
    for copy in copies:
        copy.wait_send()


def run_exchange(o):
    rows = o.shape[0] // N_TP
    dma = pltpu.SemaphoreType.DMA
    return pl.pallas_call(
        exchange_kernel,
        name="exchange",
        out_shape=jax.ShapeDtypeStruct((N_TP, rows, 256), BF16),
        in_specs=[VMEM],
        out_specs=VMEM,
        scratch_shapes=[pltpu.VMEM((N_TP, rows, 256), BF16), dma((5,)), dma((5,))],
        compiler_params=pltpu.CompilerParams(
            collective_id=2, has_side_effects=True, vmem_limit_bytes=4 * 2**20
        ),
        cost_estimate=pl.CostEstimate(flops=0, bytes_accessed=25 * 10**6, transcendentals=0),
    )(o)


def output_kernel(o_hbm, w_hbm, lat_hbm, gate, out, o, w, lat, total, sem):
    pairs = [(o_hbm, o)]
    pairs += [(w_hbm.at[pl.ds(t * 256, 256)], w.at[t]) for t in range(N_TP)]
    pairs += [(lat_hbm, lat)]
    loads = [pltpu.make_async_copy(a, b, sem.at[i]) for i, (a, b) in enumerate(pairs)]
    for load in loads:
        load.start()
    loads[0].wait()
    wide = 512
    for t in range(N_TP):
        loads[1 + t].wait()
        if t == N_TP - 1:
            loads[-1].wait()
        for n in range(out.shape[1] // wide):
            cols = slice(n * wide, (n + 1) * wide)
            term = jnp.dot(o[t], w[t, :, cols], preferred_element_type=F32)
            if t == 0:
                total[:, cols] = term
            elif t < N_TP - 1:
                total[:, cols] += term
            else:
                term = total[:, cols] + term
                out[:, cols] = (lat[:, cols].astype(F32) + gate[:, cols] * term).astype(BF16)


def run_output(o, w_out, lat, gate):
    return pl.pallas_call(
        output_kernel,
        name="output",
        out_shape=jax.ShapeDtypeStruct(lat.shape, BF16),
        in_specs=[HBM, HBM, HBM, VMEM],
        out_specs=VMEM,
        scratch_shapes=[
            pltpu.VMEM(o.shape, BF16),
            pltpu.VMEM((N_TP, 256, w_out.shape[1]), BF16),
            pltpu.VMEM(lat.shape, BF16),
            pltpu.VMEM(lat.shape, F32),
            pltpu.SemaphoreType.DMA((N_TP + 2,)),
        ],
        compiler_params=pltpu.CompilerParams(vmem_limit_bytes=67043328),
    )(o, w_out, lat, gate)


def settle_kernel(mixed, out, buf, sem_in, sem_out):
    pieces = buf.shape[0]
    count = buf.shape[1]
    loads, stores = [], []
    for i in range(pieces):
        rows = pl.ds(i * count, count)
        loads.append(pltpu.make_async_copy(mixed.at[rows], buf.at[i], sem_in.at[i]))
        stores.append(pltpu.make_async_copy(buf.at[i], out.at[rows], sem_out.at[i]))
    for load in loads:
        load.start()
    for load, store in zip(loads, stores):
        load.wait()
        store.start()
    for store in stores:
        store.wait()


def run_settle(mixed):
    rows, width = mixed.shape
    return pl.pallas_call(
        settle_kernel,
        name="settle",
        out_shape=jax.ShapeDtypeStruct(mixed.shape, mixed.dtype),
        in_specs=[HBM],
        out_specs=HBM,
        scratch_shapes=[
            pltpu.VMEM((4, rows // 4, width), BF16),
            pltpu.SemaphoreType.DMA((4,)),
            pltpu.SemaphoreType.DMA((4,)),
        ],
        compiler_params=pltpu.CompilerParams(vmem_limit_bytes=67043328),
    )(mixed)


def on_device(
    latent, cond, cond_ctx, context, norm_gain, mod_shift, mod_scale, mod_gate,
    w_query, w_key, w_value, q_gain, k_gain, ctx_lift, w_out,
):
    lat = latent[0]
    mixed, safe, o, l, q, kv_all, ctx, gate = run_attention(
        lat, cond, cond_ctx[None, :], context[0], norm_gain.reshape(-1, 128),
        mod_shift, mod_scale, mod_gate, w_query, w_key.T, w_value.T,
        q_gain[None, :], k_gain[None, :], ctx_lift, w_out,
    )

    def again(mixed, o, l, q, kv_all, ctx):
        o = run_exchange(run_repair(l, o, q, kv_all, ctx, ctx_lift))
        return run_output(o, w_out, lat, gate)

    def keep(mixed, *rest):
        return mixed

    mixed = lax.cond(safe[0] > 0, keep, again, mixed, o, l, q, kv_all, ctx)
    return run_settle(mixed)[None]


def solution(mesh):
    in_specs = (
        P("dp", ("sp", "tp"), None),
        P("dp", "sp"),
        P("sp"),
        P("dp", "sp", None),
        P(),
        P("sp", "tp"),
        P("sp", "tp"),
        P("sp", "tp"),
        P(None, "tp"),
        P(None, "tp"),
        P(None, "tp"),
        P(),
        P(),
        P("tp"),
        P(),
    )
    return jax.shard_map(
        on_device, mesh=mesh, in_specs=in_specs,
        out_specs=P("dp", ("sp", "tp"), None), check_vma=False,
    )
```

```python
import functools

import jax
import jax.numpy as jnp
import numpy as np
from jax import lax
from jax.experimental import pallas as pl
from jax.experimental.pallas import tpu as pltpu
from jax.sharding import PartitionSpec as P

MESH = pl.DeviceIdType.MESH
HD = 64
GRID_W = 128
EPS = 1e-06
THETA = 10000.0
LOG2E = 1.4426950408889634
N_SP = 16
N_TP = 4
F32 = jnp.float32
BF16 = jnp.bfloat16
VMEM = pl.BlockSpec(memory_space=pltpu.VMEM)
HBM = pl.BlockSpec(memory_space=pltpu.HBM)
SMEM = pl.BlockSpec(memory_space=pltpu.SMEM)


def angle_table():
    i = (np.arange(HD) // 2) % 16
    f = (THETA ** (-(i.astype(np.float32)) / np.float32(16))).astype(np.float32)
    return np.repeat(f[:, None], GRID_W, axis=1)


def tall(x):
    return jnp.concatenate([x, jnp.zeros_like(x)], axis=0)


PLACES = [
    (0, 0), (-1, 0), (1, 0), (0, -1), (0, 1), (2, 0), (0, 2), (-1, -1),
    (-1, 1), (1, -1), (1, 1), (2, 1), (1, 2), (2, -1), (-1, 2), (2, 2),
]
SENDS = [
    (0, 1, 1, 0), (0, 2, -1, 0), (0, 3, 0, 1), (0, 4, 0, -1),
    (1, 5, 1, 0), (1, 7, 0, 1), (1, 8, 0, -1),
    (2, 9, 0, 1), (2, 10, 0, -1),
    (3, 6, 0, 1),
    (5, 11, 0, -1), (5, 13, 0, 1),
    (8, 14, 0, -1), (9, 12, 0, 1), (11, 15, 0, -1),
]
MIRROR = [
    next(i for i, q in enumerate(PLACES) if (q[0] % 4, q[1] % 4) == (p[1] % 4, p[0] % 4))
    for p in PLACES
]
SENDS = [(h, t, dy, dz, 0) for h, t, dy, dz in SENDS] + [
    (MIRROR[h], MIRROR[t], dz, dy, 1) for h, t, dy, dz in SENDS
]
TILE = 1536
NARROW = 512
VROWS = 80
FIRST = 7
UNITS = 32
RETURNS = [(2, 576, 0, 192), (3, 384, 96, 96), (1, 480, 0, 96), (3, 192, 0, 96), (1, 288, 96, 96)]


def attention_kernel(
    lat_hbm, ctx_hbm, ms_hbm, mc_hbm, mg_hbm, wq_hbm, wk_hbm, wv_hbm, w_hbm,
    cond, condc, gain, qg, kg, table, lift,
    mixed_out, flag_out, o_out, l_out, q_all, kv_all, ctx_all, gate_out,
    xbuf, part, psum_in, mine, full, wall, ubuf, raw, cosb, sinb, scl, sft, cbuf,
    q_out, kvbuf, acc, peak, p_even, p_odd, lat, ctx, m_shift, m_scale, m_gate, wq, wk, wv, load_sem,
    x_send, x_recv, p_send, p_recv, t_send, t_recv, c_send, c_recv, kv_send, kv_recv, keep_sem,
    obuf, fbuf, flag, w, w_sem, summed, o_send, o_recv, f_send, f_recv,
):
    sp = lax.axis_index("sp")
    tp = lax.axis_index("tp")
    y, z = lax.rem(sp, 4), lax.div(sp, 4)
    rows, width = lat.shape
    half = rows // 2

    def sp_at(k):
        return {"sp": lax.rem(sp + k, N_SP)}

    def tp_at(k):
        return {"tp": lax.rem(tp + k, N_TP)}

    def near(dy, dz):
        return {"sp": lax.rem(z + dz + 4, 4) * 4 + lax.rem(y + dy + 4, 4)}

    barrier = pltpu.get_barrier_semaphore()
    for k in range(1, N_SP):
        pl.semaphore_signal(barrier, inc=1, device_id=sp_at(k), device_id_type=MESH)
    for k in range(1, N_TP):
        pl.semaphore_signal(barrier, inc=1, device_id=tp_at(k), device_id_type=MESH)
    pairs = zip(
        (ms_hbm, mc_hbm, mg_hbm, lat_hbm, ctx_hbm, wq_hbm, wk_hbm, wv_hbm),
        (m_shift, m_scale, m_gate, lat, ctx, wq, wk, wv),
    )
    loads = [pltpu.make_async_copy(a, b, load_sem.at[i]) for i, (a, b) in enumerate(pairs)]
    for load in loads:
        load.start()
    pl.semaphore_wait(barrier, N_SP - 1 + N_TP - 1)

    def send(src, dst, s_sem, r_sem, target):
        return pltpu.make_async_remote_copy(
            src_ref=src, dst_ref=dst, send_sem=s_sem, recv_sem=r_sem,
            device_id=target, device_id_type=MESH,
        )

    def x_copy(i, src, to_row, count, k):
        return send(src, xbuf.at[pl.ds(to_row, count)], x_send.at[i], x_recv.at[i], tp_at(k))

    ra = x_copy(0, lat_hbm.at[pl.ds(0, 64)], 0, 64, 1)
    la = x_copy(1, lat_hbm.at[pl.ds(half, 64)], 96, 64, 3)
    rb = x_copy(2, lat_hbm.at[pl.ds(64, 32)], 64, 32, 1)
    lb = x_copy(3, lat_hbm.at[pl.ds(half + 64, 32)], 160, 32, 3)
    rc = x_copy(4, lat_hbm.at[pl.ds(half, half)], 192, half, 1)
    lc = x_copy(5, lat_hbm.at[pl.ds(0, half)], 288, half, 3)
    rf = x_copy(6, xbuf.at[pl.ds(0, half)], 384, half, 1)
    lf = x_copy(7, xbuf.at[pl.ds(half, half)], 480, half, 3)
    x_copies = [ra, la, rb, lb, rc, lc, rf, lf]
    ra.start()
    la.start()

    at = lax.broadcasted_iota(jnp.int32, (16, 128), 0)
    given = jnp.where(
        at == 0,
        jnp.broadcast_to(cond[...].astype(F32), (16, 128)),
        jnp.where(at == 1, jnp.broadcast_to(condc[...].astype(F32), (16, 128)), 0.0),
    )
    for load in loads[0:3]:
        load.wait()
    active = (given / (1.0 + jnp.exp(-given))).astype(BF16)
    for k, weight in enumerate((m_shift, m_scale, m_gate)):
        product = jnp.dot(active, weight[...], preferred_element_type=F32)
        for r in range(2):
            for c in range(4):
                i = r * 12 + k * 4 + c
                part[i : i + 1, :] = product[r : r + 1, c * 128 : (c + 1) * 128]
    p_copies = [
        send(part, psum_in.at[k - 1], p_send.at[k - 1], p_recv.at[k - 1], sp_at(k))
        for k in range(1, N_SP)
    ]
    for copy in p_copies:
        copy.start()

    for load in loads[3:]:
        load.wait()
    wall[:, 0:256] = wq[...]
    wall[:, 256:384] = jnp.concatenate([wk[...], wv[...]], axis=0).T

    for copy in p_copies:
        copy.wait_recv()
    total = part[...]
    for k in range(N_SP - 1):
        total = total + psum_in[k]
    mine[...] = total
    full[tp] = total
    t_copies = [
        send(mine, full.at[tp], t_send.at[k - 1], t_recv.at[k - 1], tp_at(k))
        for k in range(1, N_TP)
    ]
    for copy in t_copies:
        copy.start()
    for copy in (rb, lb, rc, lc):
        copy.start()

    row_id = lax.broadcasted_iota(jnp.int32, (HD, GRID_W), 0)
    lane_id = lax.broadcasted_iota(jnp.int32, (HD, GRID_W), 1)
    even = lax.rem(row_id, 2) == 0
    left, right, opposite = (lax.rem(tp + k, N_TP) * rows for k in (3, 1, 2))
    for g in range(6):
        n = lane_id + g * 128
        shift = jnp.where(
            n < 192,
            tp * rows,
            jnp.where(
                n < 288,
                left - 192,
                jnp.where(
                    n < 384,
                    right - 192,
                    jnp.where(
                        n < 480,
                        left - 288,
                        jnp.where(n < 576, right - 480, opposite - 576),
                    ),
                ),
            ),
        )
        at_token = n + shift + sp * 768
        grid_at = jnp.where(row_id < 32, at_token >> 7, at_token & 127)
        angle = table[...] * grid_at.astype(F32)
        cosb[g] = jnp.cos(angle)
        sine = jnp.sin(angle)
        sinb[g] = jnp.where(even, -sine, sine)

    w_load = pltpu.make_async_copy(w_hbm, w, w_sem)
    w_load.start()
    for copy in t_copies:
        copy.wait_recv()

    def vector(r, k):
        pieces = [
            full[t, r * 12 + k * 4 + c : r * 12 + k * 4 + c + 1, :]
            for t in range(N_TP)
            for c in range(4)
        ]
        return jnp.concatenate(pieces, axis=1)

    gains = gain[...].astype(F32)
    gains = jnp.concatenate([gains[i : i + 1, :] for i in range(width // 128)], axis=1)
    for r in range(2):
        scl[r] = jnp.broadcast_to(gains * (1.0 + vector(r, 1)), (8, width))
        sft[r] = jnp.broadcast_to(vector(r, 0), (8, width))
    gate_out[...] = vector(0, 2)

    def modulate(src, r, count):
        values = src.astype(F32)
        inverse = lax.rsqrt(jnp.mean(values * values, axis=-1, keepdims=True) + EPS)
        normed = (values * inverse).reshape(count // 8, 8, width)
        return (normed * scl[r][None] + sft[r][None]).reshape(count, width).astype(BF16)

    uc = modulate(ctx[...], 1, ctx.shape[0])
    craw = jnp.dot(uc, wall[:, 256:384], preferred_element_type=F32)
    lane = lax.broadcasted_iota(jnp.int32, craw.shape, 1)
    square = jnp.where(lane < HD, craw * craw, 0.0)
    mean = jnp.sum(square, axis=-1, keepdims=True) * (1.0 / HD)
    k_row = kg[...].astype(F32)
    keys = craw * lax.rsqrt(mean + EPS) * jnp.concatenate([k_row, jnp.ones((1, HD), F32)], axis=1)
    cbuf[pl.ds(0, 32), :] = jnp.where(lane < HD, keys, craw).astype(BF16)

    def project(x, first, to_row, between=None):
        @pl.loop(0, rows // 32)
        def _(i):
            at_rows = pl.ds(pl.multiple_of(i * 32, 32), 32)
            from_rows = pl.ds(pl.multiple_of(first + i * 32, 32), 32)
            ubuf[at_rows, :] = modulate(x[from_rows, :], 0, 32)

        if between is not None:
            between()
        raw[pl.ds(to_row, rows), :] = jnp.dot(ubuf[...], wall[...], preferred_element_type=F32)

    def column(ref):
        r = lax.broadcasted_iota(jnp.int32, (HD, HD), 0)
        c = lax.broadcasted_iota(jnp.int32, (HD, HD), 1)
        spread = jnp.broadcast_to(ref[...].astype(F32), (HD, HD))
        return jnp.sum(jnp.where(r == c, spread, 0.0), axis=1, keepdims=True)

    q_gain = column(qg)
    k_gain = column(kg)

    def turned(x, gain_column, g):
        square = jnp.sum(x * x, axis=0, keepdims=True) * (1.0 / HD)
        normed = x * lax.rsqrt(square + EPS) * gain_column
        up = pltpu.roll(normed, HD - 1, axis=0)
        down = pltpu.roll(normed, 1, axis=0)
        return normed * cosb[g] + jnp.where(even, up, down) * sinb[g]

    scale = LOG2E * HD ** (-0.5)

    def finish_kv(s):
        slot = s * N_SP
        for i in range(3):
            g = 3 * s + i
            side = raw[g * 128 : (g + 1) * 128, 256:384].T
            k = turned(side[0:HD], k_gain, g).T
            kvbuf[slot, i * 64 : (i + 1) * 64, :] = jnp.concatenate(
                [k[0:64], k[64:128]], axis=1
            ).astype(BF16)
        order = [(g, p) for p in range(2) for g in (3 * s, 3 * s + 1, 3 * s + 2)]
        for b in range(3):
            pieces = [
                raw[g * 128 + p * 64 : g * 128 + p * 64 + 64, 256:384]
                for g, p in order[2 * b : 2 * b + 2]
            ]
            side = jnp.concatenate(pieces, axis=0).T
            at_row = 192 + b * 64
            kvbuf[slot, at_row : at_row + 64, :] = side[HD : 2 * HD].astype(BF16)

    def finish_q(blocks):
        for g in blocks:
            block = raw[g * 128 : (g + 1) * 128, :]
            for pair in range(2):
                side = block[:, pair * 128 : (pair + 1) * 128].T
                for h in range(2):
                    q = turned(side[h * HD : (h + 1) * HD], q_gain, g)
                    at_lane = g * 512 + (pair * 2 + h) * 128
                    q_out[:, at_lane : at_lane + 128] = (q * scale).astype(BF16)

    kv_copies = [[], []]
    for s in range(2):
        for i, (here, there, dy, dz, part_of) in enumerate(SENDS):
            here, there = here + s * N_SP, there + s * N_SP
            half_of = pl.ds(192 * part_of, 192)
            kv_copies[s].append(
                send(
                    kvbuf.at[here, half_of], kvbuf.at[there, half_of],
                    kv_send.at[i + s * len(SENDS)], kv_recv.at[2 * there + part_of], near(dy, dz),
                )
            )

    def start_from(s, slot):
        for copy, (here, _, _, _, _) in zip(kv_copies[s], SENDS):
            if here == slot:
                copy.start()

    def keep(s, slot):
        slot = slot + s * N_SP
        return pltpu.make_async_copy(kvbuf.at[slot], kv_all.at[slot], keep_sem.at[slot])

    def arrive(s, slot):
        for copy, (_, there, _, _, _) in zip(kv_copies[s], SENDS):
            if there == slot:
                copy.wait_recv()
        start_from(s, slot)
        keep(s, slot).start()

    lifts = jnp.concatenate([jnp.full((1, 128), lift[h] * LOG2E, F32) for h in range(4)], axis=1)
    lifts = jnp.concatenate([lifts] * (TILE // 512), axis=1)
    ones = jnp.ones((VROWS - HD, 768), BF16)

    def lanes(t):
        if isinstance(t, int):
            return pl.ds(t * TILE, TILE)
        return pl.ds(pl.multiple_of(t * TILE, TILE), TILE)

    def narrow(t, n):
        start = t * TILE + n * NARROW
        return pl.ds(start if isinstance(t, int) else pl.multiple_of(start, NARROW), NARROW)

    def context(t):
        cv = cbuf[...].astype(F32).T[HD : 2 * HD].astype(BF16)
        cv = jnp.concatenate([cv, ones[:, 0:512]], axis=0)
        scores = jnp.dot(cbuf[...], tall(q_out[:, lanes(t)]), preferred_element_type=F32) + lifts
        top = jnp.max(scores, axis=0, keepdims=True)
        peak[:, lanes(t)] = top
        weights = jnp.exp2(scores - top).astype(BF16)
        acc[:, lanes(t)] = jnp.dot(cv, weights, preferred_element_type=F32)

    def query_forms(at_lanes):
        q = q_out[:, at_lanes]
        return tall(q), jnp.concatenate([jnp.zeros_like(q), q], axis=0)

    def values_of(pair):
        v = [kvbuf[pair * 2 + s, pl.ds(192 + i * 64, 64), :] for s in range(2) for i in range(3)]
        return jnp.concatenate([jnp.concatenate(v, axis=1), ones], axis=0)

    def work(now, then, read, write):
        if now is not None:
            v = values_of(now[0])
        for n in range(TILE // NARROW):
            cols = slice(n * NARROW, (n + 1) * NARROW)
            if then is not None:
                theirs = narrow(then[1], n)
                forms = query_forms(theirs)
                top = peak[:, theirs]
            total = None
            for i in range(4):
                if then is not None:
                    s, p = i % 2, i // 2
                    k = kvbuf[then[0] * 2 + s, pl.ds(0, 192), :]
                    x = jnp.dot(k, forms[p], preferred_element_type=F32)
                    write[pl.ds(s * 384 + p * 192, 192), cols] = jnp.exp2(x - top).astype(BF16)
                if now is not None and i < 3:
                    term = jnp.dot(
                        v[:, i * 256 : (i + 1) * 256], read[pl.ds(i * 256, 256), cols],
                        preferred_element_type=F32,
                    )
                    total = term if total is None else total + term
            if now is not None:
                acc[:, narrow(now[1], n)] += total

    def unit(j):
        i = j - 16
        late = jnp.where(i < 6, i + 8, jnp.where(i == 6, 8, jnp.where(i < 9, i + 7, i)))
        pair = jnp.where(
            j < 2 * FIRST, j - FIRST, jnp.where(j < 16, FIRST + (j - 2 * FIRST) // 2, late)
        )
        late = jnp.where(i < 6, 1, jnp.where(i == 6, 0, jnp.where(i < 9, 1, 0)))
        tile = jnp.where(j < 2 * FIRST, 1, jnp.where(j < 16, lax.rem(j, 2), late))
        return pair, tile

    c_copies = [
        send(
            cbuf.at[pl.ds(0, 32)], cbuf.at[pl.ds(32 * k, 32)],
            c_send.at[k - 1], c_recv.at[k - 1], sp_at(k),
        )
        for k in range(1, N_SP)
    ]

    def start_context():
        for copy in c_copies:
            copy.start()

    project(lat, 0, 0, start_context)
    ra.wait_recv()
    rb.wait_recv()
    rf.start()
    la.wait_recv()
    lb.wait_recv()
    lf.start()
    project(xbuf, 0, 192)
    finish_kv(0)
    finish_q((0,))
    arrive(0, 0)
    finish_q((1, 2))
    for copy in c_copies:
        copy.wait_recv()
    context(0)
    arrive(0, 1)
    work(None, (0, 0), None, p_even)

    for j in range(FIRST - 1):
        arrive(0, 2 * j + 2)
        arrive(0, 2 * j + 3)
        work((j, 0), (j + 1, 0), *((p_even, p_odd) if j % 2 == 0 else (p_odd, p_even)))
        if j == 2:
            rc.wait_recv()
            lc.wait_recv()
            project(xbuf, 192, 384)
    work((FIRST - 1, 0), None, p_even, None)

    rf.wait_recv()
    lf.wait_recv()
    project(xbuf, 384, 576)
    finish_kv(1)
    finish_q((3,))
    arrive(1, 0)
    finish_q((4, 5))
    context(1)
    keep_rest = [
        pltpu.make_async_copy(q_out, q_all, keep_sem.at[2 * N_SP]),
        pltpu.make_async_copy(cbuf, ctx_all, keep_sem.at[2 * N_SP + 1]),
    ]
    for copy in keep_rest:
        copy.start()
    work(None, (0, 1), None, p_even)

    events = [(1, 1, (1, 2, 3)), (2, 0, (14, 15)), (3, 1, (4, 5)), (4, 1, (7, 8, 9)),
              (5, 1, (6, 10)), (6, 1, (11, 12)), (7, 1, (13, 14)), (8, 1, (15,))]

    def second_step(d, carry):
        for when, s, slots in events:

            @pl.when(d == when)
            def _(s=s, slots=slots):
                for slot in slots:
                    arrive(s, slot)

        j = FIRST + 2 * d
        work(unit(j), unit(j + 1), p_even, p_odd)
        work(unit(j + 1), unit(j + 2), p_odd, p_even)
        return carry

    returns = [
        send(
            o_out.at[pl.ds(here, count)], obuf.at[tp, pl.ds(there, count)],
            o_send.at[i], o_recv.at[i], tp_at(k),
        )
        for i, (k, here, there, count) in enumerate(RETURNS)
    ]

    def finish_o(blocks):
        for g in blocks:
            at_lanes = pl.ds(g * 512, 512)
            mean = acc[0:HD, at_lanes] / acc[HD : HD + 1, at_lanes]
            stack = jnp.concatenate([mean[:, h * 128 : (h + 1) * 128] for h in range(4)], axis=0)
            o_out[g * 128 : (g + 1) * 128, :] = stack.T.astype(BF16)

    steps = (UNITS - 1 - FIRST) // 2
    lax.fori_loop(0, steps - 3, second_step, 0)
    finish_o((3, 4, 5))
    lax.fori_loop(steps - 3, steps - 2, second_step, 0)
    for copy, (_, here, _, _) in zip(returns, RETURNS):
        if here >= 384:
            copy.start()
    lax.fori_loop(steps - 2, steps, second_step, 0)
    work((15, 0), None, p_even, None)
    finish_o((1, 2))
    l_out[...] = acc[HD : HD + 8, :]
    peaks = acc[HD : HD + 1, 0:128]
    for i in range(1, 24):
        peaks = jnp.maximum(peaks, acc[HD : HD + 1, i * 128 : (i + 1) * 128])
    flag[...] = jnp.broadcast_to(peaks, (8, 128))
    fbuf[tp] = flag[...]
    finish_o((0,))
    for copy, (_, here, _, _) in zip(returns, RETURNS):
        if here < 384:
            copy.start()
    flags = [
        send(flag, fbuf.at[tp], f_send.at[k - 1], f_recv.at[k - 1], tp_at(k))
        for k in range(1, N_TP)
    ]
    for copy in flags:
        copy.start()
    obuf[tp] = o_out[0:rows, :]
    w_load.wait()
    wide = 512

    def heads(source, cols):
        feature = pl.ds(pl.multiple_of(source * 256, 256), 256)
        return jnp.dot(obuf[source], w[feature, cols], preferred_element_type=F32)

    for n in range(width // wide):
        cols = slice(n * wide, (n + 1) * wide)
        summed[:, cols] = heads(tp, cols)
    for copy in returns + flags:
        copy.wait_recv()
    for n in range(width // wide):
        cols = slice(n * wide, (n + 1) * wide)
        others = sum(heads(lax.rem(tp + k, N_TP), cols) for k in range(1, N_TP))
        mixed_out[:, cols] = (
            lat[:, cols].astype(F32) + gate_out[:, cols] * (summed[:, cols] + others)
        ).astype(BF16)
    flag_out[0] = (jnp.max(fbuf[...]) < 2.0**100).astype(jnp.int32)
    waiting = x_copies + p_copies + t_copies + c_copies + kv_copies[0] + kv_copies[1]
    for copy in waiting + returns + flags:
        copy.wait_send()
    for s in range(2):
        for slot in range(N_SP):
            keep(s, slot).wait()
    for copy in keep_rest:
        copy.wait()


def run_attention(lat, cond, condc, ctx, gain, ms, mc, mg, wq, wk, wv, qg, kg, lift, w_out):
    rows, width = lat.shape
    dma = pltpu.SemaphoreType.DMA
    loaded = (lat, ctx, ms, mc, mg, wq, wk, wv)
    return pl.pallas_call(
        attention_kernel,
        name="attention",
        out_shape=(
            jax.ShapeDtypeStruct((rows, width), BF16),
            jax.ShapeDtypeStruct((1,), jnp.int32),
            jax.ShapeDtypeStruct((768, 256), BF16),
            jax.ShapeDtypeStruct((8, 3072), F32),
            jax.ShapeDtypeStruct((HD, 3072), BF16),
            jax.ShapeDtypeStruct((2 * N_SP, 384, 128), BF16),
            jax.ShapeDtypeStruct((512, 128), BF16),
            jax.ShapeDtypeStruct((1, width), F32),
        ),
        in_specs=[HBM] * 9 + [VMEM] * 6 + [SMEM],
        out_specs=(VMEM, SMEM, VMEM, VMEM, HBM, HBM, HBM, VMEM),
        scratch_shapes=[
            pltpu.VMEM((3 * rows, width), BF16),
            pltpu.VMEM((24, 128), F32),
            pltpu.VMEM((N_SP - 1, 24, 128), F32),
            pltpu.VMEM((24, 128), F32),
            pltpu.VMEM((N_TP, 24, 128), F32),
            pltpu.VMEM((width, 384), BF16),
            pltpu.VMEM((rows, width), BF16),
            pltpu.VMEM((768, 384), F32),
            pltpu.VMEM((6, HD, GRID_W), F32),
            pltpu.VMEM((6, HD, GRID_W), F32),
            pltpu.VMEM((2, 8, width), F32),
            pltpu.VMEM((2, 8, width), F32),
            pltpu.VMEM((512, 128), BF16),
            pltpu.VMEM((HD, 3072), BF16),
            pltpu.VMEM((2 * N_SP, 384, 128), BF16),
            pltpu.VMEM((VROWS, 3072), F32),
            pltpu.VMEM((1, 3072), F32),
            pltpu.VMEM((768, TILE), BF16),
            pltpu.VMEM((768, TILE), BF16),
            *[pltpu.VMEM(a.shape, BF16) for a in loaded],
            dma((len(loaded),)),
            dma((8,)), dma((8,)), dma((15,)), dma((15,)),
            dma((3,)), dma((3,)), dma((15,)), dma((15,)),
            dma((2 * len(SENDS),)), dma((4 * N_SP,)), dma((2 * N_SP + 2,)),
            pltpu.VMEM((N_TP, rows, 256), BF16),
            pltpu.VMEM((N_TP, 8, 128), F32),
            pltpu.VMEM((8, 128), F32),
            pltpu.VMEM(w_out.shape, BF16),
            dma(()),
            pltpu.VMEM((rows, width), F32),
            dma((len(RETURNS),)), dma((len(RETURNS),)), dma((N_TP - 1,)), dma((N_TP - 1,)),
        ],
        compiler_params=pltpu.CompilerParams(
            collective_id=0, has_side_effects=True, vmem_limit_bytes=67043328
        ),
        cost_estimate=pl.CostEstimate(
            flops=2 * 10**10, bytes_accessed=10**7, transcendentals=4 * 10**7
        ),
    )(
        *loaded, w_out, cond, condc, gain, qg, kg, jnp.asarray(angle_table()), lift,
    )


def repair_kernel(
    l_ref, o_in, q_hbm, kv_hbm, ctx_hbm, lift, o_out,
    q_ref, kvbuf, ctx, acc, peak, sem,
):
    safe = jnp.all(l_ref[...] < 2.0**100)
    o_out[...] = o_in[...]

    @pl.when(jnp.logical_not(safe))
    def _():
        for src, dst in ((q_hbm, q_ref), (kv_hbm, kvbuf), (ctx_hbm, ctx)):
            copy = pltpu.make_async_copy(src, dst, sem)
            copy.start()
            copy.wait()
        wide = 512
        ones = jnp.ones((VROWS - HD, 768), BF16)
        lifts = jnp.concatenate(
            [jnp.full((1, 128), lift[h] * LOG2E, F32) for h in range(4)], axis=1
        )
        cv = ctx[...].astype(F32).T[HD : 2 * HD].astype(BF16)
        cv = jnp.concatenate([cv, ones[:, 0:512]], axis=0)

        @pl.loop(0, q_ref.shape[1] // wide)
        def _(t):
            lanes = pl.ds(pl.multiple_of(t * wide, wide), wide)
            q = q_ref[:, lanes]
            left = tall(q)
            right = jnp.concatenate([jnp.zeros_like(q), q], axis=0)
            scores = jnp.dot(ctx[...], left, preferred_element_type=F32) + lifts
            top = jnp.max(scores, axis=0, keepdims=True)
            peak[...] = top
            weights = jnp.exp2(scores - top).astype(BF16)
            acc[...] = jnp.dot(cv, weights, preferred_element_type=F32)

            @pl.loop(0, N_SP)
            def _(b):
                parts = []
                for s in range(2):
                    k = kvbuf[b * 2 + s, pl.ds(0, 192), :]
                    for query in (left, right):
                        parts.append(jnp.dot(k, query, preferred_element_type=F32))
                x = jnp.concatenate(parts, axis=0)
                old = peak[...]
                new = jnp.maximum(old, jnp.max(x, axis=0, keepdims=True))
                peak[...] = new
                v = [
                    kvbuf[b * 2 + s, pl.ds(192 + i * 64, 64), :] for s in range(2) for i in range(3)
                ]
                v = jnp.concatenate([jnp.concatenate(v, axis=1), ones], axis=0)
                weights = jnp.exp2(x - new).astype(BF16)
                acc[...] = acc[...] * jnp.exp2(old - new) + jnp.dot(
                    v, weights, preferred_element_type=F32
                )

            mean = acc[0:HD, :] / acc[HD : HD + 1, :]
            stack = jnp.concatenate([mean[:, h * 128 : (h + 1) * 128] for h in range(4)], axis=0)
            rows = pl.ds(pl.multiple_of(t * 128, 128), 128)
            o_out[rows, :] = stack.T.astype(BF16)


def run_repair(l, o, q, kv_all, ctx, lift):
    return pl.pallas_call(
        repair_kernel,
        name="repair",
        out_shape=jax.ShapeDtypeStruct(o.shape, o.dtype),
        in_specs=[VMEM, VMEM, HBM, HBM, HBM, SMEM],
        out_specs=VMEM,
        scratch_shapes=[
            pltpu.VMEM((HD, 3072), BF16),
            pltpu.VMEM((2 * N_SP, 384, 128), BF16),
            pltpu.VMEM((512, 128), BF16),
            pltpu.VMEM((VROWS, 512), F32),
            pltpu.VMEM((1, 512), F32),
            pltpu.SemaphoreType.DMA(()),
        ],
        compiler_params=pltpu.CompilerParams(vmem_limit_bytes=67043328),
    )(l, o, q, kv_all, ctx, lift)


def exchange_kernel(o_ref, out, obuf, send_sem, recv_sem):
    tp = lax.axis_index("tp")
    rows = o_ref.shape[0] // N_TP

    def tp_at(k):
        return {"tp": lax.rem(tp + k, N_TP)}

    barrier = pltpu.get_barrier_semaphore()
    for k in range(1, N_TP):
        pl.semaphore_signal(barrier, inc=1, device_id=tp_at(k), device_id_type=MESH)
    pl.semaphore_wait(barrier, N_TP - 1)
    copies = []
    for i, (k, here, there, count) in enumerate(RETURNS):
        copies.append(
            pltpu.make_async_remote_copy(
                src_ref=o_ref.at[pl.ds(here, count)],
                dst_ref=obuf.at[tp, pl.ds(there, count)],
                send_sem=send_sem.at[i], recv_sem=recv_sem.at[i],
                device_id=tp_at(k), device_id_type=MESH,
            )
        )
        copies[-1].start()
    out[tp] = o_ref[0:rows, :]
    for copy in copies:
        copy.wait_recv()
    for k in range(1, N_TP):
        source = lax.rem(tp + k, N_TP)
        out[source] = obuf[source]
    for copy in copies:
        copy.wait_send()


def run_exchange(o):
    rows = o.shape[0] // N_TP
    dma = pltpu.SemaphoreType.DMA
    return pl.pallas_call(
        exchange_kernel,
        name="exchange",
        out_shape=jax.ShapeDtypeStruct((N_TP, rows, 256), BF16),
        in_specs=[VMEM],
        out_specs=VMEM,
        scratch_shapes=[pltpu.VMEM((N_TP, rows, 256), BF16), dma((5,)), dma((5,))],
        compiler_params=pltpu.CompilerParams(
            collective_id=2, has_side_effects=True, vmem_limit_bytes=4 * 2**20
        ),
        cost_estimate=pl.CostEstimate(flops=0, bytes_accessed=25 * 10**6, transcendentals=0),
    )(o)


def output_kernel(o_hbm, w_hbm, lat_hbm, gate, out, o, w, lat, total, sem):
    pairs = [(o_hbm, o)]
    pairs += [(w_hbm.at[pl.ds(t * 256, 256)], w.at[t]) for t in range(N_TP)]
    pairs += [(lat_hbm, lat)]
    loads = [pltpu.make_async_copy(a, b, sem.at[i]) for i, (a, b) in enumerate(pairs)]
    for load in loads:
        load.start()
    loads[0].wait()
    wide = 512
    for t in range(N_TP):
        loads[1 + t].wait()
        if t == N_TP - 1:
            loads[-1].wait()
        for n in range(out.shape[1] // wide):
            cols = slice(n * wide, (n + 1) * wide)
            term = jnp.dot(o[t], w[t, :, cols], preferred_element_type=F32)
            if t == 0:
                total[:, cols] = term
            elif t < N_TP - 1:
                total[:, cols] += term
            else:
                term = total[:, cols] + term
                out[:, cols] = (lat[:, cols].astype(F32) + gate[:, cols] * term).astype(BF16)


def run_output(o, w_out, lat, gate):
    return pl.pallas_call(
        output_kernel,
        name="output",
        out_shape=jax.ShapeDtypeStruct(lat.shape, BF16),
        in_specs=[HBM, HBM, HBM, VMEM],
        out_specs=VMEM,
        scratch_shapes=[
            pltpu.VMEM(o.shape, BF16),
            pltpu.VMEM((N_TP, 256, w_out.shape[1]), BF16),
            pltpu.VMEM(lat.shape, BF16),
            pltpu.VMEM(lat.shape, F32),
            pltpu.SemaphoreType.DMA((N_TP + 2,)),
        ],
        compiler_params=pltpu.CompilerParams(vmem_limit_bytes=67043328),
    )(o, w_out, lat, gate)


def settle_kernel(mixed, out, buf, sem_in, sem_out):
    pieces = buf.shape[0]
    count = buf.shape[1]
    loads, stores = [], []
    for i in range(pieces):
        rows = pl.ds(i * count, count)
        loads.append(pltpu.make_async_copy(mixed.at[rows], buf.at[i], sem_in.at[i]))
        stores.append(pltpu.make_async_copy(buf.at[i], out.at[rows], sem_out.at[i]))
    for load in loads:
        load.start()
    for load, store in zip(loads, stores):
        load.wait()
        store.start()
    for store in stores:
        store.wait()


def run_settle(mixed):
    rows, width = mixed.shape
    return pl.pallas_call(
        settle_kernel,
        name="settle",
        out_shape=jax.ShapeDtypeStruct(mixed.shape, mixed.dtype),
        in_specs=[HBM],
        out_specs=HBM,
        scratch_shapes=[
            pltpu.VMEM((4, rows // 4, width), BF16),
            pltpu.SemaphoreType.DMA((4,)),
            pltpu.SemaphoreType.DMA((4,)),
        ],
        compiler_params=pltpu.CompilerParams(vmem_limit_bytes=67043328),
    )(mixed)


def on_device(
    latent, cond, cond_ctx, context, norm_gain, mod_shift, mod_scale, mod_gate,
    w_query, w_key, w_value, q_gain, k_gain, ctx_lift, w_out,
):
    lat = latent[0]
    mixed, safe, o, l, q, kv_all, ctx, gate = run_attention(
        lat, cond, cond_ctx[None, :], context[0], norm_gain.reshape(-1, 128),
        mod_shift, mod_scale, mod_gate, w_query, w_key.T, w_value.T,
        q_gain[None, :], k_gain[None, :], ctx_lift, w_out,
    )

    def again(mixed, o, l, q, kv_all, ctx):
        o = run_exchange(run_repair(l, o, q, kv_all, ctx, ctx_lift))
        return run_output(o, w_out, lat, gate)

    def keep(mixed, *rest):
        return mixed

    mixed = lax.cond(safe[0] > 0, keep, again, mixed, o, l, q, kv_all, ctx)
    return run_settle(mixed)[None]


def solution(mesh):
    in_specs = (
        P("dp", ("sp", "tp"), None),
        P("dp", "sp"),
        P("sp"),
        P("dp", "sp", None),
        P(),
        P("sp", "tp"),
        P("sp", "tp"),
        P("sp", "tp"),
        P(None, "tp"),
        P(None, "tp"),
        P(None, "tp"),
        P(),
        P(),
        P("tp"),
        P(),
    )
    return jax.shard_map(
        on_device, mesh=mesh, in_specs=in_specs,
        out_specs=P("dp", ("sp", "tp"), None), check_vma=False,
    )
```

```python
import functools

import jax
import jax.numpy as jnp
import numpy as np
from jax import lax
from jax.experimental import pallas as pl
from jax.experimental.pallas import tpu as pltpu
from jax.sharding import PartitionSpec as P

MESH = pl.DeviceIdType.MESH
HD = 64
GRID_W = 128
EPS = 1e-06
THETA = 10000.0
LOG2E = 1.4426950408889634
N_SP = 16
N_TP = 4
F32 = jnp.float32
BF16 = jnp.bfloat16
VMEM = pl.BlockSpec(memory_space=pltpu.VMEM)
HBM = pl.BlockSpec(memory_space=pltpu.HBM)
SMEM = pl.BlockSpec(memory_space=pltpu.SMEM)


def angle_table():
    i = (np.arange(HD) // 2) % 16
    f = (THETA ** (-(i.astype(np.float32)) / np.float32(16))).astype(np.float32)
    return np.repeat(f[:, None], GRID_W, axis=1)


def tall(x):
    return jnp.concatenate([x, jnp.zeros_like(x)], axis=0)


PLACES = [
    (0, 0), (-1, 0), (1, 0), (0, -1), (0, 1), (2, 0), (0, 2), (-1, -1),
    (-1, 1), (1, -1), (1, 1), (2, 1), (1, 2), (2, -1), (-1, 2), (2, 2),
]
SENDS = [
    (0, 1, 1, 0), (0, 2, -1, 0), (0, 3, 0, 1), (0, 4, 0, -1),
    (1, 5, 1, 0), (1, 7, 0, 1), (1, 8, 0, -1),
    (2, 9, 0, 1), (2, 10, 0, -1),
    (3, 6, 0, 1),
    (5, 11, 0, -1), (5, 13, 0, 1),
    (8, 14, 0, -1), (9, 12, 0, 1), (11, 15, 0, -1),
]
MIRROR = [
    next(i for i, q in enumerate(PLACES) if (q[0] % 4, q[1] % 4) == (p[1] % 4, p[0] % 4))
    for p in PLACES
]
SENDS = [(h, t, dy, dz, 0) for h, t, dy, dz in SENDS] + [
    (MIRROR[h], MIRROR[t], dz, dy, 1) for h, t, dy, dz in SENDS
]
TILE = 1536
NARROW = 512
VROWS = 80
FIRST = 5
UNITS = 32
RETURNS = [(2, 576, 0, 192), (3, 384, 96, 96), (1, 480, 0, 96), (3, 192, 0, 96), (1, 288, 96, 96)]


def attention_kernel(
    lat_hbm, ctx_hbm, ms_hbm, mc_hbm, mg_hbm, wq_hbm, wk_hbm, wv_hbm, w_hbm,
    cond, condc, gain, qg, kg, table, lift,
    mixed_out, flag_out, o_out, l_out, q_all, kv_all, ctx_all, gate_out,
    xbuf, part, psum_in, mine, full, wall, ubuf, raw, cosb, sinb, scl, sft, cbuf,
    q_out, kvbuf, acc, peak, p_even, p_odd, lat, ctx, m_shift, m_scale, m_gate, wq, wk, wv, load_sem,
    x_send, x_recv, p_send, p_recv, t_send, t_recv, c_send, c_recv, kv_send, kv_recv, keep_sem,
    obuf, fbuf, flag, w, w_sem, summed, o_send, o_recv, f_send, f_recv,
):
    sp = lax.axis_index("sp")
    tp = lax.axis_index("tp")
    y, z = lax.rem(sp, 4), lax.div(sp, 4)
    rows, width = lat.shape
    half = rows // 2

    def sp_at(k):
        return {"sp": lax.rem(sp + k, N_SP)}

    def tp_at(k):
        return {"tp": lax.rem(tp + k, N_TP)}

    def near(dy, dz):
        return {"sp": lax.rem(z + dz + 4, 4) * 4 + lax.rem(y + dy + 4, 4)}

    barrier = pltpu.get_barrier_semaphore()
    for k in range(1, N_SP):
        pl.semaphore_signal(barrier, inc=1, device_id=sp_at(k), device_id_type=MESH)
    for k in range(1, N_TP):
        pl.semaphore_signal(barrier, inc=1, device_id=tp_at(k), device_id_type=MESH)
    pairs = zip(
        (ms_hbm, mc_hbm, mg_hbm, lat_hbm, ctx_hbm, wq_hbm, wk_hbm, wv_hbm),
        (m_shift, m_scale, m_gate, lat, ctx, wq, wk, wv),
    )
    loads = [pltpu.make_async_copy(a, b, load_sem.at[i]) for i, (a, b) in enumerate(pairs)]
    for load in loads:
        load.start()
    pl.semaphore_wait(barrier, N_SP - 1 + N_TP - 1)

    def send(src, dst, s_sem, r_sem, target):
        return pltpu.make_async_remote_copy(
            src_ref=src, dst_ref=dst, send_sem=s_sem, recv_sem=r_sem,
            device_id=target, device_id_type=MESH,
        )

    def x_copy(i, src, to_row, count, k):
        return send(src, xbuf.at[pl.ds(to_row, count)], x_send.at[i], x_recv.at[i], tp_at(k))

    ra = x_copy(0, lat_hbm.at[pl.ds(0, 64)], 0, 64, 1)
    la = x_copy(1, lat_hbm.at[pl.ds(half, 64)], 96, 64, 3)
    rb = x_copy(2, lat_hbm.at[pl.ds(64, 32)], 64, 32, 1)
    lb = x_copy(3, lat_hbm.at[pl.ds(half + 64, 32)], 160, 32, 3)
    rc = x_copy(4, lat_hbm.at[pl.ds(half, half)], 192, half, 1)
    lc = x_copy(5, lat_hbm.at[pl.ds(0, half)], 288, half, 3)
    rf = x_copy(6, xbuf.at[pl.ds(0, half)], 384, half, 1)
    lf = x_copy(7, xbuf.at[pl.ds(half, half)], 480, half, 3)
    x_copies = [ra, la, rb, lb, rc, lc, rf, lf]
    ra.start()
    la.start()

    at = lax.broadcasted_iota(jnp.int32, (16, 128), 0)
    given = jnp.where(
        at == 0,
        jnp.broadcast_to(cond[...].astype(F32), (16, 128)),
        jnp.where(at == 1, jnp.broadcast_to(condc[...].astype(F32), (16, 128)), 0.0),
    )
    for load in loads[0:3]:
        load.wait()
    active = (given / (1.0 + jnp.exp(-given))).astype(BF16)
    for k, weight in enumerate((m_shift, m_scale, m_gate)):
        product = jnp.dot(active, weight[...], preferred_element_type=F32)
        for r in range(2):
            for c in range(4):
                i = r * 12 + k * 4 + c
                part[i : i + 1, :] = product[r : r + 1, c * 128 : (c + 1) * 128]
    p_copies = [
        send(part, psum_in.at[k - 1], p_send.at[k - 1], p_recv.at[k - 1], sp_at(k))
        for k in range(1, N_SP)
    ]
    for copy in p_copies:
        copy.start()

    for load in loads[3:]:
        load.wait()
    wall[:, 0:256] = wq[...]
    wall[:, 256:384] = jnp.concatenate([wk[...], wv[...]], axis=0).T

    for copy in p_copies:
        copy.wait_recv()
    total = part[...]
    for k in range(N_SP - 1):
        total = total + psum_in[k]
    mine[...] = total
    full[tp] = total
    t_copies = [
        send(mine, full.at[tp], t_send.at[k - 1], t_recv.at[k - 1], tp_at(k))
        for k in range(1, N_TP)
    ]
    for copy in t_copies:
        copy.start()
    for copy in (rb, lb, rc, lc):
        copy.start()

    row_id = lax.broadcasted_iota(jnp.int32, (HD, GRID_W), 0)
    lane_id = lax.broadcasted_iota(jnp.int32, (HD, GRID_W), 1)
    even = lax.rem(row_id, 2) == 0
    left, right, opposite = (lax.rem(tp + k, N_TP) * rows for k in (3, 1, 2))
    for g in range(6):
        n = lane_id + g * 128
        shift = jnp.where(
            n < 192,
            tp * rows,
            jnp.where(
                n < 288,
                left - 192,
                jnp.where(
                    n < 384,
                    right - 192,
                    jnp.where(
                        n < 480,
                        left - 288,
                        jnp.where(n < 576, right - 480, opposite - 576),
                    ),
                ),
            ),
        )
        at_token = n + shift + sp * 768
        grid_at = jnp.where(row_id < 32, at_token >> 7, at_token & 127)
        angle = table[...] * grid_at.astype(F32)
        cosb[g] = jnp.cos(angle)
        sine = jnp.sin(angle)
        sinb[g] = jnp.where(even, -sine, sine)

    w_load = pltpu.make_async_copy(w_hbm, w, w_sem)
    w_load.start()
    for copy in t_copies:
        copy.wait_recv()

    def vector(r, k):
        pieces = [
            full[t, r * 12 + k * 4 + c : r * 12 + k * 4 + c + 1, :]
            for t in range(N_TP)
            for c in range(4)
        ]
        return jnp.concatenate(pieces, axis=1)

    gains = gain[...].astype(F32)
    gains = jnp.concatenate([gains[i : i + 1, :] for i in range(width // 128)], axis=1)
    for r in range(2):
        scl[r] = jnp.broadcast_to(gains * (1.0 + vector(r, 1)), (8, width))
        sft[r] = jnp.broadcast_to(vector(r, 0), (8, width))
    gate_out[...] = vector(0, 2)

    def modulate(src, r, count):
        values = src.astype(F32)
        inverse = lax.rsqrt(jnp.mean(values * values, axis=-1, keepdims=True) + EPS)
        normed = (values * inverse).reshape(count // 8, 8, width)
        return (normed * scl[r][None] + sft[r][None]).reshape(count, width).astype(BF16)

    uc = modulate(ctx[...], 1, ctx.shape[0])
    craw = jnp.dot(uc, wall[:, 256:384], preferred_element_type=F32)
    lane = lax.broadcasted_iota(jnp.int32, craw.shape, 1)
    square = jnp.where(lane < HD, craw * craw, 0.0)
    mean = jnp.sum(square, axis=-1, keepdims=True) * (1.0 / HD)
    k_row = kg[...].astype(F32)
    keys = craw * lax.rsqrt(mean + EPS) * jnp.concatenate([k_row, jnp.ones((1, HD), F32)], axis=1)
    cbuf[pl.ds(0, 32), :] = jnp.where(lane < HD, keys, craw).astype(BF16)

    def project(x, first, to_row, between=None):
        @pl.loop(0, rows // 32)
        def _(i):
            at_rows = pl.ds(pl.multiple_of(i * 32, 32), 32)
            from_rows = pl.ds(pl.multiple_of(first + i * 32, 32), 32)
            ubuf[at_rows, :] = modulate(x[from_rows, :], 0, 32)

        if between is not None:
            between()
        raw[pl.ds(to_row, rows), :] = jnp.dot(ubuf[...], wall[...], preferred_element_type=F32)

    def column(ref):
        r = lax.broadcasted_iota(jnp.int32, (HD, HD), 0)
        c = lax.broadcasted_iota(jnp.int32, (HD, HD), 1)
        spread = jnp.broadcast_to(ref[...].astype(F32), (HD, HD))
        return jnp.sum(jnp.where(r == c, spread, 0.0), axis=1, keepdims=True)

    q_gain = column(qg)
    k_gain = column(kg)

    def turned(x, gain_column, g):
        square = jnp.sum(x * x, axis=0, keepdims=True) * (1.0 / HD)
        normed = x * lax.rsqrt(square + EPS) * gain_column
        up = pltpu.roll(normed, HD - 1, axis=0)
        down = pltpu.roll(normed, 1, axis=0)
        return normed * cosb[g] + jnp.where(even, up, down) * sinb[g]

    scale = LOG2E * HD ** (-0.5)

    def finish_kv(s):
        slot = s * N_SP
        for i in range(3):
            g = 3 * s + i
            side = raw[g * 128 : (g + 1) * 128, 256:384].T
            k = turned(side[0:HD], k_gain, g).T
            kvbuf[slot, i * 64 : (i + 1) * 64, :] = jnp.concatenate(
                [k[0:64], k[64:128]], axis=1
            ).astype(BF16)
        order = [(g, p) for p in range(2) for g in (3 * s, 3 * s + 1, 3 * s + 2)]
        for b in range(3):
            pieces = [
                raw[g * 128 + p * 64 : g * 128 + p * 64 + 64, 256:384]
                for g, p in order[2 * b : 2 * b + 2]
            ]
            side = jnp.concatenate(pieces, axis=0).T
            at_row = 192 + b * 64
            kvbuf[slot, at_row : at_row + 64, :] = side[HD : 2 * HD].astype(BF16)

    def finish_q(blocks):
        for g in blocks:
            block = raw[g * 128 : (g + 1) * 128, :]
            for pair in range(2):
                side = block[:, pair * 128 : (pair + 1) * 128].T
                for h in range(2):
                    q = turned(side[h * HD : (h + 1) * HD], q_gain, g)
                    at_lane = g * 512 + (pair * 2 + h) * 128
                    q_out[:, at_lane : at_lane + 128] = (q * scale).astype(BF16)

    kv_copies = [[], []]
    for s in range(2):
        for i, (here, there, dy, dz, part_of) in enumerate(SENDS):
            here, there = here + s * N_SP, there + s * N_SP
            half_of = pl.ds(192 * part_of, 192)
            kv_copies[s].append(
                send(
                    kvbuf.at[here, half_of], kvbuf.at[there, half_of],
                    kv_send.at[i + s * len(SENDS)], kv_recv.at[2 * there + part_of], near(dy, dz),
                )
            )

    def start_from(s, slot):
        for copy, (here, _, _, _, _) in zip(kv_copies[s], SENDS):
            if here == slot:
                copy.start()

    def keep(s, slot):
        slot = slot + s * N_SP
        return pltpu.make_async_copy(kvbuf.at[slot], kv_all.at[slot], keep_sem.at[slot])

    def arrive(s, slot):
        for copy, (_, there, _, _, _) in zip(kv_copies[s], SENDS):
            if there == slot:
                copy.wait_recv()
        start_from(s, slot)
        keep(s, slot).start()

    lifts = jnp.concatenate([jnp.full((1, 128), lift[h] * LOG2E, F32) for h in range(4)], axis=1)
    lifts = jnp.concatenate([lifts] * (TILE // 512), axis=1)
    ones = jnp.ones((VROWS - HD, 768), BF16)

    def lanes(t):
        if isinstance(t, int):
            return pl.ds(t * TILE, TILE)
        return pl.ds(pl.multiple_of(t * TILE, TILE), TILE)

    def narrow(t, n):
        start = t * TILE + n * NARROW
        return pl.ds(start if isinstance(t, int) else pl.multiple_of(start, NARROW), NARROW)

    def context(t):
        cv = cbuf[...].astype(F32).T[HD : 2 * HD].astype(BF16)
        cv = jnp.concatenate([cv, ones[:, 0:512]], axis=0)
        scores = jnp.dot(cbuf[...], tall(q_out[:, lanes(t)]), preferred_element_type=F32) + lifts
        top = jnp.max(scores, axis=0, keepdims=True)
        peak[:, lanes(t)] = top
        weights = jnp.exp2(scores - top).astype(BF16)
        acc[:, lanes(t)] = jnp.dot(cv, weights, preferred_element_type=F32)

    def query_forms(at_lanes):
        q = q_out[:, at_lanes]
        return tall(q), jnp.concatenate([jnp.zeros_like(q), q], axis=0)

    def values_of(pair):
        v = [kvbuf[pair * 2 + s, pl.ds(192 + i * 64, 64), :] for s in range(2) for i in range(3)]
        return jnp.concatenate([jnp.concatenate(v, axis=1), ones], axis=0)

    def work(now, then, read, write):
        if now is not None:
            v = values_of(now[0])
        for n in range(TILE // NARROW):
            cols = slice(n * NARROW, (n + 1) * NARROW)
            if then is not None:
                theirs = narrow(then[1], n)
                forms = query_forms(theirs)
                top = peak[:, theirs]
            total = None
            for i in range(4):
                if then is not None:
                    s, p = i % 2, i // 2
                    k = kvbuf[then[0] * 2 + s, pl.ds(0, 192), :]
                    x = jnp.dot(k, forms[p], preferred_element_type=F32)
                    write[pl.ds(s * 384 + p * 192, 192), cols] = jnp.exp2(x - top).astype(BF16)
                if now is not None and i < 3:
                    term = jnp.dot(
                        v[:, i * 256 : (i + 1) * 256], read[pl.ds(i * 256, 256), cols],
                        preferred_element_type=F32,
                    )
                    total = term if total is None else total + term
            if now is not None:
                acc[:, narrow(now[1], n)] += total

    def unit(j):
        i = j - 16
        late = jnp.where(i < 6, i + 8, jnp.where(i == 6, 8, jnp.where(i < 9, i + 7, i)))
        pair = jnp.where(
            j < 2 * FIRST, j - FIRST, jnp.where(j < 16, FIRST + (j - 2 * FIRST) // 2, late)
        )
        late = jnp.where(i < 6, 1, jnp.where(i == 6, 0, jnp.where(i < 9, 1, 0)))
        tile = jnp.where(j < 2 * FIRST, 1, jnp.where(j < 16, lax.rem(j, 2), late))
        return pair, tile

    c_copies = [
        send(
            cbuf.at[pl.ds(0, 32)], cbuf.at[pl.ds(32 * k, 32)],
            c_send.at[k - 1], c_recv.at[k - 1], sp_at(k),
        )
        for k in range(1, N_SP)
    ]

    def start_context():
        for copy in c_copies:
            copy.start()

    project(lat, 0, 0, start_context)
    ra.wait_recv()
    rb.wait_recv()
    rf.start()
    la.wait_recv()
    lb.wait_recv()
    lf.start()
    project(xbuf, 0, 192)
    finish_kv(0)
    finish_q((0,))
    arrive(0, 0)
    finish_q((1, 2))
    for copy in c_copies:
        copy.wait_recv()
    context(0)
    arrive(0, 1)
    work(None, (0, 0), None, p_even)

    for j in range(FIRST - 1):
        arrive(0, 2 * j + 2)
        arrive(0, 2 * j + 3)
        work((j, 0), (j + 1, 0), *((p_even, p_odd) if j % 2 == 0 else (p_odd, p_even)))
        if j == 2:
            rc.wait_recv()
            lc.wait_recv()
            project(xbuf, 192, 384)
    work((FIRST - 1, 0), None, p_even, None)

    rf.wait_recv()
    lf.wait_recv()
    project(xbuf, 384, 576)
    finish_kv(1)
    finish_q((3,))
    arrive(1, 0)
    finish_q((4, 5))
    context(1)
    keep_rest = [
        pltpu.make_async_copy(q_out, q_all, keep_sem.at[2 * N_SP]),
        pltpu.make_async_copy(cbuf, ctx_all, keep_sem.at[2 * N_SP + 1]),
    ]
    for copy in keep_rest:
        copy.start()
    work(None, (0, 1), None, p_even)

    events = [(0, 0, (10, 11)), (1, 0, (12, 13)), (1, 1, (1, 2, 3, 4)), (3, 0, (14, 15)),
              (4, 1, (5, 7, 8)), (5, 1, (6, 9)), (6, 1, (10,)), (7, 1, (11, 12)),
              (8, 1, (13, 14)), (9, 1, (15,))]

    def second_step(d, carry):
        for when, s, slots in events:

            @pl.when(d == when)
            def _(s=s, slots=slots):
                for slot in slots:
                    arrive(s, slot)

        j = FIRST + 2 * d
        work(unit(j), unit(j + 1), p_even, p_odd)
        work(unit(j + 1), unit(j + 2), p_odd, p_even)
        return carry

    returns = [
        send(
            o_out.at[pl.ds(here, count)], obuf.at[tp, pl.ds(there, count)],
            o_send.at[i], o_recv.at[i], tp_at(k),
        )
        for i, (k, here, there, count) in enumerate(RETURNS)
    ]

    def finish_o(blocks):
        for g in blocks:
            at_lanes = pl.ds(g * 512, 512)
            mean = acc[0:HD, at_lanes] / acc[HD : HD + 1, at_lanes]
            stack = jnp.concatenate([mean[:, h * 128 : (h + 1) * 128] for h in range(4)], axis=0)
            o_out[g * 128 : (g + 1) * 128, :] = stack.T.astype(BF16)

    steps = (UNITS - 1 - FIRST) // 2
    lax.fori_loop(0, steps - 3, second_step, 0)
    finish_o((3, 4, 5))
    lax.fori_loop(steps - 3, steps - 2, second_step, 0)
    for copy, (_, here, _, _) in zip(returns, RETURNS):
        if here >= 384:
            copy.start()
    lax.fori_loop(steps - 2, steps, second_step, 0)
    work((15, 0), None, p_even, None)
    finish_o((1, 2))
    l_out[...] = acc[HD : HD + 8, :]
    peaks = acc[HD : HD + 1, 0:128]
    for i in range(1, 24):
        peaks = jnp.maximum(peaks, acc[HD : HD + 1, i * 128 : (i + 1) * 128])
    flag[...] = jnp.broadcast_to(peaks, (8, 128))
    fbuf[tp] = flag[...]
    finish_o((0,))
    for copy, (_, here, _, _) in zip(returns, RETURNS):
        if here < 384:
            copy.start()
    flags = [
        send(flag, fbuf.at[tp], f_send.at[k - 1], f_recv.at[k - 1], tp_at(k))
        for k in range(1, N_TP)
    ]
    for copy in flags:
        copy.start()
    obuf[tp] = o_out[0:rows, :]
    w_load.wait()
    wide = 512

    def heads(source, cols):
        feature = pl.ds(pl.multiple_of(source * 256, 256), 256)
        return jnp.dot(obuf[source], w[feature, cols], preferred_element_type=F32)

    for n in range(width // wide):
        cols = slice(n * wide, (n + 1) * wide)
        summed[:, cols] = heads(tp, cols)
    for copy in returns + flags:
        copy.wait_recv()
    for n in range(width // wide):
        cols = slice(n * wide, (n + 1) * wide)
        others = sum(heads(lax.rem(tp + k, N_TP), cols) for k in range(1, N_TP))
        mixed_out[:, cols] = (
            lat[:, cols].astype(F32) + gate_out[:, cols] * (summed[:, cols] + others)
        ).astype(BF16)
    flag_out[0] = (jnp.max(fbuf[...]) < 2.0**100).astype(jnp.int32)
    waiting = x_copies + p_copies + t_copies + c_copies + kv_copies[0] + kv_copies[1]
    for copy in waiting + returns + flags:
        copy.wait_send()
    for s in range(2):
        for slot in range(N_SP):
            keep(s, slot).wait()
    for copy in keep_rest:
        copy.wait()


def run_attention(lat, cond, condc, ctx, gain, ms, mc, mg, wq, wk, wv, qg, kg, lift, w_out):
    rows, width = lat.shape
    dma = pltpu.SemaphoreType.DMA
    loaded = (lat, ctx, ms, mc, mg, wq, wk, wv)
    return pl.pallas_call(
        attention_kernel,
        name="attention",
        out_shape=(
            jax.ShapeDtypeStruct((rows, width), BF16),
            jax.ShapeDtypeStruct((1,), jnp.int32),
            jax.ShapeDtypeStruct((768, 256), BF16),
            jax.ShapeDtypeStruct((8, 3072), F32),
            jax.ShapeDtypeStruct((HD, 3072), BF16),
            jax.ShapeDtypeStruct((2 * N_SP, 384, 128), BF16),
            jax.ShapeDtypeStruct((512, 128), BF16),
            jax.ShapeDtypeStruct((1, width), F32),
        ),
        in_specs=[HBM] * 9 + [VMEM] * 6 + [SMEM],
        out_specs=(VMEM, SMEM, VMEM, VMEM, HBM, HBM, HBM, VMEM),
        scratch_shapes=[
            pltpu.VMEM((3 * rows, width), BF16),
            pltpu.VMEM((24, 128), F32),
            pltpu.VMEM((N_SP - 1, 24, 128), F32),
            pltpu.VMEM((24, 128), F32),
            pltpu.VMEM((N_TP, 24, 128), F32),
            pltpu.VMEM((width, 384), BF16),
            pltpu.VMEM((rows, width), BF16),
            pltpu.VMEM((768, 384), F32),
            pltpu.VMEM((6, HD, GRID_W), F32),
            pltpu.VMEM((6, HD, GRID_W), F32),
            pltpu.VMEM((2, 8, width), F32),
            pltpu.VMEM((2, 8, width), F32),
            pltpu.VMEM((512, 128), BF16),
            pltpu.VMEM((HD, 3072), BF16),
            pltpu.VMEM((2 * N_SP, 384, 128), BF16),
            pltpu.VMEM((VROWS, 3072), F32),
            pltpu.VMEM((1, 3072), F32),
            pltpu.VMEM((768, TILE), BF16),
            pltpu.VMEM((768, TILE), BF16),
            *[pltpu.VMEM(a.shape, BF16) for a in loaded],
            dma((len(loaded),)),
            dma((8,)), dma((8,)), dma((15,)), dma((15,)),
            dma((3,)), dma((3,)), dma((15,)), dma((15,)),
            dma((2 * len(SENDS),)), dma((4 * N_SP,)), dma((2 * N_SP + 2,)),
            pltpu.VMEM((N_TP, rows, 256), BF16),
            pltpu.VMEM((N_TP, 8, 128), F32),
            pltpu.VMEM((8, 128), F32),
            pltpu.VMEM(w_out.shape, BF16),
            dma(()),
            pltpu.VMEM((rows, width), F32),
            dma((len(RETURNS),)), dma((len(RETURNS),)), dma((N_TP - 1,)), dma((N_TP - 1,)),
        ],
        compiler_params=pltpu.CompilerParams(
            collective_id=0, has_side_effects=True, vmem_limit_bytes=67043328
        ),
        cost_estimate=pl.CostEstimate(
            flops=2 * 10**10, bytes_accessed=10**7, transcendentals=4 * 10**7
        ),
    )(
        *loaded, w_out, cond, condc, gain, qg, kg, jnp.asarray(angle_table()), lift,
    )


def repair_kernel(
    l_ref, o_in, q_hbm, kv_hbm, ctx_hbm, lift, o_out,
    q_ref, kvbuf, ctx, acc, peak, sem,
):
    safe = jnp.all(l_ref[...] < 2.0**100)
    o_out[...] = o_in[...]

    @pl.when(jnp.logical_not(safe))
    def _():
        for src, dst in ((q_hbm, q_ref), (kv_hbm, kvbuf), (ctx_hbm, ctx)):
            copy = pltpu.make_async_copy(src, dst, sem)
            copy.start()
            copy.wait()
        wide = 512
        ones = jnp.ones((VROWS - HD, 768), BF16)
        lifts = jnp.concatenate(
            [jnp.full((1, 128), lift[h] * LOG2E, F32) for h in range(4)], axis=1
        )
        cv = ctx[...].astype(F32).T[HD : 2 * HD].astype(BF16)
        cv = jnp.concatenate([cv, ones[:, 0:512]], axis=0)

        @pl.loop(0, q_ref.shape[1] // wide)
        def _(t):
            lanes = pl.ds(pl.multiple_of(t * wide, wide), wide)
            q = q_ref[:, lanes]
            left = tall(q)
            right = jnp.concatenate([jnp.zeros_like(q), q], axis=0)
            scores = jnp.dot(ctx[...], left, preferred_element_type=F32) + lifts
            top = jnp.max(scores, axis=0, keepdims=True)
            peak[...] = top
            weights = jnp.exp2(scores - top).astype(BF16)
            acc[...] = jnp.dot(cv, weights, preferred_element_type=F32)

            @pl.loop(0, N_SP)
            def _(b):
                parts = []
                for s in range(2):
                    k = kvbuf[b * 2 + s, pl.ds(0, 192), :]
                    for query in (left, right):
                        parts.append(jnp.dot(k, query, preferred_element_type=F32))
                x = jnp.concatenate(parts, axis=0)
                old = peak[...]
                new = jnp.maximum(old, jnp.max(x, axis=0, keepdims=True))
                peak[...] = new
                v = [
                    kvbuf[b * 2 + s, pl.ds(192 + i * 64, 64), :] for s in range(2) for i in range(3)
                ]
                v = jnp.concatenate([jnp.concatenate(v, axis=1), ones], axis=0)
                weights = jnp.exp2(x - new).astype(BF16)
                acc[...] = acc[...] * jnp.exp2(old - new) + jnp.dot(
                    v, weights, preferred_element_type=F32
                )

            mean = acc[0:HD, :] / acc[HD : HD + 1, :]
            stack = jnp.concatenate([mean[:, h * 128 : (h + 1) * 128] for h in range(4)], axis=0)
            rows = pl.ds(pl.multiple_of(t * 128, 128), 128)
            o_out[rows, :] = stack.T.astype(BF16)


def run_repair(l, o, q, kv_all, ctx, lift):
    return pl.pallas_call(
        repair_kernel,
        name="repair",
        out_shape=jax.ShapeDtypeStruct(o.shape, o.dtype),
        in_specs=[VMEM, VMEM, HBM, HBM, HBM, SMEM],
        out_specs=VMEM,
        scratch_shapes=[
            pltpu.VMEM((HD, 3072), BF16),
            pltpu.VMEM((2 * N_SP, 384, 128), BF16),
            pltpu.VMEM((512, 128), BF16),
            pltpu.VMEM((VROWS, 512), F32),
            pltpu.VMEM((1, 512), F32),
            pltpu.SemaphoreType.DMA(()),
        ],
        compiler_params=pltpu.CompilerParams(vmem_limit_bytes=67043328),
    )(l, o, q, kv_all, ctx, lift)


def exchange_kernel(o_ref, out, obuf, send_sem, recv_sem):
    tp = lax.axis_index("tp")
    rows = o_ref.shape[0] // N_TP

    def tp_at(k):
        return {"tp": lax.rem(tp + k, N_TP)}

    barrier = pltpu.get_barrier_semaphore()
    for k in range(1, N_TP):
        pl.semaphore_signal(barrier, inc=1, device_id=tp_at(k), device_id_type=MESH)
    pl.semaphore_wait(barrier, N_TP - 1)
    copies = []
    for i, (k, here, there, count) in enumerate(RETURNS):
        copies.append(
            pltpu.make_async_remote_copy(
                src_ref=o_ref.at[pl.ds(here, count)],
                dst_ref=obuf.at[tp, pl.ds(there, count)],
                send_sem=send_sem.at[i], recv_sem=recv_sem.at[i],
                device_id=tp_at(k), device_id_type=MESH,
            )
        )
        copies[-1].start()
    out[tp] = o_ref[0:rows, :]
    for copy in copies:
        copy.wait_recv()
    for k in range(1, N_TP):
        source = lax.rem(tp + k, N_TP)
        out[source] = obuf[source]
    for copy in copies:
        copy.wait_send()


def run_exchange(o):
    rows = o.shape[0] // N_TP
    dma = pltpu.SemaphoreType.DMA
    return pl.pallas_call(
        exchange_kernel,
        name="exchange",
        out_shape=jax.ShapeDtypeStruct((N_TP, rows, 256), BF16),
        in_specs=[VMEM],
        out_specs=VMEM,
        scratch_shapes=[pltpu.VMEM((N_TP, rows, 256), BF16), dma((5,)), dma((5,))],
        compiler_params=pltpu.CompilerParams(
            collective_id=2, has_side_effects=True, vmem_limit_bytes=4 * 2**20
        ),
        cost_estimate=pl.CostEstimate(flops=0, bytes_accessed=25 * 10**6, transcendentals=0),
    )(o)


def output_kernel(o_hbm, w_hbm, lat_hbm, gate, out, o, w, lat, total, sem):
    pairs = [(o_hbm, o)]
    pairs += [(w_hbm.at[pl.ds(t * 256, 256)], w.at[t]) for t in range(N_TP)]
    pairs += [(lat_hbm, lat)]
    loads = [pltpu.make_async_copy(a, b, sem.at[i]) for i, (a, b) in enumerate(pairs)]
    for load in loads:
        load.start()
    loads[0].wait()
    wide = 512
    for t in range(N_TP):
        loads[1 + t].wait()
        if t == N_TP - 1:
            loads[-1].wait()
        for n in range(out.shape[1] // wide):
            cols = slice(n * wide, (n + 1) * wide)
            term = jnp.dot(o[t], w[t, :, cols], preferred_element_type=F32)
            if t == 0:
                total[:, cols] = term
            elif t < N_TP - 1:
                total[:, cols] += term
            else:
                term = total[:, cols] + term
                out[:, cols] = (lat[:, cols].astype(F32) + gate[:, cols] * term).astype(BF16)


def run_output(o, w_out, lat, gate):
    return pl.pallas_call(
        output_kernel,
        name="output",
        out_shape=jax.ShapeDtypeStruct(lat.shape, BF16),
        in_specs=[HBM, HBM, HBM, VMEM],
        out_specs=VMEM,
        scratch_shapes=[
            pltpu.VMEM(o.shape, BF16),
            pltpu.VMEM((N_TP, 256, w_out.shape[1]), BF16),
            pltpu.VMEM(lat.shape, BF16),
            pltpu.VMEM(lat.shape, F32),
            pltpu.SemaphoreType.DMA((N_TP + 2,)),
        ],
        compiler_params=pltpu.CompilerParams(vmem_limit_bytes=67043328),
    )(o, w_out, lat, gate)


def settle_kernel(mixed, out, buf, sem_in, sem_out):
    pieces = buf.shape[0]
    count = buf.shape[1]
    loads, stores = [], []
    for i in range(pieces):
        rows = pl.ds(i * count, count)
        loads.append(pltpu.make_async_copy(mixed.at[rows], buf.at[i], sem_in.at[i]))
        stores.append(pltpu.make_async_copy(buf.at[i], out.at[rows], sem_out.at[i]))
    for load in loads:
        load.start()
    for load, store in zip(loads, stores):
        load.wait()
        store.start()
    for store in stores:
        store.wait()


def run_settle(mixed):
    rows, width = mixed.shape
    return pl.pallas_call(
        settle_kernel,
        name="settle",
        out_shape=jax.ShapeDtypeStruct(mixed.shape, mixed.dtype),
        in_specs=[HBM],
        out_specs=HBM,
        scratch_shapes=[
            pltpu.VMEM((4, rows // 4, width), BF16),
            pltpu.SemaphoreType.DMA((4,)),
            pltpu.SemaphoreType.DMA((4,)),
        ],
        compiler_params=pltpu.CompilerParams(vmem_limit_bytes=67043328),
    )(mixed)


def on_device(
    latent, cond, cond_ctx, context, norm_gain, mod_shift, mod_scale, mod_gate,
    w_query, w_key, w_value, q_gain, k_gain, ctx_lift, w_out,
):
    lat = latent[0]
    mixed, safe, o, l, q, kv_all, ctx, gate = run_attention(
        lat, cond, cond_ctx[None, :], context[0], norm_gain.reshape(-1, 128),
        mod_shift, mod_scale, mod_gate, w_query, w_key.T, w_value.T,
        q_gain[None, :], k_gain[None, :], ctx_lift, w_out,
    )

    def again(mixed, o, l, q, kv_all, ctx):
        o = run_exchange(run_repair(l, o, q, kv_all, ctx, ctx_lift))
        return run_output(o, w_out, lat, gate)

    def keep(mixed, *rest):
        return mixed

    mixed = lax.cond(safe[0] > 0, keep, again, mixed, o, l, q, kv_all, ctx)
    return run_settle(mixed)[None]


def solution(mesh):
    in_specs = (
        P("dp", ("sp", "tp"), None),
        P("dp", "sp"),
        P("sp"),
        P("dp", "sp", None),
        P(),
        P("sp", "tp"),
        P("sp", "tp"),
        P("sp", "tp"),
        P(None, "tp"),
        P(None, "tp"),
        P(None, "tp"),
        P(),
        P(),
        P("tp"),
        P(),
    )
    return jax.shard_map(
        on_device, mesh=mesh, in_specs=in_specs,
        out_specs=P("dp", ("sp", "tp"), None), check_vma=False,
    )
```

```python
import functools

import jax
import jax.numpy as jnp
import numpy as np
from jax import lax
from jax.experimental import pallas as pl
from jax.experimental.pallas import tpu as pltpu
from jax.sharding import PartitionSpec as P

MESH = pl.DeviceIdType.MESH
HD = 64
GRID_W = 128
EPS = 1e-06
THETA = 10000.0
LOG2E = 1.4426950408889634
N_SP = 16
N_TP = 4
F32 = jnp.float32
BF16 = jnp.bfloat16
VMEM = pl.BlockSpec(memory_space=pltpu.VMEM)
HBM = pl.BlockSpec(memory_space=pltpu.HBM)
SMEM = pl.BlockSpec(memory_space=pltpu.SMEM)


def angle_table():
    i = (np.arange(HD) // 2) % 16
    f = (THETA ** (-(i.astype(np.float32)) / np.float32(16))).astype(np.float32)
    return np.repeat(f[:, None], GRID_W, axis=1)


def tall(x):
    return jnp.concatenate([x, jnp.zeros_like(x)], axis=0)


PLACES = [
    (0, 0), (-1, 0), (1, 0), (0, -1), (0, 1), (2, 0), (0, 2), (-1, -1),
    (-1, 1), (1, -1), (1, 1), (2, 1), (1, 2), (2, -1), (-1, 2), (2, 2),
]
SENDS = [
    (0, 1, 1, 0), (0, 2, -1, 0), (0, 3, 0, 1), (0, 4, 0, -1),
    (1, 5, 1, 0), (1, 7, 0, 1), (1, 8, 0, -1),
    (2, 9, 0, 1), (2, 10, 0, -1),
    (3, 6, 0, 1),
    (5, 11, 0, -1), (5, 13, 0, 1),
    (8, 14, 0, -1), (9, 12, 0, 1), (11, 15, 0, -1),
]
MIRROR = [
    next(i for i, q in enumerate(PLACES) if (q[0] % 4, q[1] % 4) == (p[1] % 4, p[0] % 4))
    for p in PLACES
]
SENDS = [(h, t, dy, dz, 0) for h, t, dy, dz in SENDS] + [
    (MIRROR[h], MIRROR[t], dz, dy, 1) for h, t, dy, dz in SENDS
]
TILE = 1536
NARROW = 512
VROWS = 80
FIRST = 5
UNITS = 32
RETURNS = [(2, 576, 0, 192), (3, 384, 96, 96), (1, 480, 0, 96), (3, 192, 0, 96), (1, 288, 96, 96)]


def attention_kernel(
    lat_hbm, ctx_hbm, ms_hbm, mc_hbm, mg_hbm, wq_hbm, wk_hbm, wv_hbm, w_hbm,
    cond, condc, gain, qg, kg, table, lift,
    mixed_out, flag_out, o_out, l_out, q_all, kv_all, ctx_all, gate_out,
    xbuf, part, psum_in, mine, full, wall, ubuf, raw, cosb, sinb, scl, sft, cbuf,
    q_out, kvbuf, acc, peak, p_even, p_odd, lat, ctx, m_shift, m_scale, m_gate, wq, wk, wv, load_sem,
    x_send, x_recv, p_send, p_recv, t_send, t_recv, c_send, c_recv, kv_send, kv_recv, keep_sem,
    obuf, fbuf, flag, w, w_sem, summed, o_send, o_recv, f_send, f_recv,
):
    sp = lax.axis_index("sp")
    tp = lax.axis_index("tp")
    y, z = lax.rem(sp, 4), lax.div(sp, 4)
    rows, width = lat.shape
    half = rows // 2

    def sp_at(k):
        return {"sp": lax.rem(sp + k, N_SP)}

    def tp_at(k):
        return {"tp": lax.rem(tp + k, N_TP)}

    def near(dy, dz):
        return {"sp": lax.rem(z + dz + 4, 4) * 4 + lax.rem(y + dy + 4, 4)}

    barrier = pltpu.get_barrier_semaphore()
    for k in range(1, N_SP):
        pl.semaphore_signal(barrier, inc=1, device_id=sp_at(k), device_id_type=MESH)
    for k in range(1, N_TP):
        pl.semaphore_signal(barrier, inc=1, device_id=tp_at(k), device_id_type=MESH)
    pairs = zip(
        (ms_hbm, mc_hbm, mg_hbm, lat_hbm, ctx_hbm, wq_hbm, wk_hbm, wv_hbm),
        (m_shift, m_scale, m_gate, lat, ctx, wq, wk, wv),
    )
    loads = [pltpu.make_async_copy(a, b, load_sem.at[i]) for i, (a, b) in enumerate(pairs)]
    for load in loads:
        load.start()
    pl.semaphore_wait(barrier, N_SP - 1 + N_TP - 1)

    def send(src, dst, s_sem, r_sem, target):
        return pltpu.make_async_remote_copy(
            src_ref=src, dst_ref=dst, send_sem=s_sem, recv_sem=r_sem,
            device_id=target, device_id_type=MESH,
        )

    def x_copy(i, src, to_row, count, k):
        return send(src, xbuf.at[pl.ds(to_row, count)], x_send.at[i], x_recv.at[i], tp_at(k))

    ra = x_copy(0, lat_hbm.at[pl.ds(0, 64)], 0, 64, 1)
    la = x_copy(1, lat_hbm.at[pl.ds(half, 64)], 96, 64, 3)
    rb = x_copy(2, lat_hbm.at[pl.ds(64, 32)], 64, 32, 1)
    lb = x_copy(3, lat_hbm.at[pl.ds(half + 64, 32)], 160, 32, 3)
    rc = x_copy(4, lat_hbm.at[pl.ds(half, half)], 192, half, 1)
    lc = x_copy(5, lat_hbm.at[pl.ds(0, half)], 288, half, 3)
    rf = x_copy(6, xbuf.at[pl.ds(0, half)], 384, half, 1)
    lf = x_copy(7, xbuf.at[pl.ds(half, half)], 480, half, 3)
    x_copies = [ra, la, rb, lb, rc, lc, rf, lf]
    ra.start()
    la.start()

    at = lax.broadcasted_iota(jnp.int32, (16, 128), 0)
    given = jnp.where(
        at == 0,
        jnp.broadcast_to(cond[...].astype(F32), (16, 128)),
        jnp.where(at == 1, jnp.broadcast_to(condc[...].astype(F32), (16, 128)), 0.0),
    )
    for load in loads[0:3]:
        load.wait()
    active = (given / (1.0 + jnp.exp(-given))).astype(BF16)
    for k, weight in enumerate((m_shift, m_scale, m_gate)):
        product = jnp.dot(active, weight[...], preferred_element_type=F32)
        for r in range(2):
            for c in range(4):
                i = r * 12 + k * 4 + c
                part[i : i + 1, :] = product[r : r + 1, c * 128 : (c + 1) * 128]
    p_copies = [
        send(part, psum_in.at[k - 1], p_send.at[k - 1], p_recv.at[k - 1], sp_at(k))
        for k in range(1, N_SP)
    ]
    for copy in p_copies:
        copy.start()

    for load in loads[3:]:
        load.wait()
    wall[:, 0:256] = wq[...]
    wall[:, 256:384] = jnp.concatenate([wk[...], wv[...]], axis=0).T

    for copy in p_copies:
        copy.wait_recv()
    total = part[...]
    for k in range(N_SP - 1):
        total = total + psum_in[k]
    mine[...] = total
    full[tp] = total
    t_copies = [
        send(mine, full.at[tp], t_send.at[k - 1], t_recv.at[k - 1], tp_at(k))
        for k in range(1, N_TP)
    ]
    for copy in t_copies:
        copy.start()
    for copy in (rb, lb, rc, lc):
        copy.start()

    row_id = lax.broadcasted_iota(jnp.int32, (HD, GRID_W), 0)
    lane_id = lax.broadcasted_iota(jnp.int32, (HD, GRID_W), 1)
    even = lax.rem(row_id, 2) == 0
    left, right, opposite = (lax.rem(tp + k, N_TP) * rows for k in (3, 1, 2))
    for g in range(6):
        n = lane_id + g * 128
        shift = jnp.where(
            n < 192,
            tp * rows,
            jnp.where(
                n < 288,
                left - 192,
                jnp.where(
                    n < 384,
                    right - 192,
                    jnp.where(
                        n < 480,
                        left - 288,
                        jnp.where(n < 576, right - 480, opposite - 576),
                    ),
                ),
            ),
        )
        at_token = n + shift + sp * 768
        grid_at = jnp.where(row_id < 32, at_token >> 7, at_token & 127)
        angle = table[...] * grid_at.astype(F32)
        cosb[g] = jnp.cos(angle)
        sine = jnp.sin(angle)
        sinb[g] = jnp.where(even, -sine, sine)

    w_load = pltpu.make_async_copy(w_hbm, w, w_sem)
    w_load.start()
    for copy in t_copies:
        copy.wait_recv()

    def vector(r, k):
        pieces = [
            full[t, r * 12 + k * 4 + c : r * 12 + k * 4 + c + 1, :]
            for t in range(N_TP)
            for c in range(4)
        ]
        return jnp.concatenate(pieces, axis=1)

    gains = gain[...].astype(F32)
    gains = jnp.concatenate([gains[i : i + 1, :] for i in range(width // 128)], axis=1)
    for r in range(2):
        scl[r] = jnp.broadcast_to(gains * (1.0 + vector(r, 1)), (8, width))
        sft[r] = jnp.broadcast_to(vector(r, 0), (8, width))
    gate_out[...] = vector(0, 2)

    def modulate(src, r, count):
        values = src.astype(F32)
        inverse = lax.rsqrt(jnp.mean(values * values, axis=-1, keepdims=True) + EPS)
        normed = (values * inverse).reshape(count // 8, 8, width)
        return (normed * scl[r][None] + sft[r][None]).reshape(count, width).astype(BF16)

    uc = modulate(ctx[...], 1, ctx.shape[0])
    craw = jnp.dot(uc, wall[:, 256:384], preferred_element_type=F32)
    lane = lax.broadcasted_iota(jnp.int32, craw.shape, 1)
    square = jnp.where(lane < HD, craw * craw, 0.0)
    mean = jnp.sum(square, axis=-1, keepdims=True) * (1.0 / HD)
    k_row = kg[...].astype(F32)
    keys = craw * lax.rsqrt(mean + EPS) * jnp.concatenate([k_row, jnp.ones((1, HD), F32)], axis=1)
    cbuf[pl.ds(0, 32), :] = jnp.where(lane < HD, keys, craw).astype(BF16)

    def project(x, first, to_row, between=None):
        @pl.loop(0, rows // 32)
        def _(i):
            at_rows = pl.ds(pl.multiple_of(i * 32, 32), 32)
            from_rows = pl.ds(pl.multiple_of(first + i * 32, 32), 32)
            ubuf[at_rows, :] = modulate(x[from_rows, :], 0, 32)

        if between is not None:
            between()
        raw[pl.ds(to_row, rows), :] = jnp.dot(ubuf[...], wall[...], preferred_element_type=F32)

    def column(ref):
        r = lax.broadcasted_iota(jnp.int32, (HD, HD), 0)
        c = lax.broadcasted_iota(jnp.int32, (HD, HD), 1)
        spread = jnp.broadcast_to(ref[...].astype(F32), (HD, HD))
        return jnp.sum(jnp.where(r == c, spread, 0.0), axis=1, keepdims=True)

    q_gain = column(qg)
    k_gain = column(kg)

    def turned(x, gain_column, g):
        square = jnp.sum(x * x, axis=0, keepdims=True) * (1.0 / HD)
        normed = x * lax.rsqrt(square + EPS) * gain_column
        up = pltpu.roll(normed, HD - 1, axis=0)
        down = pltpu.roll(normed, 1, axis=0)
        return normed * cosb[g] + jnp.where(even, up, down) * sinb[g]

    scale = LOG2E * HD ** (-0.5)

    def finish_kv(s):
        slot = s * N_SP
        for i in range(3):
            g = 3 * s + i
            side = raw[g * 128 : (g + 1) * 128, 256:384].T
            k = turned(side[0:HD], k_gain, g).T
            kvbuf[slot, i * 64 : (i + 1) * 64, :] = jnp.concatenate(
                [k[0:64], k[64:128]], axis=1
            ).astype(BF16)
        order = [(g, p) for p in range(2) for g in (3 * s, 3 * s + 1, 3 * s + 2)]
        for b in range(3):
            pieces = [
                raw[g * 128 + p * 64 : g * 128 + p * 64 + 64, 256:384]
                for g, p in order[2 * b : 2 * b + 2]
            ]
            side = jnp.concatenate(pieces, axis=0).T
            at_row = 192 + b * 64
            kvbuf[slot, at_row : at_row + 64, :] = side[HD : 2 * HD].astype(BF16)

    def finish_q(blocks):
        for g in blocks:
            block = raw[g * 128 : (g + 1) * 128, :]
            for pair in range(2):
                side = block[:, pair * 128 : (pair + 1) * 128].T
                for h in range(2):
                    q = turned(side[h * HD : (h + 1) * HD], q_gain, g)
                    at_lane = g * 512 + (pair * 2 + h) * 128
                    q_out[:, at_lane : at_lane + 128] = (q * scale).astype(BF16)

    kv_copies = [[], []]
    for s in range(2):
        for i, (here, there, dy, dz, part_of) in enumerate(SENDS):
            here, there = here + s * N_SP, there + s * N_SP
            half_of = pl.ds(192 * part_of, 192)
            kv_copies[s].append(
                send(
                    kvbuf.at[here, half_of], kvbuf.at[there, half_of],
                    kv_send.at[i + s * len(SENDS)], kv_recv.at[2 * there + part_of], near(dy, dz),
                )
            )

    def start_from(s, slot):
        for copy, (here, _, _, _, _) in zip(kv_copies[s], SENDS):
            if here == slot:
                copy.start()

    def keep(s, slot):
        slot = slot + s * N_SP
        return pltpu.make_async_copy(kvbuf.at[slot], kv_all.at[slot], keep_sem.at[slot])

    def arrive(s, slot):
        for copy, (_, there, _, _, _) in zip(kv_copies[s], SENDS):
            if there == slot:
                copy.wait_recv()
        start_from(s, slot)
        keep(s, slot).start()

    lifts = jnp.concatenate([jnp.full((1, 128), lift[h] * LOG2E, F32) for h in range(4)], axis=1)
    lifts = jnp.concatenate([lifts] * (TILE // 512), axis=1)
    ones = jnp.ones((VROWS - HD, 768), BF16)

    def lanes(t):
        if isinstance(t, int):
            return pl.ds(t * TILE, TILE)
        return pl.ds(pl.multiple_of(t * TILE, TILE), TILE)

    def narrow(t, n):
        start = t * TILE + n * NARROW
        return pl.ds(start if isinstance(t, int) else pl.multiple_of(start, NARROW), NARROW)

    def context(t):
        cv = cbuf[...].astype(F32).T[HD : 2 * HD].astype(BF16)
        cv = jnp.concatenate([cv, ones[:, 0:512]], axis=0)
        scores = jnp.dot(cbuf[...], tall(q_out[:, lanes(t)]), preferred_element_type=F32) + lifts
        top = jnp.max(scores, axis=0, keepdims=True)
        peak[:, lanes(t)] = top
        weights = jnp.exp2(scores - top).astype(BF16)
        acc[:, lanes(t)] = jnp.dot(cv, weights, preferred_element_type=F32)

    def query_forms(at_lanes):
        q = q_out[:, at_lanes]
        return tall(q), jnp.concatenate([jnp.zeros_like(q), q], axis=0)

    def values_of(pair):
        v = [kvbuf[pair * 2 + s, pl.ds(192 + i * 64, 64), :] for s in range(2) for i in range(3)]
        return jnp.concatenate([jnp.concatenate(v, axis=1), ones], axis=0)

    def work(now, then, read, write):
        if now is not None:
            v = values_of(now[0])
        for n in range(TILE // NARROW):
            cols = slice(n * NARROW, (n + 1) * NARROW)
            if then is not None:
                theirs = narrow(then[1], n)
                forms = query_forms(theirs)
                top = peak[:, theirs]
            total = None
            for i in range(4):
                if then is not None:
                    s, p = i % 2, i // 2
                    k = kvbuf[then[0] * 2 + s, pl.ds(0, 192), :]
                    x = jnp.dot(k, forms[p], preferred_element_type=F32)
                    write[pl.ds(s * 384 + p * 192, 192), cols] = jnp.exp2(x - top).astype(BF16)
                if now is not None and i < 3:
                    term = jnp.dot(
                        v[:, i * 256 : (i + 1) * 256], read[pl.ds(i * 256, 256), cols],
                        preferred_element_type=F32,
                    )
                    total = term if total is None else total + term
            if now is not None:
                acc[:, narrow(now[1], n)] += total

    def unit(j):
        i = j - 16
        late = jnp.where(i < 6, i + 8, jnp.where(i == 6, 8, jnp.where(i < 9, i + 7, i)))
        pair = jnp.where(
            j < 2 * FIRST, j - FIRST, jnp.where(j < 16, FIRST + (j - 2 * FIRST) // 2, late)
        )
        late = jnp.where(i < 6, 1, jnp.where(i == 6, 0, jnp.where(i < 9, 1, 0)))
        tile = jnp.where(j < 2 * FIRST, 1, jnp.where(j < 16, lax.rem(j, 2), late))
        return pair, tile

    c_copies = [
        send(
            cbuf.at[pl.ds(0, 32)], cbuf.at[pl.ds(32 * k, 32)],
            c_send.at[k - 1], c_recv.at[k - 1], sp_at(k),
        )
        for k in range(1, N_SP)
    ]

    def start_context():
        for copy in c_copies:
            copy.start()

    project(lat, 0, 0, start_context)
    ra.wait_recv()
    rb.wait_recv()
    rf.start()
    la.wait_recv()
    lb.wait_recv()
    lf.start()
    project(xbuf, 0, 192)
    finish_kv(0)
    finish_q((0,))
    arrive(0, 0)
    finish_q((1, 2))
    for copy in c_copies:
        copy.wait_recv()
    context(0)
    arrive(0, 1)
    work(None, (0, 0), None, p_even)

    turns = [0, 1, 2, 4, 3]
    for j in range(FIRST - 1):
        now, then = turns[j], turns[j + 1]
        arrive(0, 2 * then)
        arrive(0, 2 * then + 1)
        work((now, 0), (then, 0), *((p_even, p_odd) if j % 2 == 0 else (p_odd, p_even)))
        if j == 1:
            rc.wait_recv()
            lc.wait_recv()
            project(xbuf, 192, 384)
    work((turns[-1], 0), None, p_even, None)

    rf.wait_recv()
    lf.wait_recv()
    project(xbuf, 384, 576)
    finish_kv(1)
    finish_q((3,))
    arrive(1, 0)
    finish_q((4, 5))
    context(1)
    keep_rest = [
        pltpu.make_async_copy(q_out, q_all, keep_sem.at[2 * N_SP]),
        pltpu.make_async_copy(cbuf, ctx_all, keep_sem.at[2 * N_SP + 1]),
    ]
    for copy in keep_rest:
        copy.start()
    work(None, (0, 1), None, p_even)

    events = [(0, 0, (10, 11)), (1, 0, (12, 13)), (1, 1, (1, 2, 3, 4)), (3, 0, (14, 15)),
              (4, 1, (5, 7, 8)), (5, 1, (6, 9)), (6, 1, (10,)), (7, 1, (11, 12)),
              (8, 1, (13, 14)), (9, 1, (15,))]

    def second_step(d, carry):
        for when, s, slots in events:

            @pl.when(d == when)
            def _(s=s, slots=slots):
                for slot in slots:
                    arrive(s, slot)

        j = FIRST + 2 * d
        work(unit(j), unit(j + 1), p_even, p_odd)
        work(unit(j + 1), unit(j + 2), p_odd, p_even)
        return carry

    returns = [
        send(
            o_out.at[pl.ds(here, count)], obuf.at[tp, pl.ds(there, count)],
            o_send.at[i], o_recv.at[i], tp_at(k),
        )
        for i, (k, here, there, count) in enumerate(RETURNS)
    ]

    def finish_o(blocks):
        for g in blocks:
            at_lanes = pl.ds(g * 512, 512)
            mean = acc[0:HD, at_lanes] / acc[HD : HD + 1, at_lanes]
            stack = jnp.concatenate([mean[:, h * 128 : (h + 1) * 128] for h in range(4)], axis=0)
            o_out[g * 128 : (g + 1) * 128, :] = stack.T.astype(BF16)

    steps = (UNITS - 1 - FIRST) // 2
    lax.fori_loop(0, steps - 3, second_step, 0)
    finish_o((3, 4, 5))
    lax.fori_loop(steps - 3, steps - 2, second_step, 0)
    for copy, (_, here, _, _) in zip(returns, RETURNS):
        if here >= 384:
            copy.start()
    lax.fori_loop(steps - 2, steps, second_step, 0)
    work((15, 0), None, p_even, None)
    finish_o((1, 2))
    l_out[...] = acc[HD : HD + 8, :]
    peaks = acc[HD : HD + 1, 0:128]
    for i in range(1, 24):
        peaks = jnp.maximum(peaks, acc[HD : HD + 1, i * 128 : (i + 1) * 128])
    flag[...] = jnp.broadcast_to(peaks, (8, 128))
    fbuf[tp] = flag[...]
    finish_o((0,))
    for copy, (_, here, _, _) in zip(returns, RETURNS):
        if here < 384:
            copy.start()
    flags = [
        send(flag, fbuf.at[tp], f_send.at[k - 1], f_recv.at[k - 1], tp_at(k))
        for k in range(1, N_TP)
    ]
    for copy in flags:
        copy.start()
    obuf[tp] = o_out[0:rows, :]
    w_load.wait()
    wide = 512

    def heads(source, cols):
        feature = pl.ds(pl.multiple_of(source * 256, 256), 256)
        return jnp.dot(obuf[source], w[feature, cols], preferred_element_type=F32)

    for n in range(width // wide):
        cols = slice(n * wide, (n + 1) * wide)
        summed[:, cols] = heads(tp, cols)
    for copy in returns + flags:
        copy.wait_recv()
    for n in range(width // wide):
        cols = slice(n * wide, (n + 1) * wide)
        others = sum(heads(lax.rem(tp + k, N_TP), cols) for k in range(1, N_TP))
        mixed_out[:, cols] = (
            lat[:, cols].astype(F32) + gate_out[:, cols] * (summed[:, cols] + others)
        ).astype(BF16)
    flag_out[0] = (jnp.max(fbuf[...]) < 2.0**100).astype(jnp.int32)
    waiting = x_copies + p_copies + t_copies + c_copies + kv_copies[0] + kv_copies[1]
    for copy in waiting + returns + flags:
        copy.wait_send()
    for s in range(2):
        for slot in range(N_SP):
            keep(s, slot).wait()
    for copy in keep_rest:
        copy.wait()


def run_attention(lat, cond, condc, ctx, gain, ms, mc, mg, wq, wk, wv, qg, kg, lift, w_out):
    rows, width = lat.shape
    dma = pltpu.SemaphoreType.DMA
    loaded = (lat, ctx, ms, mc, mg, wq, wk, wv)
    return pl.pallas_call(
        attention_kernel,
        name="attention",
        out_shape=(
            jax.ShapeDtypeStruct((rows, width), BF16),
            jax.ShapeDtypeStruct((1,), jnp.int32),
            jax.ShapeDtypeStruct((768, 256), BF16),
            jax.ShapeDtypeStruct((8, 3072), F32),
            jax.ShapeDtypeStruct((HD, 3072), BF16),
            jax.ShapeDtypeStruct((2 * N_SP, 384, 128), BF16),
            jax.ShapeDtypeStruct((512, 128), BF16),
            jax.ShapeDtypeStruct((1, width), F32),
        ),
        in_specs=[HBM] * 9 + [VMEM] * 6 + [SMEM],
        out_specs=(VMEM, SMEM, VMEM, VMEM, HBM, HBM, HBM, VMEM),
        scratch_shapes=[
            pltpu.VMEM((3 * rows, width), BF16),
            pltpu.VMEM((24, 128), F32),
            pltpu.VMEM((N_SP - 1, 24, 128), F32),
            pltpu.VMEM((24, 128), F32),
            pltpu.VMEM((N_TP, 24, 128), F32),
            pltpu.VMEM((width, 384), BF16),
            pltpu.VMEM((rows, width), BF16),
            pltpu.VMEM((768, 384), F32),
            pltpu.VMEM((6, HD, GRID_W), F32),
            pltpu.VMEM((6, HD, GRID_W), F32),
            pltpu.VMEM((2, 8, width), F32),
            pltpu.VMEM((2, 8, width), F32),
            pltpu.VMEM((512, 128), BF16),
            pltpu.VMEM((HD, 3072), BF16),
            pltpu.VMEM((2 * N_SP, 384, 128), BF16),
            pltpu.VMEM((VROWS, 3072), F32),
            pltpu.VMEM((1, 3072), F32),
            pltpu.VMEM((768, TILE), BF16),
            pltpu.VMEM((768, TILE), BF16),
            *[pltpu.VMEM(a.shape, BF16) for a in loaded],
            dma((len(loaded),)),
            dma((8,)), dma((8,)), dma((15,)), dma((15,)),
            dma((3,)), dma((3,)), dma((15,)), dma((15,)),
            dma((2 * len(SENDS),)), dma((4 * N_SP,)), dma((2 * N_SP + 2,)),
            pltpu.VMEM((N_TP, rows, 256), BF16),
            pltpu.VMEM((N_TP, 8, 128), F32),
            pltpu.VMEM((8, 128), F32),
            pltpu.VMEM(w_out.shape, BF16),
            dma(()),
            pltpu.VMEM((rows, width), F32),
            dma((len(RETURNS),)), dma((len(RETURNS),)), dma((N_TP - 1,)), dma((N_TP - 1,)),
        ],
        compiler_params=pltpu.CompilerParams(
            collective_id=0, has_side_effects=True, vmem_limit_bytes=67043328
        ),
        cost_estimate=pl.CostEstimate(
            flops=2 * 10**10, bytes_accessed=10**7, transcendentals=4 * 10**7
        ),
    )(
        *loaded, w_out, cond, condc, gain, qg, kg, jnp.asarray(angle_table()), lift,
    )


def repair_kernel(
    l_ref, o_in, q_hbm, kv_hbm, ctx_hbm, lift, o_out,
    q_ref, kvbuf, ctx, acc, peak, sem,
):
    safe = jnp.all(l_ref[...] < 2.0**100)
    o_out[...] = o_in[...]

    @pl.when(jnp.logical_not(safe))
    def _():
        for src, dst in ((q_hbm, q_ref), (kv_hbm, kvbuf), (ctx_hbm, ctx)):
            copy = pltpu.make_async_copy(src, dst, sem)
            copy.start()
            copy.wait()
        wide = 512
        ones = jnp.ones((VROWS - HD, 768), BF16)
        lifts = jnp.concatenate(
            [jnp.full((1, 128), lift[h] * LOG2E, F32) for h in range(4)], axis=1
        )
        cv = ctx[...].astype(F32).T[HD : 2 * HD].astype(BF16)
        cv = jnp.concatenate([cv, ones[:, 0:512]], axis=0)

        @pl.loop(0, q_ref.shape[1] // wide)
        def _(t):
            lanes = pl.ds(pl.multiple_of(t * wide, wide), wide)
            q = q_ref[:, lanes]
            left = tall(q)
            right = jnp.concatenate([jnp.zeros_like(q), q], axis=0)
            scores = jnp.dot(ctx[...], left, preferred_element_type=F32) + lifts
            top = jnp.max(scores, axis=0, keepdims=True)
            peak[...] = top
            weights = jnp.exp2(scores - top).astype(BF16)
            acc[...] = jnp.dot(cv, weights, preferred_element_type=F32)

            @pl.loop(0, N_SP)
            def _(b):
                parts = []
                for s in range(2):
                    k = kvbuf[b * 2 + s, pl.ds(0, 192), :]
                    for query in (left, right):
                        parts.append(jnp.dot(k, query, preferred_element_type=F32))
                x = jnp.concatenate(parts, axis=0)
                old = peak[...]
                new = jnp.maximum(old, jnp.max(x, axis=0, keepdims=True))
                peak[...] = new
                v = [
                    kvbuf[b * 2 + s, pl.ds(192 + i * 64, 64), :] for s in range(2) for i in range(3)
                ]
                v = jnp.concatenate([jnp.concatenate(v, axis=1), ones], axis=0)
                weights = jnp.exp2(x - new).astype(BF16)
                acc[...] = acc[...] * jnp.exp2(old - new) + jnp.dot(
                    v, weights, preferred_element_type=F32
                )

            mean = acc[0:HD, :] / acc[HD : HD + 1, :]
            stack = jnp.concatenate([mean[:, h * 128 : (h + 1) * 128] for h in range(4)], axis=0)
            rows = pl.ds(pl.multiple_of(t * 128, 128), 128)
            o_out[rows, :] = stack.T.astype(BF16)


def run_repair(l, o, q, kv_all, ctx, lift):
    return pl.pallas_call(
        repair_kernel,
        name="repair",
        out_shape=jax.ShapeDtypeStruct(o.shape, o.dtype),
        in_specs=[VMEM, VMEM, HBM, HBM, HBM, SMEM],
        out_specs=VMEM,
        scratch_shapes=[
            pltpu.VMEM((HD, 3072), BF16),
            pltpu.VMEM((2 * N_SP, 384, 128), BF16),
            pltpu.VMEM((512, 128), BF16),
            pltpu.VMEM((VROWS, 512), F32),
            pltpu.VMEM((1, 512), F32),
            pltpu.SemaphoreType.DMA(()),
        ],
        compiler_params=pltpu.CompilerParams(vmem_limit_bytes=67043328),
    )(l, o, q, kv_all, ctx, lift)


def exchange_kernel(o_ref, out, obuf, send_sem, recv_sem):
    tp = lax.axis_index("tp")
    rows = o_ref.shape[0] // N_TP

    def tp_at(k):
        return {"tp": lax.rem(tp + k, N_TP)}

    barrier = pltpu.get_barrier_semaphore()
    for k in range(1, N_TP):
        pl.semaphore_signal(barrier, inc=1, device_id=tp_at(k), device_id_type=MESH)
    pl.semaphore_wait(barrier, N_TP - 1)
    copies = []
    for i, (k, here, there, count) in enumerate(RETURNS):
        copies.append(
            pltpu.make_async_remote_copy(
                src_ref=o_ref.at[pl.ds(here, count)],
                dst_ref=obuf.at[tp, pl.ds(there, count)],
                send_sem=send_sem.at[i], recv_sem=recv_sem.at[i],
                device_id=tp_at(k), device_id_type=MESH,
            )
        )
        copies[-1].start()
    out[tp] = o_ref[0:rows, :]
    for copy in copies:
        copy.wait_recv()
    for k in range(1, N_TP):
        source = lax.rem(tp + k, N_TP)
        out[source] = obuf[source]
    for copy in copies:
        copy.wait_send()


def run_exchange(o):
    rows = o.shape[0] // N_TP
    dma = pltpu.SemaphoreType.DMA
    return pl.pallas_call(
        exchange_kernel,
        name="exchange",
        out_shape=jax.ShapeDtypeStruct((N_TP, rows, 256), BF16),
        in_specs=[VMEM],
        out_specs=VMEM,
        scratch_shapes=[pltpu.VMEM((N_TP, rows, 256), BF16), dma((5,)), dma((5,))],
        compiler_params=pltpu.CompilerParams(
            collective_id=2, has_side_effects=True, vmem_limit_bytes=4 * 2**20
        ),
        cost_estimate=pl.CostEstimate(flops=0, bytes_accessed=25 * 10**6, transcendentals=0),
    )(o)


def output_kernel(o_hbm, w_hbm, lat_hbm, gate, out, o, w, lat, total, sem):
    pairs = [(o_hbm, o)]
    pairs += [(w_hbm.at[pl.ds(t * 256, 256)], w.at[t]) for t in range(N_TP)]
    pairs += [(lat_hbm, lat)]
    loads = [pltpu.make_async_copy(a, b, sem.at[i]) for i, (a, b) in enumerate(pairs)]
    for load in loads:
        load.start()
    loads[0].wait()
    wide = 512
    for t in range(N_TP):
        loads[1 + t].wait()
        if t == N_TP - 1:
            loads[-1].wait()
        for n in range(out.shape[1] // wide):
            cols = slice(n * wide, (n + 1) * wide)
            term = jnp.dot(o[t], w[t, :, cols], preferred_element_type=F32)
            if t == 0:
                total[:, cols] = term
            elif t < N_TP - 1:
                total[:, cols] += term
            else:
                term = total[:, cols] + term
                out[:, cols] = (lat[:, cols].astype(F32) + gate[:, cols] * term).astype(BF16)


def run_output(o, w_out, lat, gate):
    return pl.pallas_call(
        output_kernel,
        name="output",
        out_shape=jax.ShapeDtypeStruct(lat.shape, BF16),
        in_specs=[HBM, HBM, HBM, VMEM],
        out_specs=VMEM,
        scratch_shapes=[
            pltpu.VMEM(o.shape, BF16),
            pltpu.VMEM((N_TP, 256, w_out.shape[1]), BF16),
            pltpu.VMEM(lat.shape, BF16),
            pltpu.VMEM(lat.shape, F32),
            pltpu.SemaphoreType.DMA((N_TP + 2,)),
        ],
        compiler_params=pltpu.CompilerParams(vmem_limit_bytes=67043328),
    )(o, w_out, lat, gate)


def settle_kernel(mixed, out, buf, sem_in, sem_out):
    pieces = buf.shape[0]
    count = buf.shape[1]
    loads, stores = [], []
    for i in range(pieces):
        rows = pl.ds(i * count, count)
        loads.append(pltpu.make_async_copy(mixed.at[rows], buf.at[i], sem_in.at[i]))
        stores.append(pltpu.make_async_copy(buf.at[i], out.at[rows], sem_out.at[i]))
    for load in loads:
        load.start()
    for load, store in zip(loads, stores):
        load.wait()
        store.start()
    for store in stores:
        store.wait()


def run_settle(mixed):
    rows, width = mixed.shape
    return pl.pallas_call(
        settle_kernel,
        name="settle",
        out_shape=jax.ShapeDtypeStruct(mixed.shape, mixed.dtype),
        in_specs=[HBM],
        out_specs=HBM,
        scratch_shapes=[
            pltpu.VMEM((4, rows // 4, width), BF16),
            pltpu.SemaphoreType.DMA((4,)),
            pltpu.SemaphoreType.DMA((4,)),
        ],
        compiler_params=pltpu.CompilerParams(vmem_limit_bytes=67043328),
    )(mixed)


def on_device(
    latent, cond, cond_ctx, context, norm_gain, mod_shift, mod_scale, mod_gate,
    w_query, w_key, w_value, q_gain, k_gain, ctx_lift, w_out,
):
    lat = latent[0]
    mixed, safe, o, l, q, kv_all, ctx, gate = run_attention(
        lat, cond, cond_ctx[None, :], context[0], norm_gain.reshape(-1, 128),
        mod_shift, mod_scale, mod_gate, w_query, w_key.T, w_value.T,
        q_gain[None, :], k_gain[None, :], ctx_lift, w_out,
    )

    def again(mixed, o, l, q, kv_all, ctx):
        o = run_exchange(run_repair(l, o, q, kv_all, ctx, ctx_lift))
        return run_output(o, w_out, lat, gate)

    def keep(mixed, *rest):
        return mixed

    mixed = lax.cond(safe[0] > 0, keep, again, mixed, o, l, q, kv_all, ctx)
    return run_settle(mixed)[None]


def solution(mesh):
    in_specs = (
        P("dp", ("sp", "tp"), None),
        P("dp", "sp"),
        P("sp"),
        P("dp", "sp", None),
        P(),
        P("sp", "tp"),
        P("sp", "tp"),
        P("sp", "tp"),
        P(None, "tp"),
        P(None, "tp"),
        P(None, "tp"),
        P(),
        P(),
        P("tp"),
        P(),
    )
    return jax.shard_map(
        on_device, mesh=mesh, in_specs=in_specs,
        out_specs=P("dp", ("sp", "tp"), None), check_vma=False,
    )
```

```python
import functools

import jax
import jax.numpy as jnp
import numpy as np
from jax import lax
from jax.experimental import pallas as pl
from jax.experimental.pallas import tpu as pltpu
from jax.sharding import PartitionSpec as P

MESH = pl.DeviceIdType.MESH
HD = 64
GRID_W = 128
EPS = 1e-06
THETA = 10000.0
LOG2E = 1.4426950408889634
N_SP = 16
N_TP = 4
F32 = jnp.float32
BF16 = jnp.bfloat16
VMEM = pl.BlockSpec(memory_space=pltpu.VMEM)
HBM = pl.BlockSpec(memory_space=pltpu.HBM)
SMEM = pl.BlockSpec(memory_space=pltpu.SMEM)


def angle_table():
    i = (np.arange(HD) // 2) % 16
    f = (THETA ** (-(i.astype(np.float32)) / np.float32(16))).astype(np.float32)
    return np.repeat(f[:, None], GRID_W, axis=1)


def tall(x):
    return jnp.concatenate([x, jnp.zeros_like(x)], axis=0)


PLACES = [
    (0, 0), (-1, 0), (1, 0), (0, -1), (0, 1), (2, 0), (0, 2), (-1, -1),
    (-1, 1), (1, -1), (1, 1), (2, 1), (1, 2), (2, -1), (-1, 2), (2, 2),
]
SENDS = [
    (0, 1, 1, 0), (0, 2, -1, 0), (0, 3, 0, 1), (0, 4, 0, -1),
    (1, 5, 1, 0), (1, 7, 0, 1), (1, 8, 0, -1),
    (2, 9, 0, 1), (2, 10, 0, -1),
    (3, 6, 0, 1),
    (5, 11, 0, -1), (5, 13, 0, 1),
    (8, 14, 0, -1), (9, 12, 0, 1), (11, 15, 0, -1),
]
MIRROR = [
    next(i for i, q in enumerate(PLACES) if (q[0] % 4, q[1] % 4) == (p[1] % 4, p[0] % 4))
    for p in PLACES
]
SENDS = [(h, t, dy, dz, 0) for h, t, dy, dz in SENDS] + [
    (MIRROR[h], MIRROR[t], dz, dy, 1) for h, t, dy, dz in SENDS
]
TILE = 1536
NARROW = 512
VROWS = 80
FIRST = 5
UNITS = 32
RETURNS = [(2, 576, 0, 192), (3, 384, 96, 96), (1, 480, 0, 96), (3, 192, 0, 96), (1, 288, 96, 96)]


def attention_kernel(
    lat_hbm, ctx_hbm, ms_hbm, mc_hbm, mg_hbm, wq_hbm, wk_hbm, wv_hbm, w_hbm,
    cond, condc, gain, qg, kg, table, lift,
    mixed_out, flag_out, o_all, l_all, q_all, kv_all, ctx_all, gate_out,
    xbuf, part, psum_in, mine, full, wall, ubuf, raw, cosb, sinb, scl, sft, cbuf,
    q_out, kvbuf, acc, peak, p_even, p_odd, lat, ctx, m_shift, m_scale, m_gate, wq, wk, wv, load_sem,
    x_send, x_recv, p_send, p_recv, t_send, t_recv, c_send, c_recv, kv_send, kv_recv, keep_sem,
    o_out, l_out, obuf, fbuf, flag, w, w_sem, summed, o_send, o_recv, f_send, f_recv,
):
    sp = lax.axis_index("sp")
    tp = lax.axis_index("tp")
    y, z = lax.rem(sp, 4), lax.div(sp, 4)
    rows, width = lat.shape
    half = rows // 2

    def sp_at(k):
        return {"sp": lax.rem(sp + k, N_SP)}

    def tp_at(k):
        return {"tp": lax.rem(tp + k, N_TP)}

    def near(dy, dz):
        return {"sp": lax.rem(z + dz + 4, 4) * 4 + lax.rem(y + dy + 4, 4)}

    barrier = pltpu.get_barrier_semaphore()
    for k in range(1, N_SP):
        pl.semaphore_signal(barrier, inc=1, device_id=sp_at(k), device_id_type=MESH)
    for k in range(1, N_TP):
        pl.semaphore_signal(barrier, inc=1, device_id=tp_at(k), device_id_type=MESH)
    pairs = zip(
        (ms_hbm, mc_hbm, mg_hbm, lat_hbm, ctx_hbm, wq_hbm, wk_hbm, wv_hbm),
        (m_shift, m_scale, m_gate, lat, ctx, wq, wk, wv),
    )
    loads = [pltpu.make_async_copy(a, b, load_sem.at[i]) for i, (a, b) in enumerate(pairs)]
    for load in loads:
        load.start()
    pl.semaphore_wait(barrier, N_SP - 1 + N_TP - 1)

    def send(src, dst, s_sem, r_sem, target):
        return pltpu.make_async_remote_copy(
            src_ref=src, dst_ref=dst, send_sem=s_sem, recv_sem=r_sem,
            device_id=target, device_id_type=MESH,
        )

    def x_copy(i, src, to_row, count, k):
        return send(src, xbuf.at[pl.ds(to_row, count)], x_send.at[i], x_recv.at[i], tp_at(k))

    ra = x_copy(0, lat_hbm.at[pl.ds(0, 64)], 0, 64, 1)
    la = x_copy(1, lat_hbm.at[pl.ds(half, 64)], 96, 64, 3)
    rb = x_copy(2, lat_hbm.at[pl.ds(64, 32)], 64, 32, 1)
    lb = x_copy(3, lat_hbm.at[pl.ds(half + 64, 32)], 160, 32, 3)
    rc = x_copy(4, lat_hbm.at[pl.ds(half, half)], 192, half, 1)
    lc = x_copy(5, lat_hbm.at[pl.ds(0, half)], 288, half, 3)
    rf = x_copy(6, xbuf.at[pl.ds(0, half)], 384, half, 1)
    lf = x_copy(7, xbuf.at[pl.ds(half, half)], 480, half, 3)
    x_copies = [ra, la, rb, lb, rc, lc, rf, lf]
    ra.start()
    la.start()

    at = lax.broadcasted_iota(jnp.int32, (16, 128), 0)
    given = jnp.where(
        at == 0,
        jnp.broadcast_to(cond[...].astype(F32), (16, 128)),
        jnp.where(at == 1, jnp.broadcast_to(condc[...].astype(F32), (16, 128)), 0.0),
    )
    for load in loads[0:3]:
        load.wait()
    active = (given / (1.0 + jnp.exp(-given))).astype(BF16)
    for k, weight in enumerate((m_shift, m_scale, m_gate)):
        product = jnp.dot(active, weight[...], preferred_element_type=F32)
        for r in range(2):
            for c in range(4):
                i = r * 12 + k * 4 + c
                part[i : i + 1, :] = product[r : r + 1, c * 128 : (c + 1) * 128]
    p_copies = [
        send(part, psum_in.at[k - 1], p_send.at[k - 1], p_recv.at[k - 1], sp_at(k))
        for k in range(1, N_SP)
    ]
    for copy in p_copies:
        copy.start()

    for load in loads[3:]:
        load.wait()
    wall[:, 0:256] = wq[...]
    wall[:, 256:384] = jnp.concatenate([wk[...], wv[...]], axis=0).T

    for copy in p_copies:
        copy.wait_recv()
    total = part[...]
    for k in range(N_SP - 1):
        total = total + psum_in[k]
    mine[...] = total
    full[tp] = total
    t_copies = [
        send(mine, full.at[tp], t_send.at[k - 1], t_recv.at[k - 1], tp_at(k))
        for k in range(1, N_TP)
    ]
    for copy in t_copies:
        copy.start()
    for copy in (rb, lb, rc, lc):
        copy.start()

    row_id = lax.broadcasted_iota(jnp.int32, (HD, GRID_W), 0)
    lane_id = lax.broadcasted_iota(jnp.int32, (HD, GRID_W), 1)
    even = lax.rem(row_id, 2) == 0
    left, right, opposite = (lax.rem(tp + k, N_TP) * rows for k in (3, 1, 2))
    for g in range(6):
        n = lane_id + g * 128
        shift = jnp.where(
            n < 192,
            tp * rows,
            jnp.where(
                n < 288,
                left - 192,
                jnp.where(
                    n < 384,
                    right - 192,
                    jnp.where(
                        n < 480,
                        left - 288,
                        jnp.where(n < 576, right - 480, opposite - 576),
                    ),
                ),
            ),
        )
        at_token = n + shift + sp * 768
        grid_at = jnp.where(row_id < 32, at_token >> 7, at_token & 127)
        angle = table[...] * grid_at.astype(F32)
        cosb[g] = jnp.cos(angle)
        sine = jnp.sin(angle)
        sinb[g] = jnp.where(even, -sine, sine)

    w_load = pltpu.make_async_copy(w_hbm, w, w_sem)
    w_load.start()
    for copy in t_copies:
        copy.wait_recv()

    def vector(r, k):
        pieces = [
            full[t, r * 12 + k * 4 + c : r * 12 + k * 4 + c + 1, :]
            for t in range(N_TP)
            for c in range(4)
        ]
        return jnp.concatenate(pieces, axis=1)

    gains = gain[...].astype(F32)
    gains = jnp.concatenate([gains[i : i + 1, :] for i in range(width // 128)], axis=1)
    for r in range(2):
        scl[r] = jnp.broadcast_to(gains * (1.0 + vector(r, 1)), (8, width))
        sft[r] = jnp.broadcast_to(vector(r, 0), (8, width))
    gate_out[...] = vector(0, 2)

    def modulate(src, r, count):
        values = src.astype(F32)
        inverse = lax.rsqrt(jnp.mean(values * values, axis=-1, keepdims=True) + EPS)
        normed = (values * inverse).reshape(count // 8, 8, width)
        return (normed * scl[r][None] + sft[r][None]).reshape(count, width).astype(BF16)

    uc = modulate(ctx[...], 1, ctx.shape[0])
    craw = jnp.dot(uc, wall[:, 256:384], preferred_element_type=F32)
    lane = lax.broadcasted_iota(jnp.int32, craw.shape, 1)
    square = jnp.where(lane < HD, craw * craw, 0.0)
    mean = jnp.sum(square, axis=-1, keepdims=True) * (1.0 / HD)
    k_row = kg[...].astype(F32)
    keys = craw * lax.rsqrt(mean + EPS) * jnp.concatenate([k_row, jnp.ones((1, HD), F32)], axis=1)
    cbuf[pl.ds(0, 32), :] = jnp.where(lane < HD, keys, craw).astype(BF16)

    def project(x, first, to_row, between=None):
        @pl.loop(0, rows // 32)
        def _(i):
            at_rows = pl.ds(pl.multiple_of(i * 32, 32), 32)
            from_rows = pl.ds(pl.multiple_of(first + i * 32, 32), 32)
            ubuf[at_rows, :] = modulate(x[from_rows, :], 0, 32)

        if between is not None:
            between()
        raw[pl.ds(to_row, rows), :] = jnp.dot(ubuf[...], wall[...], preferred_element_type=F32)

    def column(ref):
        r = lax.broadcasted_iota(jnp.int32, (HD, HD), 0)
        c = lax.broadcasted_iota(jnp.int32, (HD, HD), 1)
        spread = jnp.broadcast_to(ref[...].astype(F32), (HD, HD))
        return jnp.sum(jnp.where(r == c, spread, 0.0), axis=1, keepdims=True)

    q_gain = column(qg)
    k_gain = column(kg)

    def turned(x, gain_column, g):
        square = jnp.sum(x * x, axis=0, keepdims=True) * (1.0 / HD)
        normed = x * lax.rsqrt(square + EPS) * gain_column
        up = pltpu.roll(normed, HD - 1, axis=0)
        down = pltpu.roll(normed, 1, axis=0)
        return normed * cosb[g] + jnp.where(even, up, down) * sinb[g]

    scale = LOG2E * HD ** (-0.5)

    def finish_kv(s):
        slot = s * N_SP
        for i in range(3):
            g = 3 * s + i
            side = raw[g * 128 : (g + 1) * 128, 256:384].T
            k = turned(side[0:HD], k_gain, g).T
            kvbuf[slot, i * 64 : (i + 1) * 64, :] = jnp.concatenate(
                [k[0:64], k[64:128]], axis=1
            ).astype(BF16)
        order = [(g, p) for p in range(2) for g in (3 * s, 3 * s + 1, 3 * s + 2)]
        for b in range(3):
            pieces = [
                raw[g * 128 + p * 64 : g * 128 + p * 64 + 64, 256:384]
                for g, p in order[2 * b : 2 * b + 2]
            ]
            side = jnp.concatenate(pieces, axis=0).T
            at_row = 192 + b * 64
            kvbuf[slot, at_row : at_row + 64, :] = side[HD : 2 * HD].astype(BF16)

    def finish_q(blocks):
        for g in blocks:
            block = raw[g * 128 : (g + 1) * 128, :]
            for pair in range(2):
                side = block[:, pair * 128 : (pair + 1) * 128].T
                for h in range(2):
                    q = turned(side[h * HD : (h + 1) * HD], q_gain, g)
                    at_lane = g * 512 + (pair * 2 + h) * 128
                    q_out[:, at_lane : at_lane + 128] = (q * scale).astype(BF16)

    kv_copies = [[], []]
    for s in range(2):
        for i, (here, there, dy, dz, part_of) in enumerate(SENDS):
            here, there = here + s * N_SP, there + s * N_SP
            half_of = pl.ds(192 * part_of, 192)
            kv_copies[s].append(
                send(
                    kvbuf.at[here, half_of], kvbuf.at[there, half_of],
                    kv_send.at[i + s * len(SENDS)], kv_recv.at[2 * there + part_of], near(dy, dz),
                )
            )

    def start_from(s, slot):
        for copy, (here, _, _, _, _) in zip(kv_copies[s], SENDS):
            if here == slot:
                copy.start()

    def keep(s, slot):
        slot = slot + s * N_SP
        return pltpu.make_async_copy(kvbuf.at[slot], kv_all.at[slot], keep_sem.at[slot])

    def arrive(s, slot):
        for copy, (_, there, _, _, _) in zip(kv_copies[s], SENDS):
            if there == slot:
                copy.wait_recv()
        start_from(s, slot)
        keep(s, slot).start()

    lifts = jnp.concatenate([jnp.full((1, 128), lift[h] * LOG2E, F32) for h in range(4)], axis=1)
    lifts = jnp.concatenate([lifts] * (TILE // 512), axis=1)
    ones = jnp.ones((VROWS - HD, 768), BF16)

    def lanes(t):
        if isinstance(t, int):
            return pl.ds(t * TILE, TILE)
        return pl.ds(pl.multiple_of(t * TILE, TILE), TILE)

    def narrow(t, n):
        start = t * TILE + n * NARROW
        return pl.ds(start if isinstance(t, int) else pl.multiple_of(start, NARROW), NARROW)

    def context(t):
        cv = cbuf[...].astype(F32).T[HD : 2 * HD].astype(BF16)
        cv = jnp.concatenate([cv, ones[:, 0:512]], axis=0)
        scores = jnp.dot(cbuf[...], tall(q_out[:, lanes(t)]), preferred_element_type=F32) + lifts
        top = jnp.max(scores, axis=0, keepdims=True)
        peak[:, lanes(t)] = top
        weights = jnp.exp2(scores - top).astype(BF16)
        acc[:, lanes(t)] = jnp.dot(cv, weights, preferred_element_type=F32)

    def query_forms(at_lanes):
        q = q_out[:, at_lanes]
        return tall(q), jnp.concatenate([jnp.zeros_like(q), q], axis=0)

    def values_of(pair):
        v = [kvbuf[pair * 2 + s, pl.ds(192 + i * 64, 64), :] for s in range(2) for i in range(3)]
        return jnp.concatenate([jnp.concatenate(v, axis=1), ones], axis=0)

    def work(now, then, read, write):
        if now is not None:
            v = values_of(now[0])
        for n in range(TILE // NARROW):
            cols = slice(n * NARROW, (n + 1) * NARROW)
            if then is not None:
                theirs = narrow(then[1], n)
                forms = query_forms(theirs)
                top = peak[:, theirs]
            total = None
            for i in range(4):
                if then is not None:
                    s, p = i % 2, i // 2
                    k = kvbuf[then[0] * 2 + s, pl.ds(0, 192), :]
                    x = jnp.dot(k, forms[p], preferred_element_type=F32)
                    write[pl.ds(s * 384 + p * 192, 192), cols] = jnp.exp2(x - top).astype(BF16)
                if now is not None and i < 3:
                    term = jnp.dot(
                        v[:, i * 256 : (i + 1) * 256], read[pl.ds(i * 256, 256), cols],
                        preferred_element_type=F32,
                    )
                    total = term if total is None else total + term
            if now is not None:
                acc[:, narrow(now[1], n)] += total

    def unit(j):
        i = j - 16
        late = jnp.where(i < 6, i + 8, jnp.where(i == 6, 8, jnp.where(i < 9, i + 7, i)))
        pair = jnp.where(
            j < 2 * FIRST, j - FIRST, jnp.where(j < 16, FIRST + (j - 2 * FIRST) // 2, late)
        )
        late = jnp.where(i < 6, 1, jnp.where(i == 6, 0, jnp.where(i < 9, 1, 0)))
        tile = jnp.where(j < 2 * FIRST, 1, jnp.where(j < 16, lax.rem(j, 2), late))
        return pair, tile

    c_copies = [
        send(
            cbuf.at[pl.ds(0, 32)], cbuf.at[pl.ds(32 * k, 32)],
            c_send.at[k - 1], c_recv.at[k - 1], sp_at(k),
        )
        for k in range(1, N_SP)
    ]

    def start_context():
        for copy in c_copies:
            copy.start()

    project(lat, 0, 0, start_context)
    ra.wait_recv()
    rb.wait_recv()
    rf.start()
    la.wait_recv()
    lb.wait_recv()
    lf.start()
    project(xbuf, 0, 192)
    finish_kv(0)
    finish_q((0,))
    arrive(0, 0)
    finish_q((1, 2))
    for copy in c_copies:
        copy.wait_recv()
    context(0)
    arrive(0, 1)
    work(None, (0, 0), None, p_even)

    turns = [0, 1, 2, 4, 3]
    for j in range(FIRST - 1):
        now, then = turns[j], turns[j + 1]
        arrive(0, 2 * then)
        arrive(0, 2 * then + 1)
        work((now, 0), (then, 0), *((p_even, p_odd) if j % 2 == 0 else (p_odd, p_even)))
        if j == 1:
            rc.wait_recv()
            lc.wait_recv()
            project(xbuf, 192, 384)
    work((turns[-1], 0), None, p_even, None)

    rf.wait_recv()
    lf.wait_recv()
    project(xbuf, 384, 576)
    finish_kv(1)
    finish_q((3,))
    arrive(1, 0)
    finish_q((4, 5))
    context(1)
    keep_rest = [
        pltpu.make_async_copy(q_out, q_all, keep_sem.at[2 * N_SP]),
        pltpu.make_async_copy(cbuf, ctx_all, keep_sem.at[2 * N_SP + 1]),
    ]
    for copy in keep_rest:
        copy.start()
    work(None, (0, 1), None, p_even)

    events = [(0, 0, (10, 11)), (1, 0, (12, 13)), (1, 1, (1, 2, 3, 4)), (3, 0, (14, 15)),
              (4, 1, (5, 7, 8)), (5, 1, (6, 9)), (6, 1, (10,)), (7, 1, (11, 12)),
              (8, 1, (13, 14)), (9, 1, (15,))]

    def second_step(d, carry):
        for when, s, slots in events:

            @pl.when(d == when)
            def _(s=s, slots=slots):
                for slot in slots:
                    arrive(s, slot)

        j = FIRST + 2 * d
        work(unit(j), unit(j + 1), p_even, p_odd)
        work(unit(j + 1), unit(j + 2), p_odd, p_even)
        return carry

    returns = [
        send(
            o_out.at[pl.ds(here, count)], obuf.at[tp, pl.ds(there, count)],
            o_send.at[i], o_recv.at[i], tp_at(k),
        )
        for i, (k, here, there, count) in enumerate(RETURNS)
    ]

    def finish_o(blocks):
        for g in blocks:
            at_lanes = pl.ds(g * 512, 512)
            mean = acc[0:HD, at_lanes] / acc[HD : HD + 1, at_lanes]
            stack = jnp.concatenate([mean[:, h * 128 : (h + 1) * 128] for h in range(4)], axis=0)
            o_out[g * 128 : (g + 1) * 128, :] = stack.T.astype(BF16)

    steps = (UNITS - 1 - FIRST) // 2
    lax.fori_loop(0, steps - 3, second_step, 0)
    finish_o((3, 4, 5))
    lax.fori_loop(steps - 3, steps - 2, second_step, 0)
    for copy, (_, here, _, _) in zip(returns, RETURNS):
        if here >= 384:
            copy.start()
    lax.fori_loop(steps - 2, steps, second_step, 0)
    work((15, 0), None, p_even, None)
    finish_o((1, 2))
    l_out[...] = acc[HD : HD + 8, :]
    peaks = acc[HD : HD + 1, 0:128]
    for i in range(1, 24):
        peaks = jnp.maximum(peaks, acc[HD : HD + 1, i * 128 : (i + 1) * 128])
    flag[...] = jnp.broadcast_to(peaks, (8, 128))
    fbuf[tp] = flag[...]
    finish_o((0,))
    for copy, (_, here, _, _) in zip(returns, RETURNS):
        if here < 384:
            copy.start()
    flags = [
        send(flag, fbuf.at[tp], f_send.at[k - 1], f_recv.at[k - 1], tp_at(k))
        for k in range(1, N_TP)
    ]
    for copy in flags:
        copy.start()
    keep_rest += [
        pltpu.make_async_copy(o_out, o_all, keep_sem.at[2 * N_SP + 2]),
        pltpu.make_async_copy(l_out, l_all, keep_sem.at[2 * N_SP + 3]),
    ]
    for copy in keep_rest[2:]:
        copy.start()
    obuf[tp] = o_out[0:rows, :]
    w_load.wait()
    wide = 512

    def heads(source, cols):
        feature = pl.ds(pl.multiple_of(source * 256, 256), 256)
        return jnp.dot(obuf[source], w[feature, cols], preferred_element_type=F32)

    for n in range(width // wide):
        cols = slice(n * wide, (n + 1) * wide)
        summed[:, cols] = heads(tp, cols)
    for copy in returns + flags:
        copy.wait_recv()
    for n in range(width // wide):
        cols = slice(n * wide, (n + 1) * wide)
        others = sum(heads(lax.rem(tp + k, N_TP), cols) for k in range(1, N_TP))
        mixed_out[:, cols] = (
            lat[:, cols].astype(F32) + gate_out[:, cols] * (summed[:, cols] + others)
        ).astype(BF16)
    flag_out[0] = (jnp.max(fbuf[...]) < 2.0**100).astype(jnp.int32)
    waiting = x_copies + p_copies + t_copies + c_copies + kv_copies[0] + kv_copies[1]
    for copy in waiting + returns + flags:
        copy.wait_send()
    for s in range(2):
        for slot in range(N_SP):
            keep(s, slot).wait()
    for copy in keep_rest:
        copy.wait()


def run_attention(lat, cond, condc, ctx, gain, ms, mc, mg, wq, wk, wv, qg, kg, lift, w_out):
    rows, width = lat.shape
    dma = pltpu.SemaphoreType.DMA
    loaded = (lat, ctx, ms, mc, mg, wq, wk, wv)
    return pl.pallas_call(
        attention_kernel,
        name="attention",
        out_shape=(
            jax.ShapeDtypeStruct((rows, width), BF16),
            jax.ShapeDtypeStruct((1,), jnp.int32),
            jax.ShapeDtypeStruct((768, 256), BF16),
            jax.ShapeDtypeStruct((8, 3072), F32),
            jax.ShapeDtypeStruct((HD, 3072), BF16),
            jax.ShapeDtypeStruct((2 * N_SP, 384, 128), BF16),
            jax.ShapeDtypeStruct((512, 128), BF16),
            jax.ShapeDtypeStruct((1, width), F32),
        ),
        in_specs=[HBM] * 9 + [VMEM] * 6 + [SMEM],
        out_specs=(VMEM, SMEM, HBM, HBM, HBM, HBM, HBM, VMEM),
        scratch_shapes=[
            pltpu.VMEM((3 * rows, width), BF16),
            pltpu.VMEM((24, 128), F32),
            pltpu.VMEM((N_SP - 1, 24, 128), F32),
            pltpu.VMEM((24, 128), F32),
            pltpu.VMEM((N_TP, 24, 128), F32),
            pltpu.VMEM((width, 384), BF16),
            pltpu.VMEM((rows, width), BF16),
            pltpu.VMEM((768, 384), F32),
            pltpu.VMEM((6, HD, GRID_W), F32),
            pltpu.VMEM((6, HD, GRID_W), F32),
            pltpu.VMEM((2, 8, width), F32),
            pltpu.VMEM((2, 8, width), F32),
            pltpu.VMEM((512, 128), BF16),
            pltpu.VMEM((HD, 3072), BF16),
            pltpu.VMEM((2 * N_SP, 384, 128), BF16),
            pltpu.VMEM((VROWS, 3072), F32),
            pltpu.VMEM((1, 3072), F32),
            pltpu.VMEM((768, TILE), BF16),
            pltpu.VMEM((768, TILE), BF16),
            *[pltpu.VMEM(a.shape, BF16) for a in loaded],
            dma((len(loaded),)),
            dma((8,)), dma((8,)), dma((15,)), dma((15,)),
            dma((3,)), dma((3,)), dma((15,)), dma((15,)),
            dma((2 * len(SENDS),)), dma((4 * N_SP,)), dma((2 * N_SP + 4,)),
            pltpu.VMEM((768, 256), BF16),
            pltpu.VMEM((8, 3072), F32),
            pltpu.VMEM((N_TP, rows, 256), BF16),
            pltpu.VMEM((N_TP, 8, 128), F32),
            pltpu.VMEM((8, 128), F32),
            pltpu.VMEM(w_out.shape, BF16),
            dma(()),
            pltpu.VMEM((rows, width), F32),
            dma((len(RETURNS),)), dma((len(RETURNS),)), dma((N_TP - 1,)), dma((N_TP - 1,)),
        ],
        compiler_params=pltpu.CompilerParams(
            collective_id=0, has_side_effects=True, vmem_limit_bytes=67043328
        ),
        cost_estimate=pl.CostEstimate(
            flops=2 * 10**10, bytes_accessed=10**7, transcendentals=4 * 10**7
        ),
    )(
        *loaded, w_out, cond, condc, gain, qg, kg, jnp.asarray(angle_table()), lift,
    )


def repair_kernel(
    l_ref, o_in, q_hbm, kv_hbm, ctx_hbm, lift, o_out,
    q_ref, kvbuf, ctx, acc, peak, sem,
):
    safe = jnp.all(l_ref[...] < 2.0**100)
    o_out[...] = o_in[...]

    @pl.when(jnp.logical_not(safe))
    def _():
        for src, dst in ((q_hbm, q_ref), (kv_hbm, kvbuf), (ctx_hbm, ctx)):
            copy = pltpu.make_async_copy(src, dst, sem)
            copy.start()
            copy.wait()
        wide = 512
        ones = jnp.ones((VROWS - HD, 768), BF16)
        lifts = jnp.concatenate(
            [jnp.full((1, 128), lift[h] * LOG2E, F32) for h in range(4)], axis=1
        )
        cv = ctx[...].astype(F32).T[HD : 2 * HD].astype(BF16)
        cv = jnp.concatenate([cv, ones[:, 0:512]], axis=0)

        @pl.loop(0, q_ref.shape[1] // wide)
        def _(t):
            lanes = pl.ds(pl.multiple_of(t * wide, wide), wide)
            q = q_ref[:, lanes]
            left = tall(q)
            right = jnp.concatenate([jnp.zeros_like(q), q], axis=0)
            scores = jnp.dot(ctx[...], left, preferred_element_type=F32) + lifts
            top = jnp.max(scores, axis=0, keepdims=True)
            peak[...] = top
            weights = jnp.exp2(scores - top).astype(BF16)
            acc[...] = jnp.dot(cv, weights, preferred_element_type=F32)

            @pl.loop(0, N_SP)
            def _(b):
                parts = []
                for s in range(2):
                    k = kvbuf[b * 2 + s, pl.ds(0, 192), :]
                    for query in (left, right):
                        parts.append(jnp.dot(k, query, preferred_element_type=F32))
                x = jnp.concatenate(parts, axis=0)
                old = peak[...]
                new = jnp.maximum(old, jnp.max(x, axis=0, keepdims=True))
                peak[...] = new
                v = [
                    kvbuf[b * 2 + s, pl.ds(192 + i * 64, 64), :] for s in range(2) for i in range(3)
                ]
                v = jnp.concatenate([jnp.concatenate(v, axis=1), ones], axis=0)
                weights = jnp.exp2(x - new).astype(BF16)
                acc[...] = acc[...] * jnp.exp2(old - new) + jnp.dot(
                    v, weights, preferred_element_type=F32
                )

            mean = acc[0:HD, :] / acc[HD : HD + 1, :]
            stack = jnp.concatenate([mean[:, h * 128 : (h + 1) * 128] for h in range(4)], axis=0)
            rows = pl.ds(pl.multiple_of(t * 128, 128), 128)
            o_out[rows, :] = stack.T.astype(BF16)


def run_repair(l, o, q, kv_all, ctx, lift):
    return pl.pallas_call(
        repair_kernel,
        name="repair",
        out_shape=jax.ShapeDtypeStruct(o.shape, o.dtype),
        in_specs=[VMEM, VMEM, HBM, HBM, HBM, SMEM],
        out_specs=VMEM,
        scratch_shapes=[
            pltpu.VMEM((HD, 3072), BF16),
            pltpu.VMEM((2 * N_SP, 384, 128), BF16),
            pltpu.VMEM((512, 128), BF16),
            pltpu.VMEM((VROWS, 512), F32),
            pltpu.VMEM((1, 512), F32),
            pltpu.SemaphoreType.DMA(()),
        ],
        compiler_params=pltpu.CompilerParams(vmem_limit_bytes=67043328),
    )(l, o, q, kv_all, ctx, lift)


def exchange_kernel(o_ref, out, obuf, send_sem, recv_sem):
    tp = lax.axis_index("tp")
    rows = o_ref.shape[0] // N_TP

    def tp_at(k):
        return {"tp": lax.rem(tp + k, N_TP)}

    barrier = pltpu.get_barrier_semaphore()
    for k in range(1, N_TP):
        pl.semaphore_signal(barrier, inc=1, device_id=tp_at(k), device_id_type=MESH)
    pl.semaphore_wait(barrier, N_TP - 1)
    copies = []
    for i, (k, here, there, count) in enumerate(RETURNS):
        copies.append(
            pltpu.make_async_remote_copy(
                src_ref=o_ref.at[pl.ds(here, count)],
                dst_ref=obuf.at[tp, pl.ds(there, count)],
                send_sem=send_sem.at[i], recv_sem=recv_sem.at[i],
                device_id=tp_at(k), device_id_type=MESH,
            )
        )
        copies[-1].start()
    out[tp] = o_ref[0:rows, :]
    for copy in copies:
        copy.wait_recv()
    for k in range(1, N_TP):
        source = lax.rem(tp + k, N_TP)
        out[source] = obuf[source]
    for copy in copies:
        copy.wait_send()


def run_exchange(o):
    rows = o.shape[0] // N_TP
    dma = pltpu.SemaphoreType.DMA
    return pl.pallas_call(
        exchange_kernel,
        name="exchange",
        out_shape=jax.ShapeDtypeStruct((N_TP, rows, 256), BF16),
        in_specs=[VMEM],
        out_specs=VMEM,
        scratch_shapes=[pltpu.VMEM((N_TP, rows, 256), BF16), dma((5,)), dma((5,))],
        compiler_params=pltpu.CompilerParams(
            collective_id=2, has_side_effects=True, vmem_limit_bytes=4 * 2**20
        ),
        cost_estimate=pl.CostEstimate(flops=0, bytes_accessed=25 * 10**6, transcendentals=0),
    )(o)


def output_kernel(o_hbm, w_hbm, lat_hbm, gate, out, o, w, lat, total, sem):
    pairs = [(o_hbm, o)]
    pairs += [(w_hbm.at[pl.ds(t * 256, 256)], w.at[t]) for t in range(N_TP)]
    pairs += [(lat_hbm, lat)]
    loads = [pltpu.make_async_copy(a, b, sem.at[i]) for i, (a, b) in enumerate(pairs)]
    for load in loads:
        load.start()
    loads[0].wait()
    wide = 512
    for t in range(N_TP):
        loads[1 + t].wait()
        if t == N_TP - 1:
            loads[-1].wait()
        for n in range(out.shape[1] // wide):
            cols = slice(n * wide, (n + 1) * wide)
            term = jnp.dot(o[t], w[t, :, cols], preferred_element_type=F32)
            if t == 0:
                total[:, cols] = term
            elif t < N_TP - 1:
                total[:, cols] += term
            else:
                term = total[:, cols] + term
                out[:, cols] = (lat[:, cols].astype(F32) + gate[:, cols] * term).astype(BF16)


def run_output(o, w_out, lat, gate):
    return pl.pallas_call(
        output_kernel,
        name="output",
        out_shape=jax.ShapeDtypeStruct(lat.shape, BF16),
        in_specs=[HBM, HBM, HBM, VMEM],
        out_specs=VMEM,
        scratch_shapes=[
            pltpu.VMEM(o.shape, BF16),
            pltpu.VMEM((N_TP, 256, w_out.shape[1]), BF16),
            pltpu.VMEM(lat.shape, BF16),
            pltpu.VMEM(lat.shape, F32),
            pltpu.SemaphoreType.DMA((N_TP + 2,)),
        ],
        compiler_params=pltpu.CompilerParams(vmem_limit_bytes=67043328),
    )(o, w_out, lat, gate)


def settle_kernel(mixed, out, buf, sem_in, sem_out):
    pieces = buf.shape[0]
    count = buf.shape[1]
    loads, stores = [], []
    for i in range(pieces):
        rows = pl.ds(i * count, count)
        loads.append(pltpu.make_async_copy(mixed.at[rows], buf.at[i], sem_in.at[i]))
        stores.append(pltpu.make_async_copy(buf.at[i], out.at[rows], sem_out.at[i]))
    for load in loads:
        load.start()
    for load, store in zip(loads, stores):
        load.wait()
        store.start()
    for store in stores:
        store.wait()


def run_settle(mixed):
    rows, width = mixed.shape
    return pl.pallas_call(
        settle_kernel,
        name="settle",
        out_shape=jax.ShapeDtypeStruct(mixed.shape, mixed.dtype),
        in_specs=[HBM],
        out_specs=HBM,
        scratch_shapes=[
            pltpu.VMEM((4, rows // 4, width), BF16),
            pltpu.SemaphoreType.DMA((4,)),
            pltpu.SemaphoreType.DMA((4,)),
        ],
        compiler_params=pltpu.CompilerParams(vmem_limit_bytes=67043328),
    )(mixed)


def on_device(
    latent, cond, cond_ctx, context, norm_gain, mod_shift, mod_scale, mod_gate,
    w_query, w_key, w_value, q_gain, k_gain, ctx_lift, w_out,
):
    lat = latent[0]
    mixed, safe, o, l, q, kv_all, ctx, gate = run_attention(
        lat, cond, cond_ctx[None, :], context[0], norm_gain.reshape(-1, 128),
        mod_shift, mod_scale, mod_gate, w_query, w_key.T, w_value.T,
        q_gain[None, :], k_gain[None, :], ctx_lift, w_out,
    )

    def again(mixed, o, l, q, kv_all, ctx):
        o = run_exchange(run_repair(l, o, q, kv_all, ctx, ctx_lift))
        return run_output(o, w_out, lat, gate)

    def keep(mixed, *rest):
        return mixed

    mixed = lax.cond(safe[0] > 0, keep, again, mixed, o, l, q, kv_all, ctx)
    return run_settle(mixed)[None]


def solution(mesh):
    in_specs = (
        P("dp", ("sp", "tp"), None),
        P("dp", "sp"),
        P("sp"),
        P("dp", "sp", None),
        P(),
        P("sp", "tp"),
        P("sp", "tp"),
        P("sp", "tp"),
        P(None, "tp"),
        P(None, "tp"),
        P(None, "tp"),
        P(),
        P(),
        P("tp"),
        P(),
    )
    return jax.shard_map(
        on_device, mesh=mesh, in_specs=in_specs,
        out_specs=P("dp", ("sp", "tp"), None), check_vma=False,
    )
```
